32 devices in a mesh: rep: 2 (over x), fs: 8 (over z, y), tp: 2 (over core).
Axes of the slice: x: 2, y: 2, z: 4, core: 2. Of those that a mesh axis runs over, the one named last changes fastest.
Arguments:
- tokens: bfloat16 [6144, 2048], P(('rep', 'fs'), 'tp'), may hold values from -6 to 6
- mixing_norm_gain: float32 [2048], replicated, may hold values from 0.1 to 1.9
- recurrent_input_weight: float32 [2048, 3072], P('fs', 'tp'), may hold values from -0.125 to 0.125
- recurrent_input_scale: float32 [3072], P('tp'), may hold values from 0.5 to 2
- convolution_kernel_taps: float32 [4, 3072], P(None, 'tp'), may hold values from -3 to 3
- recurrence_gate_weight_blocks: bfloat16 [24, 128, 128], P('tp'), may hold values from -0.5 to 0.5
- input_gate_weight_blocks: bfloat16 [24, 128, 128], P('tp'), may hold values from -0.5 to 0.5
- channel_decay_parameter: float32 [3072], P('tp'), may hold values from 3 to 9
- token_extra_log_decay: float32 [6144], P(('rep', 'fs')), may hold values from -0.7 to 0
- mixing_output_weight: float32 [3072, 2048], P('tp', 'fs'), may hold values from -0.109375 to 0.109375
- mixing_output_scale: float32 [2048], P('fs'), may hold values from 0.5 to 2
- feedforward_norm_gain: float32 [2048], replicated, may hold values from 0.1 to 1.9
- feedforward_gate_weight: float32 [2048, 5120], P('fs', 'tp'), may hold values from -0.125 to 0.125
- feedforward_gate_scale: float32 [5120], P('tp'), may hold values from 0.5 to 2
- feedforward_up_weight: float32 [2048, 5120], P('fs', 'tp'), may hold values from -0.125 to 0.125
- feedforward_up_scale: float32 [5120], P('tp'), may hold values from 0.5 to 2
- feedforward_down_weight: float32 [5120, 2048], P('tp', 'fs'), may hold values from -0.078125 to 0.078125
- feedforward_down_scale: float32 [2048], P('fs'), may hold values from 0.5 to 2
Outputs:
- layer_out: bfloat16 [6144, 2048], P(('rep', 'fs'), 'tp')
The draws below stay inside these ranges and needn't reach their ends.
All inputs are finite; a program needn't handle non-finite values.
Results may differ from the reference program's by a relative error of at most 0.02.
Values may be sent and summed in bfloat16 or wider, within the bound.
A program may use at most 128 MiB of HBM per device.

```python
import math
import jax
import jax.numpy as jnp
from jax import lax

MODEL_DIM = 2048
W = 3072
FF = 5120
BLOCK = 128
CONV = 4
SEQUENCE_LENGTH = 384
NB = 24
TOKENS = 6144
N_TP = 2


def draw_token_extra_log_decay(key, part):
    first_key, second_key = jax.random.split(jax.random.fold_in(key, 17))
    chosen = jax.random.randint(first_key, (TOKENS,), 0, 64) == 0
    depth = jax.random.uniform(second_key, (TOKENS,), jnp.float32, 0.22, 0.7)
    return jnp.where(chosen, -depth, 0.0).astype(jnp.float32)


def block_levels(key, dims, pieces, least, high):
    level = 1.0
    for dim, shards_of in pieces:
        draws = jax.random.uniform(jax.random.fold_in(jax.random.fold_in(key, 6), dim), (shards_of,), jnp.float32, least / len(pieces), high / len(pieces))
        level = level * jnp.repeat(jnp.exp(draws), dims[dim] // shards_of).reshape((-1,) + (1,) * (len(dims) - 1 - dim))
    return level


def scatter_about(key, extent, scale, reach, pieces=(), held_as=jnp.bfloat16):
    result = jax.random.normal(key, extent, jnp.float32) * scale
    if len(pieces) > 0:
        result = block_levels(key, extent, pieces, -0.22, 0.18) * result
    return jnp.clip(result, min=-reach, max=reach).astype(held_as)


def setup_inputs(seed: int = 0) -> dict:
    key_of = jax.random.split(jax.random.key(seed), 19)
    return {
        "tokens": scatter_about(key_of[0], (TOKENS, MODEL_DIM), 1.0, 6.0, ((0, 16), (1, 2))),
        "mixing_norm_gain": jnp.clip(1.0 + 0.18 * jax.random.normal(key_of[1], (MODEL_DIM,), jnp.float32), 0.1, 1.9),
        "recurrent_input_weight": scatter_about(key_of[2], (MODEL_DIM, W), MODEL_DIM ** -0.5, 0.125, ((0, 8), (1, 2)), jnp.float32),
        "recurrent_input_scale": jnp.clip(jnp.exp(math.log(2.0) - 1.3862944 * jax.random.uniform(key_of[3], (W,), jnp.float32) ** block_levels(key_of[3], (W,), ((0, 2),), -0.2, 0.2)), 0.5, 2.0),
        "convolution_kernel_taps": scatter_about(key_of[4], (CONV, W), 0.5, 3.0, ((1, 2),), jnp.float32),
        "recurrence_gate_weight_blocks": scatter_about(key_of[5], (NB, BLOCK, BLOCK), BLOCK ** -0.5, 0.5, ((0, 2),)),
        "input_gate_weight_blocks": scatter_about(key_of[6], (NB, BLOCK, BLOCK), BLOCK ** -0.5, 0.5, ((0, 2),)),
        "channel_decay_parameter": jnp.clip(3.0 + 6.0 * jax.random.uniform(key_of[7], (W,), jnp.float32) ** block_levels(key_of[7], (W,), ((0, 2),), -0.2, 0.2), 3.0, 9.0),
        "token_extra_log_decay": draw_token_extra_log_decay(jax.random.fold_in(key_of[18], 71), 0),
        "mixing_output_weight": scatter_about(key_of[9], (W, MODEL_DIM), W ** -0.5, 0.109375, ((0, 2), (1, 8)), jnp.float32),
        "mixing_output_scale": jnp.clip(jnp.exp(math.log(2.0) - 1.3862944 * jax.random.uniform(key_of[10], (MODEL_DIM,), jnp.float32) ** block_levels(key_of[10], (MODEL_DIM,), ((0, 8),), -0.2, 0.2)), 0.5, 2.0),
        "feedforward_norm_gain": jnp.clip(1.0 + 0.18 * jax.random.normal(key_of[11], (MODEL_DIM,), jnp.float32), 0.1, 1.9),
        "feedforward_gate_weight": scatter_about(key_of[12], (MODEL_DIM, FF), MODEL_DIM ** -0.5, 0.125, ((0, 8), (1, 2)), jnp.float32),
        "feedforward_gate_scale": jnp.clip(jnp.exp(math.log(2.0) - 1.3862944 * jax.random.uniform(key_of[13], (FF,), jnp.float32) ** block_levels(key_of[13], (FF,), ((0, 2),), -0.2, 0.2)), 0.5, 2.0),
        "feedforward_up_weight": scatter_about(key_of[14], (MODEL_DIM, FF), MODEL_DIM ** -0.5, 0.125, ((0, 8), (1, 2)), jnp.float32),
        "feedforward_up_scale": jnp.clip(jnp.exp(math.log(2.0) - 1.3862944 * jax.random.uniform(key_of[15], (FF,), jnp.float32) ** block_levels(key_of[15], (FF,), ((0, 2),), -0.2, 0.2)), 0.5, 2.0),
        "feedforward_down_weight": scatter_about(key_of[16], (FF, MODEL_DIM), FF ** -0.5, 0.078125, ((0, 2), (1, 8)), jnp.float32),
        "feedforward_down_scale": jnp.clip(jnp.exp(math.log(2.0) - 1.3862944 * jax.random.uniform(key_of[17], (MODEL_DIM,), jnp.float32) ** block_levels(key_of[17], (MODEL_DIM,), ((0, 8),), -0.2, 0.2)), 0.5, 2.0),
    }


EPS = 1e-06
DECAY_FACTOR = 8.0

def row_norm(rows, gain_vec):
    values = rows.astype(jnp.float32)
    inverse = lax.rsqrt(lax.optimization_barrier(jnp.mean(values * values, axis=-1, keepdims=True)) + EPS)
    return (values * inverse * gain_vec).astype(jnp.bfloat16)

def combine_pairs(earlier, later):
    decay_one, value_one = earlier
    decay_two, value_two = later
    return (decay_one * decay_two, decay_two * value_one + value_two)

def grouped_sum(left_rows, weight_low, col_scale, groups):
    seq_rows, inner = left_rows.shape
    left_groups = left_rows.reshape(seq_rows, groups, inner // groups).astype(jnp.float32)
    weight_groups = weight_low.reshape(groups, inner // groups, weight_low.shape[1]).astype(jnp.float32)
    parts = jnp.einsum('lgw,gwd->gld', left_groups, weight_groups) * col_scale
    parts_low = parts.astype(jnp.bfloat16)
    parts_low = lax.optimization_barrier(parts_low)
    return lax.optimization_barrier(jnp.sum(parts_low.astype(jnp.float32), axis=0))

def reference(tokens, mixing_norm_gain, recurrent_input_weight, recurrent_input_scale, convolution_kernel_taps, recurrence_gate_weight_blocks, input_gate_weight_blocks, channel_decay_parameter, token_extra_log_decay, mixing_output_weight, mixing_output_scale, feedforward_norm_gain, feedforward_gate_weight, feedforward_gate_scale, feedforward_up_weight, feedforward_up_scale, feedforward_down_weight, feedforward_down_scale):
    rec_low = recurrent_input_weight.astype(jnp.bfloat16)
    mix_low = mixing_output_weight.astype(jnp.bfloat16)
    gate_low = feedforward_gate_weight.astype(jnp.bfloat16)
    up_low = feedforward_up_weight.astype(jnp.bfloat16)
    down_low = feedforward_down_weight.astype(jnp.bfloat16)
    recur_f32 = recurrence_gate_weight_blocks.astype(jnp.float32)
    input_f32 = input_gate_weight_blocks.astype(jnp.float32)

    def single_sequence(packed_arrays):
        sequence_token_rows, sequence_extra_decay = packed_arrays
        normed = row_norm(sequence_token_rows, mixing_norm_gain)
        rec_input = (jnp.dot(normed, rec_low, preferred_element_type=jnp.float32) * recurrent_input_scale).astype(jnp.bfloat16)
        rec_f32 = rec_input.astype(jnp.float32)
        padded = jnp.pad(rec_f32, ((CONV - 1, 0), (0, 0)))
        conv_out = jnp.zeros((SEQUENCE_LENGTH, W), jnp.float32)
        for tap_index in range(CONV):
            conv_out = conv_out + convolution_kernel_taps[tap_index] * padded[tap_index:tap_index + SEQUENCE_LENGTH]
        blocks = conv_out.astype(jnp.bfloat16).reshape(SEQUENCE_LENGTH, NB, BLOCK).astype(jnp.float32)
        recurrence_gate_values = jax.nn.sigmoid(jnp.einsum('lni,nij->lnj', blocks, recur_f32).reshape(SEQUENCE_LENGTH, W))
        input_gate = jax.nn.sigmoid(jnp.einsum('lni,nij->lnj', blocks, input_f32).reshape(SEQUENCE_LENGTH, W))
        decay_logarithm = -DECAY_FACTOR * recurrence_gate_values * jax.nn.softplus(-channel_decay_parameter) + sequence_extra_decay[:, None]
        decay = jnp.exp(decay_logarithm)
        drive = jnp.sqrt(-jnp.expm1(2.0 * decay_logarithm)) * input_gate * conv_out
        _, state = lax.associative_scan(combine_pairs, (decay, drive), axis=0)
        state_low = state.astype(jnp.bfloat16)
        mix_sum = grouped_sum(state_low, mix_low, mixing_output_scale, N_TP)
        mixed = (sequence_token_rows.astype(jnp.float32) + mix_sum).astype(jnp.bfloat16)
        normed_ffn = row_norm(mixed, feedforward_norm_gain)
        ffn_gate = jnp.dot(normed_ffn, gate_low, preferred_element_type=jnp.float32) * feedforward_gate_scale
        ffn_up = jnp.dot(normed_ffn, up_low, preferred_element_type=jnp.float32) * feedforward_up_scale
        hidden = (jax.nn.silu(ffn_gate) * ffn_up).astype(jnp.bfloat16)
        down_sum = grouped_sum(hidden, down_low, feedforward_down_scale, N_TP)
        return (mixed.astype(jnp.float32) + down_sum).astype(jnp.bfloat16)
    sequence_count = TOKENS // SEQUENCE_LENGTH
    output_list = lax.map(single_sequence, (tokens.reshape(sequence_count, SEQUENCE_LENGTH, MODEL_DIM), token_extra_log_decay.reshape(sequence_count, SEQUENCE_LENGTH)))
    return output_list.reshape(TOKENS, MODEL_DIM)
```

```python
import jax
import jax.numpy as jnp
from jax import lax
from jax.experimental import pallas as pl
from jax.experimental.pallas import tpu as pltpu
from jax.sharding import PartitionSpec as P

EPS = 1e-06
DECAY_FACTOR = 8.0


def row_norm(rows, gain_vec):
    values = rows.astype(jnp.float32)
    inverse = lax.rsqrt(jnp.mean(values * values, axis=-1, keepdims=True) + EPS)
    return (values * inverse * gain_vec).astype(jnp.bfloat16)


def gather_normed(rows, gain_vec):
    whole_rows = lax.all_gather(rows, "tp", axis=1, tiled=True)
    return row_norm(whole_rows, gain_vec)


def share_sums(terms):
    return lax.psum_scatter(
        terms.astype(jnp.bfloat16), "tp", scatter_dimension=1, tiled=True
    ).astype(jnp.float32)


def combine_pairs(earlier, later):
    decay_one, value_one = earlier
    decay_two, value_two = later
    return (decay_one * decay_two, decay_two * value_one + value_two)


def add_one(left_rows, weight_piece):
    return jnp.dot(left_rows, weight_piece, preferred_element_type=jnp.float32)


def place_columns(left_rows, total_now, pieces, start_row):
    weight_piece, scale_piece = pieces
    product = jnp.dot(left_rows, weight_piece, preferred_element_type=jnp.float32) * scale_piece
    return lax.dynamic_update_slice_in_dim(total_now, product, start_row, 1)


def plain_body(
    tokens,
    mixing_norm_gain,
    recurrent_input_weight,
    recurrent_input_scale,
    convolution_kernel_taps,
    recurrence_gate_weight_blocks,
    input_gate_weight_blocks,
    channel_decay_parameter,
    token_extra_log_decay,
    mixing_output_weight,
    mixing_output_scale,
    feedforward_norm_gain,
    feedforward_gate_weight,
    feedforward_gate_scale,
    feedforward_up_weight,
    feedforward_up_scale,
    feedforward_down_weight,
    feedforward_down_scale,
):
    normed = gather_normed(tokens, mixing_norm_gain)
    seq_rows = normed.shape[0]
    model_width = normed.shape[1]
    width_dev = recurrent_input_weight.shape[1]
    rec_sum = add_one(
        normed,
        lax.all_gather(recurrent_input_weight.astype(jnp.bfloat16), "fs", axis=0, tiled=True),
    )
    rec_input = (rec_sum * recurrent_input_scale).astype(jnp.bfloat16)
    rec_f32 = rec_input.astype(jnp.float32)
    tap_count = convolution_kernel_taps.shape[0]
    padded = jnp.pad(rec_f32, ((tap_count - 1, 0), (0, 0)))
    conv_out = jnp.zeros((seq_rows, width_dev), jnp.float32)
    for tap_index in range(tap_count):
        conv_out = (
            conv_out + convolution_kernel_taps[tap_index] * padded[tap_index : tap_index + seq_rows]
        )
    block_count = recurrence_gate_weight_blocks.shape[0]
    block_size = recurrence_gate_weight_blocks.shape[1]
    blocks = conv_out.astype(jnp.bfloat16).reshape(seq_rows, block_count, block_size)
    recurrence_gate_values = jax.nn.sigmoid(
        jnp.einsum(
            "lni,nij->lnj",
            blocks,
            recurrence_gate_weight_blocks,
            preferred_element_type=jnp.float32,
        ).reshape(seq_rows, width_dev)
    )
    input_gate = jax.nn.sigmoid(
        jnp.einsum(
            "lni,nij->lnj", blocks, input_gate_weight_blocks, preferred_element_type=jnp.float32
        ).reshape(seq_rows, width_dev)
    )
    decay_logarithm = (
        -DECAY_FACTOR * recurrence_gate_values * jax.nn.softplus(-channel_decay_parameter)
        + token_extra_log_decay[:, None]
    )
    decay = jnp.exp(decay_logarithm)
    drive = jnp.sqrt(-jnp.expm1(2.0 * decay_logarithm)) * input_gate * conv_out
    _, state = lax.associative_scan(combine_pairs, (decay, drive), axis=0)
    state_low = state.astype(jnp.bfloat16)
    mix_terms = place_columns(
        state_low,
        jnp.zeros((seq_rows, model_width), jnp.float32),
        (
            lax.all_gather(mixing_output_weight.astype(jnp.bfloat16), "fs", axis=1, tiled=True),
            lax.all_gather(
                mixing_output_scale.reshape(1, -1).astype(jnp.bfloat16), "fs", axis=1, tiled=True
            ).astype(jnp.float32),
        ),
        jnp.int32(0),
    )
    mixed = (tokens.astype(jnp.float32) + share_sums(mix_terms)).astype(jnp.bfloat16)
    normed_ffn = gather_normed(mixed, feedforward_norm_gain)
    gate_sum = add_one(
        normed_ffn,
        lax.all_gather(feedforward_gate_weight.astype(jnp.bfloat16), "fs", axis=0, tiled=True),
    )
    up_sum = add_one(
        normed_ffn,
        lax.all_gather(feedforward_up_weight.astype(jnp.bfloat16), "fs", axis=0, tiled=True),
    )
    hidden = (
        jax.nn.silu(gate_sum * feedforward_gate_scale) * (up_sum * feedforward_up_scale)
    ).astype(jnp.bfloat16)
    down_terms = place_columns(
        hidden,
        jnp.zeros((seq_rows, model_width), jnp.float32),
        (
            lax.all_gather(feedforward_down_weight.astype(jnp.bfloat16), "fs", axis=1, tiled=True),
            lax.all_gather(
                feedforward_down_scale.reshape(1, -1).astype(jnp.bfloat16), "fs", axis=1, tiled=True
            ).astype(jnp.float32),
        ),
        jnp.int32(0),
    )
    return (mixed.astype(jnp.float32) + share_sums(down_terms)).astype(jnp.bfloat16)


REC, MIX, GU, DOWN = range(4)
LOW = jnp.bfloat16
F32 = jnp.float32


def remote(src, dst, send_sem, recv_sem, device):
    return pltpu.make_async_remote_copy(
        src_ref=src,
        dst_ref=dst,
        send_sem=send_sem,
        recv_sem=recv_sem,
        device_id=device,
        device_id_type=pl.DeviceIdType.MESH,
    )


def layer_kernel(
    tokens,
    w_rec,
    w_mix,
    w_gate,
    w_up,
    w_down,
    gain_one,
    rec_scale,
    taps,
    recur_blocks,
    input_blocks,
    decay_param,
    extra,
    mix_scale,
    gain_two,
    gate_scale,
    up_scale,
    down_scale,
    out,
    nbuf,
    rec_w,
    mix_w,
    gu_w,
    down_w,
    f_rec,
    f_mix,
    f_gu,
    f_down,
    y_rec,
    y_mix,
    y_gu,
    y_down,
    tk,
    mx,
    st,
    hid,
    ri,
    ext,
    ecol,
    oth,
    kept,
    rt,
    r1,
    r2,
    oo,
    ob,
    load_sem,
    out_sem,
    wy_send,
    wo_send,
    wf_send,
    w_recv,
    g_send,
    g_recv,
    tt_sem,
    ex_send,
    ex_recv,
    m_send,
    m_recv,
    o_send,
    o_recv,
):
    rows, half_width = tokens.shape
    half, part = rows // 2, rows // 4
    width = half_width * 2
    chans = rec_w.shape[2]
    units = down_w.shape[1]
    cols = mix_w.shape[2]
    block = recur_blocks.shape[1]
    tap_count = taps.shape[0]

    r, f, t = lax.axis_index("rep"), lax.axis_index("fs"), lax.axis_index("tp")
    y, z = lax.rem(f, 2), lax.div(f, 2)
    fp = f + 1 - 2 * y
    q = r * 2 + y
    own, own_x, own_y, own_d = q, (1 - r) * 2 + y, r * 2 + 1 - y, (1 - r) * 2 + 1 - y
    x_dev, y_dev, t_dev = {"rep": 1 - r}, {"fs": fp}, {"tp": 1 - t}
    d_dev = {"rep": 1 - r, "fs": fp}
    inner = lax.div(z + 1, 2) == 1
    near = (1 + lax.rem(z, 2), lax.rem(2 + 3 * z, 5))
    near = tuple({"fs": plane * 2 + y} for plane in near)
    planes = (z, z + 1 - 2 * lax.rem(z, 2), z + 2 - 4 * lax.div(z, 2), 3 - z)
    mats = (rec_w, mix_w, gu_w, down_w)
    top, low = pl.ds(0, part), pl.ds(part, part)

    quarters = (q, r * 2 + 1 - y)
    loads = {}

    def load(name, number, src, dst):
        copy = pltpu.make_async_copy(src, dst, load_sem.at[number])
        copy.start()
        loads[name] = copy

    mine = pl.ds(pl.multiple_of(t * half, half), half)
    theirs = pl.ds(pl.multiple_of((1 - t) * half, half), half)
    side = pl.ds(pl.multiple_of(t * half_width, half_width), half_width)
    load("tok", 0, tokens.at[mine, :], tk.at[:, side])
    for i, piece in enumerate(quarters):
        at = pl.ds(pl.multiple_of(piece * chans, chans), chans)
        load(("rec", i), 1 + i, w_rec.at[:, at], f_rec.at[i])
    for i, piece in enumerate(quarters):
        at = pl.ds(pl.multiple_of(piece * chans, chans), chans)
        load(("mix", i), 3 + i, w_mix.at[at, :], f_mix.at[i])
    for i, piece in enumerate(quarters):
        at = pl.ds(pl.multiple_of(piece * units, units), units)
        load(("gate", i), 5 + i, w_gate.at[:, at], f_gu.at[i, 0])
        load(("up", i), 7 + i, w_up.at[:, at], f_gu.at[i, 1])
        load(("down", i), 9 + i, w_down.at[at, :], f_down.at[i])

    barrier = pltpu.get_barrier_semaphore()
    peers = [x_dev, y_dev, t_dev, d_dev]
    peers += [{"fs": plane * 2 + y} for plane in planes[1:]]
    for device in peers:
        pl.semaphore_signal(barrier, inc=1, device_id=device, device_id_type=pl.DeviceIdType.MESH)
    pl.semaphore_wait(barrier, len(peers))

    token_swap = remote(tokens.at[theirs, :], tk.at[:, side], tt_sem.at[0], tt_sem.at[1], t_dev)
    token_swap.start()

    def block_copy(k, place, send_sem, device):
        view = mats[k].at[place]
        return remote(view, view, send_sem, w_recv.at[k, place], device)

    def wait_block(k, place):
        block_copy(k, place, wo_send.at[0, 0, 0], y_dev).wait_recv()

    def send_own(k, j):
        place = f if j == 0 else fp
        if j == 1:
            wait_block(k, fp)
        for i, device in enumerate(near):
            block_copy(k, place, wo_send.at[k, j, i], device).start()

    y_bufs = (y_rec, y_mix, y_gu, y_down)

    def y_copy(k):
        return remote(y_bufs[k], mats[k].at[f], wy_send.at[k], w_recv.at[k, f], y_dev)

    def forward_copy(k, far, j):
        plane = 3 * (2 - z) if far else 3 - z
        place = plane * 2 + (y if j == 0 else 1 - y)
        edge = 3 * (z - 1)
        return place, block_copy(k, place, wf_send.at[k, far, j], {"fs": edge * 2 + y})

    def forward(k, far, j):
        @pl.when(inner)
        def _():
            place, copy = forward_copy(k, far, j)
            wait_block(k, place)
            copy.start()

    def need(k, p):
        def both():
            wait_block(k, planes[p] * 2)
            wait_block(k, planes[p] * 2 + 1)

        if p == 1:
            both()
        elif p > 1:
            pl.when(jnp.logical_not(inner))(both)

    def norm_rows(src, gain):
        def step(i, carry):
            at = pl.ds(pl.multiple_of(i * 16, 16), 16)
            v = src[at, :].astype(F32)
            inverse = lax.rsqrt(jnp.mean(v * v, axis=-1, keepdims=True) + EPS)
            nbuf[own, t, at, :] = (v * inverse * gain[...]).astype(LOW)
            return carry

        lax.fori_loop(0, half // 16, step, 0)

    def rows_copy(phase, role):
        seq, at, device = (
            (own, top, x_dev),
            (own, low, x_dev),
            (own, top, y_dev),
            (own, low, y_dev),
            (own_y, top, x_dev),
            (own_x, low, y_dev),
            (own, pl.ds(0, half), t_dev),
            (own_x, top, t_dev),
            (own_x, low, t_dev),
            (own_y, top, t_dev),
            (own_y, low, t_dev),
            (own_d, top, t_dev),
            (own_d, low, t_dev),
        )[role]
        view = nbuf.at[seq, t, at, :]
        return remote(view, view, g_send.at[phase, role], g_recv.at[phase, role], device)

    def rows_wait(phase, role):
        seq, side_at, at = (
            (own_x, t, top),
            (own_x, t, low),
            (own_y, t, top),
            (own_y, t, low),
            (own_d, t, top),
            (own_d, t, low),
            (own, 1 - t, pl.ds(0, half)),
            (own_x, 1 - t, top),
            (own_x, 1 - t, low),
            (own_y, 1 - t, top),
            (own_y, 1 - t, low),
            (own_d, 1 - t, top),
            (own_d, 1 - t, low),
        )[role]
        view = nbuf.at[seq, side_at, at, :]
        remote(view, view, g_send.at[phase, role], g_recv.at[phase, role], t_dev).wait_recv()

    def gather_start(phase):
        for role in (1, 2, 0, 3, 6):
            rows_copy(phase, role).start()

    def gather_first(phase):
        rows_wait(phase, 2)
        rows_copy(phase, 4).start()
        rows_wait(phase, 1)
        rows_copy(phase, 5).start()
        rows_copy(phase, 9).start()
        rows_copy(phase, 8).start()

    def gather_second(phase):
        rows_wait(phase, 0)
        rows_copy(phase, 7).start()
        rows_wait(phase, 3)
        rows_copy(phase, 10).start()

    def gather_last(phase):
        rows_wait(phase, 4)
        rows_copy(phase, 11).start()
        rows_wait(phase, 5)
        rows_copy(phase, 12).start()
        for role in range(6, 13):
            rows_wait(phase, role)
        for role in range(13):
            rows_copy(phase, role).wait_send()

    def products(phase, p, left, weights, k):
        need(k, p)
        first = planes[p] * 2

        def other(s, carry):
            for c in range(2):
                value = jnp.dot(left[s, 1 - t], weights[first + c], preferred_element_type=F32)
                oth[p, s, :, c * cols : (c + 1) * cols] = value.astype(LOW)
            return carry

        def keep(s, carry):
            for c in range(2):
                value = jnp.dot(left[s, t], weights[first + c], preferred_element_type=F32)
                kept[p, lax.div(s, 2), lax.rem(s, 2), :, c * cols : (c + 1) * cols] = value.astype(LOW)
            return carry

        lax.fori_loop(0, 4, other, 0)
        sum_copies(phase, p, 0).start()
        lax.fori_loop(0, 4, keep, 0)

    def sum_copies(phase, p, number):
        src, dst, device = (
            (oth.at[p], rt.at[phase, p], t_dev),
            (kept.at[p, 1 - r, :, top, :], r1.at[phase, p, 0], x_dev),
            (kept.at[p, :, 1 - y, low, :], r1.at[phase, p, 1], y_dev),
            (kept.at[p, r, 1 - y, top, :], r2.at[phase, p, 0], y_dev),
            (kept.at[p, 1 - r, y, low, :], r2.at[phase, p, 1], x_dev),
        )[number]
        return remote(src, dst, m_send.at[phase, p, number], m_recv.at[phase, p, number], device)

    def pair_sums(phase, p):
        sum_copies(phase, p, 0).wait_recv()

        def step(s, carry):
            a, b = lax.div(s, 2), lax.rem(s, 2)
            value = kept[p, a, b].astype(F32) + rt[phase, p, s].astype(F32)
            kept[p, a, b] = value.astype(LOW)
            return carry

        lax.fori_loop(0, 4, step, 0)
        sum_copies(phase, p, 1).start()
        sum_copies(phase, p, 2).start()

    def line_sums(phase, p):
        sum_copies(phase, p, 1).wait_recv()
        for i in range(2):
            value = kept[p, r, i, 0:part, :].astype(F32) + r1[phase, p, 0, i].astype(F32)
            kept[p, r, i, 0:part, :] = value.astype(LOW)
        sum_copies(phase, p, 3).start()
        sum_copies(phase, p, 2).wait_recv()
        for i in range(2):
            value = kept[p, i, y, part:half, :].astype(F32) + r1[phase, p, 1, i].astype(F32)
            kept[p, i, y, part:half, :] = value.astype(LOW)
        sum_copies(phase, p, 4).start()

    def last_sums(phase, p, base):
        at = pl.ds(pl.multiple_of(planes[p] * 2 * cols, 2 * cols), 2 * cols)
        values = []
        for i, number in enumerate((3, 4)):
            span = slice(i * part, (i + 1) * part)
            sum_copies(phase, p, number).wait_recv()
            value = kept[p, r, y, span, :].astype(F32) + r2[phase, p, i].astype(F32)
            values.append((base[span, at].astype(F32) + value).astype(LOW))
        for number in range(5):
            sum_copies(phase, p, number).wait_send()
        return at, values

    def mix_done(p):
        at, values = last_sums(0, p, tk)
        for i, value in enumerate(values):
            mx[i * part : (i + 1) * part, at] = value

    def out_copy(p):
        at = pl.ds(pl.multiple_of(lax.rem(planes[p], 2) * 2 * cols, 2 * cols), 2 * cols)
        return remote(oo.at[p], ob.at[t, :, at], o_send.at[p], o_recv.at[p], t_dev)

    def down_done(p):
        _, values = last_sums(1, p, mx)
        local = lax.div(planes[p], 2) == t
        at = pl.ds(pl.multiple_of(lax.rem(planes[p], 2) * 2 * cols, 2 * cols), 2 * cols)

        @pl.when(local)
        def _():
            for i, value in enumerate(values):
                ob[t, i * part : (i + 1) * part, at] = value

        @pl.when(jnp.logical_not(local))
        def _():
            for i, value in enumerate(values):
                oo[p, i * part : (i + 1) * part, :] = value
            out_copy(p).start()

    for i in range(2):
        loads["rec", i].wait()
    y_rec[...] = f_rec[1].astype(LOW)
    rec_w[f] = f_rec[0].astype(LOW)
    y_copy(REC).start()
    send_own(REC, 0)

    ext[own] = jnp.broadcast_to(extra[...], ext.shape[1:])
    loads["tok"].wait()
    token_swap.wait()
    norm_rows(tk, gain_one)
    gather_start(0)
    ext_copies = [
        remote(ext.at[own], ext.at[own], ex_send.at[i], ex_recv.at[i], device)
        for i, device in enumerate((x_dev, y_dev, d_dev))
    ]
    for copy in ext_copies:
        copy.start()

    for i in range(2):
        loads["mix", i].wait()
    y_mix[...] = (f_mix[1] * mix_scale[...]).astype(LOW)
    mix_w[f] = (f_mix[0] * mix_scale[...]).astype(LOW)
    y_copy(MIX).start()
    send_own(MIX, 0)
    send_own(REC, 1)
    for i in range(2):
        for name in ("gate", "up", "down"):
            loads[name, i].wait()
    for i in range(2):
        y_gu[:, i * units : (i + 1) * units] = f_gu[1, i].astype(LOW)
        gu_w[f, :, i * units : (i + 1) * units] = f_gu[0, i].astype(LOW)
    y_down[...] = (f_down[1] * down_scale[...]).astype(LOW)
    down_w[f] = (f_down[0] * down_scale[...]).astype(LOW)

    gather_first(0)
    forward(REC, 0, 0)
    forward(REC, 1, 0)
    send_own(MIX, 1)
    forward(REC, 0, 1)
    forward(REC, 1, 1)
    gather_second(0)
    y_copy(GU).start()
    send_own(GU, 0)
    gather_last(0)
    for i, seq in enumerate((own_x, own_y, own_d)):
        remote(ext.at[seq], ext.at[seq], ex_send.at[i], ex_recv.at[i], t_dev).wait_recv()
    forward(MIX, 0, 0)
    forward(MIX, 0, 1)
    for p in range(1, 4):
        need(REC, p)

    at_chans = pl.multiple_of(q * chans, chans)

    def recur(s, carry):
        left = nbuf[s].reshape(rows, width)
        total = jnp.dot(left, rec_w[...].reshape(width, chans), preferred_element_type=F32)
        ri[...] = (total * rec_scale[:, pl.ds(at_chans, chans)]).astype(LOW)
        ecol[...] = jnp.broadcast_to(ext[s, 0:1, :], (block, rows)).T
        for b in range(chans // block):
            here = slice(b * block, (b + 1) * block)
            lanes = pl.ds(pl.multiple_of(at_chans + b * block, block), block)
            number = q * (chans // block) + b
            values = ri[:, here].astype(F32)
            places = lax.broadcasted_iota(jnp.int32, values.shape, 0)
            conv_out = taps[tap_count - 1 : tap_count, lanes] * values
            for back in range(1, tap_count):
                moved = jnp.where(places >= back, pltpu.roll(values, back, 0), 0.0)
                tap = tap_count - 1 - back
                conv_out = conv_out + taps[tap : tap + 1, lanes] * moved
            conv_low = conv_out.astype(LOW)
            recur_gate = jax.nn.sigmoid(
                jnp.dot(conv_low, recur_blocks[number], preferred_element_type=F32)
            )
            input_gate = jax.nn.sigmoid(
                jnp.dot(conv_low, input_blocks[number], preferred_element_type=F32)
            )
            param = -decay_param[:, lanes]
            soft = jnp.maximum(param, 0.0) + jnp.log1p(jnp.exp(-jnp.abs(param)))
            log_decay = -DECAY_FACTOR * recur_gate * soft + ecol[...]
            decay = jnp.exp(log_decay)
            drive = jnp.sqrt(-jnp.tanh(log_decay) * (1.0 + decay * decay)) * input_gate * conv_out
            step = 1
            while step < rows:
                keep = places >= step
                drive = drive + decay * jnp.where(keep, pltpu.roll(drive, step, 0), 0.0)
                if step * 2 < rows:
                    decay = decay * jnp.where(keep, pltpu.roll(decay, step, 0), 1.0)
                step *= 2
            state = drive.astype(LOW)
            st[s, 0, :, here] = state[:half]
            st[s, 1, :, here] = state[half:]
        return carry

    lax.fori_loop(0, 4, recur, 0)

    forward(MIX, 1, 0)
    forward(MIX, 1, 1)
    send_own(GU, 1)
    y_copy(DOWN).start()
    send_own(DOWN, 0)

    products(0, 0, st, mix_w, MIX)
    products(0, 1, st, mix_w, MIX)
    pair_sums(0, 0)
    products(0, 2, st, mix_w, MIX)
    pair_sums(0, 1)
    line_sums(0, 0)
    products(0, 3, st, mix_w, MIX)
    pair_sums(0, 2)
    line_sums(0, 1)
    mix_done(0)
    pair_sums(0, 3)
    line_sums(0, 2)
    mix_done(1)
    line_sums(0, 3)
    mix_done(2)
    mix_done(3)

    norm_rows(mx, gain_two)
    gather_start(1)
    send_own(DOWN, 1)
    forward(GU, 0, 0)
    gather_first(1)
    forward(GU, 1, 0)
    gather_second(1)
    forward(GU, 0, 1)
    gather_last(1)
    forward(GU, 1, 1)
    for p in range(1, 4):
        need(GU, p)

    at_units = pl.ds(pl.multiple_of(q * units, units), units)

    def hidden(s, carry):
        left = nbuf[s].reshape(rows, width)
        total = jnp.dot(left, gu_w[...].reshape(width, 2 * units), preferred_element_type=F32)
        gate = total[:, :units] * gate_scale[:, at_units]
        up = total[:, units:] * up_scale[:, at_units]
        value = (gate * jax.nn.sigmoid(gate) * up).astype(LOW)
        hid[s, 0] = value[:half]
        hid[s, 1] = value[half:]
        return carry

    lax.fori_loop(0, 4, hidden, 0)

    products(1, 0, hid, down_w, DOWN)
    pair_sums(1, 0)
    forward(DOWN, 0, 0)
    forward(DOWN, 0, 1)
    line_sums(1, 0)
    forward(DOWN, 1, 0)
    forward(DOWN, 1, 1)
    down_done(0)
    for p in range(1, 4):
        products(1, p, hid, down_w, DOWN)
        pair_sums(1, p)
        line_sums(1, p)
        down_done(p)

    for p in range(4):
        local = lax.div(planes[p], 2) == t

        @pl.when(local)
        def _():
            out_copy(p).wait_recv()

        @pl.when(jnp.logical_not(local))
        def _():
            out_copy(p).wait_send()

    result = pltpu.make_async_copy(ob, out, out_sem)
    result.start()
    for k in range(4):
        y_copy(k).wait_send()
        for j in range(2):
            for i, device in enumerate(near):
                block_copy(k, f if j == 0 else fp, wo_send.at[k, j, i], device).wait_send()

        @pl.when(inner)
        def _():
            for far in range(2):
                for j in range(2):
                    forward_copy(k, far, j)[1].wait_send()

    for copy in ext_copies:
        copy.wait_send()
    result.wait()


def team_body(
    tokens,
    mixing_norm_gain,
    recurrent_input_weight,
    recurrent_input_scale,
    convolution_kernel_taps,
    recurrence_gate_weight_blocks,
    input_gate_weight_blocks,
    channel_decay_parameter,
    token_extra_log_decay,
    mixing_output_weight,
    mixing_output_scale,
    feedforward_norm_gain,
    feedforward_gate_weight,
    feedforward_gate_scale,
    feedforward_up_weight,
    feedforward_up_scale,
    feedforward_down_weight,
    feedforward_down_scale,
):
    rows, half_width = tokens.shape
    half, part = rows // 2, rows // 4
    width = half_width * 2
    depth = recurrent_input_weight.shape[0]
    chans = recurrent_input_weight.shape[1] // 4
    units = feedforward_gate_weight.shape[1] // 4
    cols = mixing_output_weight.shape[1]
    block = recurrence_gate_weight_blocks.shape[1]
    planes = width // depth
    any_spec = pl.BlockSpec(memory_space=pl.ANY)
    vmem_spec = pl.BlockSpec(memory_space=pltpu.VMEM)
    vmem = pltpu.VMEM
    dma = pltpu.SemaphoreType.DMA

    def row(vector):
        return vector.reshape(1, -1)

    out = pl.pallas_call(
        layer_kernel,
        out_shape=jax.ShapeDtypeStruct((2, half, half_width), LOW),
        in_specs=[any_spec] * 6 + [vmem_spec] * 12,
        out_specs=any_spec,
        scratch_shapes=[
            vmem((4, 2, half, width), LOW),
            vmem((planes, depth, chans), LOW),
            vmem((planes, chans, cols), LOW),
            vmem((planes, depth, 2 * units), LOW),
            vmem((planes, units, cols), LOW),
            vmem((2, depth, chans), F32),
            vmem((2, chans, cols), F32),
            vmem((2, 2, depth, units), F32),
            vmem((2, units, cols), F32),
            vmem((depth, chans), LOW),
            vmem((chans, cols), LOW),
            vmem((depth, 2 * units), LOW),
            vmem((units, cols), LOW),
            vmem((half, width), LOW),
            vmem((half, width), LOW),
            vmem((4, 2, half, chans), LOW),
            vmem((4, 2, half, units), LOW),
            vmem((rows, chans), LOW),
            vmem((4, 8, rows), F32),
            vmem((rows, block), F32),
            vmem((4, 4, half, 2 * cols), LOW),
            vmem((4, 2, 2, half, 2 * cols), LOW),
            vmem((2, 4, 4, half, 2 * cols), LOW),
            vmem((2, 4, 2, 2, part, 2 * cols), LOW),
            vmem((2, 4, 2, part, 2 * cols), LOW),
            vmem((4, half, 2 * cols), LOW),
            vmem((2, half, half_width), LOW),
            dma((11,)),
            dma,
            dma((4,)),
            dma((4, 2, 2)),
            dma((4, 2, 2)),
            dma((4, planes)),
            dma((2, 13)),
            dma((2, 13)),
            dma((2,)),
            dma((3,)),
            dma((3,)),
            dma((2, 4, 5)),
            dma((2, 4, 5)),
            dma((4,)),
            dma((4,)),
        ],
        compiler_params=pltpu.CompilerParams(
            collective_id=0, has_side_effects=True, vmem_limit_bytes=VMEM_BYTES
        ),
    )(
        tokens,
        recurrent_input_weight,
        mixing_output_weight,
        feedforward_gate_weight,
        feedforward_up_weight,
        feedforward_down_weight,
        row(mixing_norm_gain),
        row(recurrent_input_scale),
        convolution_kernel_taps,
        recurrence_gate_weight_blocks,
        input_gate_weight_blocks,
        row(channel_decay_parameter),
        row(token_extra_log_decay),
        row(mixing_output_scale),
        row(feedforward_norm_gain),
        row(feedforward_gate_scale),
        row(feedforward_up_scale),
        row(feedforward_down_scale),
    )
    return out.reshape(rows, half_width)


VMEM_BYTES = 66_000_000


def team_fits(mesh):
    sizes = mesh.shape
    return sizes["rep"] == 2 and sizes["tp"] == 2 and sizes["fs"] == 8


def solution(mesh):
    placed = (
        P(("rep", "fs"), "tp"),
        P(),
        P("fs", "tp"),
        P("tp"),
        P(None, "tp"),
        P("tp", None, None),
        P("tp", None, None),
        P("tp"),
        P(("rep", "fs")),
        P("tp", "fs"),
        P("fs"),
        P(),
        P("fs", "tp"),
        P("tp"),
        P("fs", "tp"),
        P("tp"),
        P("tp", "fs"),
        P("fs"),
    )

    def body(*args):
        blocks, hidden, rows = args[5].shape[0], args[12].shape[1], args[0].shape[0]
        if not team_fits(mesh) or blocks % 4 or hidden % 512 or rows % 64:
            return plain_body(*args)
        return team_body(*args)

    return jax.shard_map(
        body, mesh=mesh, in_specs=placed, out_specs=P(("rep", "fs"), "tp"), check_vma=False
    )
```

```python
import jax
import jax.numpy as jnp
from jax import lax
from jax.experimental import pallas as pl
from jax.experimental.pallas import tpu as pltpu
from jax.sharding import PartitionSpec as P

EPS = 1e-06
DECAY_FACTOR = 8.0


def row_norm(rows, gain_vec):
    values = rows.astype(jnp.float32)
    inverse = lax.rsqrt(jnp.mean(values * values, axis=-1, keepdims=True) + EPS)
    return (values * inverse * gain_vec).astype(jnp.bfloat16)


def gather_normed(rows, gain_vec):
    whole_rows = lax.all_gather(rows, "tp", axis=1, tiled=True)
    return row_norm(whole_rows, gain_vec)


def share_sums(terms):
    return lax.psum_scatter(
        terms.astype(jnp.bfloat16), "tp", scatter_dimension=1, tiled=True
    ).astype(jnp.float32)


def combine_pairs(earlier, later):
    decay_one, value_one = earlier
    decay_two, value_two = later
    return (decay_one * decay_two, decay_two * value_one + value_two)


def add_one(left_rows, weight_piece):
    return jnp.dot(left_rows, weight_piece, preferred_element_type=jnp.float32)


def place_columns(left_rows, total_now, pieces, start_row):
    weight_piece, scale_piece = pieces
    product = jnp.dot(left_rows, weight_piece, preferred_element_type=jnp.float32) * scale_piece
    return lax.dynamic_update_slice_in_dim(total_now, product, start_row, 1)


def plain_body(
    tokens,
    mixing_norm_gain,
    recurrent_input_weight,
    recurrent_input_scale,
    convolution_kernel_taps,
    recurrence_gate_weight_blocks,
    input_gate_weight_blocks,
    channel_decay_parameter,
    token_extra_log_decay,
    mixing_output_weight,
    mixing_output_scale,
    feedforward_norm_gain,
    feedforward_gate_weight,
    feedforward_gate_scale,
    feedforward_up_weight,
    feedforward_up_scale,
    feedforward_down_weight,
    feedforward_down_scale,
):
    normed = gather_normed(tokens, mixing_norm_gain)
    seq_rows = normed.shape[0]
    model_width = normed.shape[1]
    width_dev = recurrent_input_weight.shape[1]
    rec_sum = add_one(
        normed,
        lax.all_gather(recurrent_input_weight.astype(jnp.bfloat16), "fs", axis=0, tiled=True),
    )
    rec_input = (rec_sum * recurrent_input_scale).astype(jnp.bfloat16)
    rec_f32 = rec_input.astype(jnp.float32)
    tap_count = convolution_kernel_taps.shape[0]
    padded = jnp.pad(rec_f32, ((tap_count - 1, 0), (0, 0)))
    conv_out = jnp.zeros((seq_rows, width_dev), jnp.float32)
    for tap_index in range(tap_count):
        conv_out = (
            conv_out + convolution_kernel_taps[tap_index] * padded[tap_index : tap_index + seq_rows]
        )
    block_count = recurrence_gate_weight_blocks.shape[0]
    block_size = recurrence_gate_weight_blocks.shape[1]
    blocks = conv_out.astype(jnp.bfloat16).reshape(seq_rows, block_count, block_size)
    recurrence_gate_values = jax.nn.sigmoid(
        jnp.einsum(
            "lni,nij->lnj",
            blocks,
            recurrence_gate_weight_blocks,
            preferred_element_type=jnp.float32,
        ).reshape(seq_rows, width_dev)
    )
    input_gate = jax.nn.sigmoid(
        jnp.einsum(
            "lni,nij->lnj", blocks, input_gate_weight_blocks, preferred_element_type=jnp.float32
        ).reshape(seq_rows, width_dev)
    )
    decay_logarithm = (
        -DECAY_FACTOR * recurrence_gate_values * jax.nn.softplus(-channel_decay_parameter)
        + token_extra_log_decay[:, None]
    )
    decay = jnp.exp(decay_logarithm)
    drive = jnp.sqrt(-jnp.expm1(2.0 * decay_logarithm)) * input_gate * conv_out
    _, state = lax.associative_scan(combine_pairs, (decay, drive), axis=0)
    state_low = state.astype(jnp.bfloat16)
    mix_terms = place_columns(
        state_low,
        jnp.zeros((seq_rows, model_width), jnp.float32),
        (
            lax.all_gather(mixing_output_weight.astype(jnp.bfloat16), "fs", axis=1, tiled=True),
            lax.all_gather(
                mixing_output_scale.reshape(1, -1).astype(jnp.bfloat16), "fs", axis=1, tiled=True
            ).astype(jnp.float32),
        ),
        jnp.int32(0),
    )
    mixed = (tokens.astype(jnp.float32) + share_sums(mix_terms)).astype(jnp.bfloat16)
    normed_ffn = gather_normed(mixed, feedforward_norm_gain)
    gate_sum = add_one(
        normed_ffn,
        lax.all_gather(feedforward_gate_weight.astype(jnp.bfloat16), "fs", axis=0, tiled=True),
    )
    up_sum = add_one(
        normed_ffn,
        lax.all_gather(feedforward_up_weight.astype(jnp.bfloat16), "fs", axis=0, tiled=True),
    )
    hidden = (
        jax.nn.silu(gate_sum * feedforward_gate_scale) * (up_sum * feedforward_up_scale)
    ).astype(jnp.bfloat16)
    down_terms = place_columns(
        hidden,
        jnp.zeros((seq_rows, model_width), jnp.float32),
        (
            lax.all_gather(feedforward_down_weight.astype(jnp.bfloat16), "fs", axis=1, tiled=True),
            lax.all_gather(
                feedforward_down_scale.reshape(1, -1).astype(jnp.bfloat16), "fs", axis=1, tiled=True
            ).astype(jnp.float32),
        ),
        jnp.int32(0),
    )
    return (mixed.astype(jnp.float32) + share_sums(down_terms)).astype(jnp.bfloat16)


REC, MIX, GU, DOWN = range(4)
LOW = jnp.bfloat16
F32 = jnp.float32


def remote(src, dst, send_sem, recv_sem, device):
    return pltpu.make_async_remote_copy(
        src_ref=src,
        dst_ref=dst,
        send_sem=send_sem,
        recv_sem=recv_sem,
        device_id=device,
        device_id_type=pl.DeviceIdType.MESH,
    )


def layer_kernel(
    tokens,
    w_rec,
    w_mix,
    w_gate,
    w_up,
    w_down,
    gain_one,
    rec_scale,
    taps,
    recur_blocks,
    input_blocks,
    decay_param,
    extra,
    mix_scale,
    gain_two,
    gate_scale,
    up_scale,
    down_scale,
    out,
    nbuf,
    rec_w,
    mix_w,
    gu_w,
    down_w,
    f_rec,
    f_mix,
    f_gu,
    f_down,
    y_rec,
    y_mix,
    y_gu,
    y_down,
    tk,
    mx,
    st,
    hid,
    ri,
    ext,
    ecol,
    oth,
    kept,
    rt,
    r1,
    r2,
    oo,
    ob,
    load_sem,
    out_sem,
    wy_send,
    wo_send,
    wf_send,
    w_recv,
    g_send,
    g_recv,
    tt_sem,
    ex_send,
    ex_recv,
    m_send,
    m_recv,
    o_send,
    o_recv,
):
    rows, half_width = tokens.shape
    half, part = rows // 2, rows // 4
    width = half_width * 2
    chans = rec_w.shape[2]
    units = down_w.shape[1]
    cols = mix_w.shape[2]
    block = recur_blocks.shape[1]
    tap_count = taps.shape[0]

    r, f, t = lax.axis_index("rep"), lax.axis_index("fs"), lax.axis_index("tp")
    y, z = lax.rem(f, 2), lax.div(f, 2)
    fp = f + 1 - 2 * y
    q = r * 2 + y
    own, own_x, own_y, own_d = q, (1 - r) * 2 + y, r * 2 + 1 - y, (1 - r) * 2 + 1 - y
    x_dev, y_dev, t_dev = {"rep": 1 - r}, {"fs": fp}, {"tp": 1 - t}
    d_dev = {"rep": 1 - r, "fs": fp}
    inner = lax.div(z + 1, 2) == 1
    near = (1 + lax.rem(z, 2), lax.rem(2 + 3 * z, 5))
    near = tuple({"fs": plane * 2 + y} for plane in near)
    planes = (z, z + 1 - 2 * lax.rem(z, 2), z + 2 - 4 * lax.div(z, 2), 3 - z)
    mats = (rec_w, mix_w, gu_w, down_w)
    top, low = pl.ds(0, part), pl.ds(part, part)

    quarters = (q, r * 2 + 1 - y)
    loads = {}

    def load(name, number, src, dst):
        copy = pltpu.make_async_copy(src, dst, load_sem.at[number])
        copy.start()
        loads[name] = copy

    mine = pl.ds(pl.multiple_of(t * half, half), half)
    theirs = pl.ds(pl.multiple_of((1 - t) * half, half), half)
    side = pl.ds(pl.multiple_of(t * half_width, half_width), half_width)
    load("tok", 0, tokens.at[mine, :], tk.at[:, side])
    for i, piece in enumerate(quarters):
        at = pl.ds(pl.multiple_of(piece * chans, chans), chans)
        load(("rec", i), 1 + i, w_rec.at[:, at], f_rec.at[i])
    for i, piece in enumerate(quarters):
        at = pl.ds(pl.multiple_of(piece * chans, chans), chans)
        load(("mix", i), 3 + i, w_mix.at[at, :], f_mix.at[i])
    for i, piece in enumerate(quarters):
        at = pl.ds(pl.multiple_of(piece * units, units), units)
        load(("gate", i), 5 + i, w_gate.at[:, at], f_gu.at[i, 0])
        load(("up", i), 7 + i, w_up.at[:, at], f_gu.at[i, 1])
        load(("down", i), 9 + i, w_down.at[at, :], f_down.at[i])

    barrier = pltpu.get_barrier_semaphore()
    peers = [x_dev, y_dev, t_dev, d_dev]
    peers += [{"fs": plane * 2 + y} for plane in planes[1:]]
    for device in peers:
        pl.semaphore_signal(barrier, inc=1, device_id=device, device_id_type=pl.DeviceIdType.MESH)

    token_swap = remote(tokens.at[theirs, :], tk.at[:, side], tt_sem.at[0], tt_sem.at[1], t_dev)

    def block_copy(k, place, send_sem, device):
        view = mats[k].at[place]
        return remote(view, view, send_sem, w_recv.at[k, place], device)

    def wait_block(k, place):
        block_copy(k, place, wo_send.at[0, 0, 0], y_dev).wait_recv()

    def own_place(k, j):
        return z * 2 + j if k == DOWN else (f if j == 0 else fp)

    def send_own(k, j):
        if j == 1 and k != DOWN:
            wait_block(k, fp)
        for i, device in enumerate(near):
            block_copy(k, own_place(k, j), wo_send.at[k, j, i], device).start()

    y_bufs = (y_rec, y_mix, y_gu, y_down)

    def y_copy(k):
        return remote(y_bufs[k], mats[k].at[f], wy_send.at[k], w_recv.at[k, f], y_dev)

    def forward_copy(k, far, j):
        plane = 3 * (2 - z) if far else 3 - z
        place = plane * 2 + (j if k == DOWN else (y if j == 0 else 1 - y))
        edge = 3 * (z - 1)
        return place, block_copy(k, place, wf_send.at[k, far, j], {"fs": edge * 2 + y})

    def forward(k, far, j):
        @pl.when(inner)
        def _():
            place, copy = forward_copy(k, far, j)
            wait_block(k, place)
            copy.start()

    def need(k, p, blocks=(0, 1)):
        def wait():
            for j in blocks:
                wait_block(k, planes[p] * 2 + j)

        if p == 1:
            wait()
        elif p > 1:
            pl.when(jnp.logical_not(inner))(wait)

    def norm_rows(src, gain):
        def step(i, carry):
            at = pl.ds(pl.multiple_of(i * 16, 16), 16)
            v = src[at, :].astype(F32)
            inverse = lax.rsqrt(jnp.mean(v * v, axis=-1, keepdims=True) + EPS)
            nbuf[own, t, at, :] = (v * inverse * gain[...]).astype(LOW)
            return carry

        lax.fori_loop(0, half // 16, step, 0)

    def rows_copy(phase, role):
        seq, at, device = (
            (own, top, x_dev),
            (own, low, x_dev),
            (own, top, y_dev),
            (own, low, y_dev),
            (own_y, top, x_dev),
            (own_x, low, y_dev),
            (own, pl.ds(0, half), t_dev),
            (own_x, top, t_dev),
            (own_x, low, t_dev),
            (own_y, top, t_dev),
            (own_y, low, t_dev),
            (own_d, top, t_dev),
            (own_d, low, t_dev),
        )[role]
        view = nbuf.at[seq, t, at, :]
        return remote(view, view, g_send.at[phase, role], g_recv.at[phase, role], device)

    def rows_wait(phase, role):
        seq, side_at, at = (
            (own_x, t, top),
            (own_x, t, low),
            (own_y, t, top),
            (own_y, t, low),
            (own_d, t, top),
            (own_d, t, low),
            (own, 1 - t, pl.ds(0, half)),
            (own_x, 1 - t, top),
            (own_x, 1 - t, low),
            (own_y, 1 - t, top),
            (own_y, 1 - t, low),
            (own_d, 1 - t, top),
            (own_d, 1 - t, low),
        )[role]
        view = nbuf.at[seq, side_at, at, :]
        remote(view, view, g_send.at[phase, role], g_recv.at[phase, role], t_dev).wait_recv()

    def gather_start(phase):
        for role in (1, 2, 0, 3, 6):
            rows_copy(phase, role).start()

    def gather_first(phase):
        rows_wait(phase, 2)
        rows_copy(phase, 4).start()
        rows_wait(phase, 1)
        rows_copy(phase, 5).start()
        rows_copy(phase, 9).start()
        rows_copy(phase, 8).start()

    def gather_second(phase):
        rows_wait(phase, 0)
        rows_copy(phase, 7).start()
        rows_wait(phase, 3)
        rows_copy(phase, 10).start()

    def gather_last(phase):
        rows_wait(phase, 4)
        rows_copy(phase, 11).start()
        rows_wait(phase, 5)
        rows_copy(phase, 12).start()
        for role in range(6, 13):
            rows_wait(phase, role)
        for role in range(13):
            rows_copy(phase, role).wait_send()

    def products(phase, p, left, weights, k, blocks=(0, 1)):
        need(k, p, blocks)
        first = planes[p] * 2

        def product(side, c):
            rows_now = left[:, side].reshape(4 * half, left.shape[-1])
            value = jnp.dot(rows_now, weights[first + c], preferred_element_type=F32)
            return value.astype(LOW).reshape(4, half, cols)

        for c in blocks:
            oth[p, :, :, c * cols : (c + 1) * cols] = product(1 - t, c)
        sum_copies(phase, p, 0, blocks).start()
        for c in blocks:
            value = product(t, c).reshape(2, 2, half, cols)
            kept[p, :, :, :, c * cols : (c + 1) * cols] = value

    def span_of(blocks):
        return pl.ds(blocks[0] * cols, len(blocks) * cols)

    def sum_copies(phase, p, number, blocks):
        at = span_of(blocks)
        src, dst, device = (
            (oth.at[p, :, :, at], rt.at[phase, p, :, :, at], t_dev),
            (kept.at[p, 1 - r, :, top, at], r1.at[phase, p, 0, :, :, at], x_dev),
            (kept.at[p, :, 1 - y, low, at], r1.at[phase, p, 1, :, :, at], y_dev),
            (kept.at[p, r, 1 - y, top, at], r2.at[phase, p, 0, :, at], y_dev),
            (kept.at[p, 1 - r, y, low, at], r2.at[phase, p, 1, :, at], x_dev),
        )[number]
        number += 5 * blocks[0]
        return remote(src, dst, m_send.at[phase, p, number], m_recv.at[phase, p, number], device)

    def pair_sums(phase, p, blocks=(0, 1)):
        sum_copies(phase, p, 0, blocks).wait_recv()
        at = span_of(blocks)

        def step(s, carry):
            a, b = lax.div(s, 2), lax.rem(s, 2)
            value = kept[p, a, b, :, at].astype(F32) + rt[phase, p, s, :, at].astype(F32)
            kept[p, a, b, :, at] = value.astype(LOW)
            return carry

        lax.fori_loop(0, 4, step, 0)
        sum_copies(phase, p, 1, blocks).start()
        sum_copies(phase, p, 2, blocks).start()

    def line_sums(phase, p, blocks=(0, 1)):
        at = span_of(blocks)
        sum_copies(phase, p, 1, blocks).wait_recv()
        for i in range(2):
            value = kept[p, r, i, top, at].astype(F32) + r1[phase, p, 0, i, :, at].astype(F32)
            kept[p, r, i, top, at] = value.astype(LOW)
        sum_copies(phase, p, 3, blocks).start()
        sum_copies(phase, p, 2, blocks).wait_recv()
        for i in range(2):
            value = kept[p, i, y, low, at].astype(F32) + r1[phase, p, 1, i, :, at].astype(F32)
            kept[p, i, y, low, at] = value.astype(LOW)
        sum_copies(phase, p, 4, blocks).start()

    def columns_of(plane, blocks):
        start = pl.multiple_of((plane * 2 + blocks[0]) * cols, cols)
        return pl.ds(start, len(blocks) * cols)

    def last_sums(phase, p, base, blocks):
        at, piece = columns_of(planes[p], blocks), span_of(blocks)
        values = []
        for i, number in enumerate((3, 4)):
            span = slice(i * part, (i + 1) * part)
            sum_copies(phase, p, number, blocks).wait_recv()
            value = kept[p, r, y, span, piece].astype(F32) + r2[phase, p, i, :, piece].astype(F32)
            values.append((base[span, at].astype(F32) + value).astype(LOW))
        for number in range(5):
            sum_copies(phase, p, number, blocks).wait_send()
        return at, values

    def mix_done(p):
        at, values = last_sums(0, p, tk, (0, 1))
        for i, value in enumerate(values):
            mx[i * part : (i + 1) * part, at] = value

    def out_copy(p, blocks):
        at = columns_of(lax.rem(planes[p], 2), blocks)
        src = oo.at[p, :, span_of(blocks)]
        return remote(src, ob.at[t, :, at], o_send.at[p, blocks[0]], o_recv.at[p, blocks[0]], t_dev)

    def down_done(p, blocks=(0, 1)):
        _, values = last_sums(1, p, mx, blocks)
        local = lax.div(planes[p], 2) == t
        at = columns_of(lax.rem(planes[p], 2), blocks)

        @pl.when(local)
        def _():
            for i, value in enumerate(values):
                ob[t, i * part : (i + 1) * part, at] = value

        @pl.when(jnp.logical_not(local))
        def _():
            for i, value in enumerate(values):
                oo[p, i * part : (i + 1) * part, span_of(blocks)] = value
            out_copy(p, blocks).start()

    for i in range(2):
        loads["rec", i].wait()
    y_rec[...] = f_rec[1].astype(LOW)
    rec_w[f] = f_rec[0].astype(LOW)
    pl.semaphore_wait(barrier, len(peers))
    token_swap.start()
    y_copy(REC).start()
    send_own(REC, 0)
    loads["tok"].wait()
    token_swap.wait()
    norm_rows(tk, gain_one)
    gather_start(0)

    for i in range(2):
        loads["mix", i].wait()
    y_mix[...] = (f_mix[1] * mix_scale[...]).astype(LOW)
    mix_w[f] = (f_mix[0] * mix_scale[...]).astype(LOW)
    send_own(MIX, 0)
    send_own(REC, 1)
    for i in range(extra.shape[0]):
        lanes = slice(i * block, (i + 1) * block)
        ext[own, :, lanes] = jnp.broadcast_to(extra[i : i + 1, :], (ext.shape[1], block))
    ext_copies = [
        remote(ext.at[own], ext.at[own], ex_send.at[i], ex_recv.at[i], device)
        for i, device in enumerate((x_dev, y_dev, d_dev))
    ]
    for copy in ext_copies:
        copy.start()
    for i in range(2):
        for name in ("gate", "up", "down"):
            loads[name, i].wait()
    for i in range(2):
        y_gu[:, i * units : (i + 1) * units] = f_gu[1, i].astype(LOW)
        gu_w[f, :, i * units : (i + 1) * units] = f_gu[0, i].astype(LOW)
    y_down[...] = (f_down[1] * down_scale[...]).astype(LOW)
    down_w[f] = (f_down[0] * down_scale[...]).astype(LOW)

    forward(REC, 0, 0)
    forward(REC, 1, 0)
    gather_first(0)
    y_copy(MIX).start()
    y_copy(GU).start()
    y_copy(DOWN).start()
    forward(REC, 0, 1)
    forward(REC, 1, 1)
    gather_second(0)
    forward(MIX, 0, 0)
    forward(MIX, 1, 0)
    gather_last(0)
    for i, seq in enumerate((own_x, own_y, own_d)):
        remote(ext.at[seq], ext.at[seq], ex_send.at[i], ex_recv.at[i], t_dev).wait_recv()
    for p in range(1, 4):
        need(REC, p)

    at_chans = pl.multiple_of(q * chans, chans)

    def recur(s, carry):
        @pl.when(s == 1)
        def _():
            send_own(MIX, 1)
            send_own(GU, 0)

        @pl.when(s == 2)
        def _():
            forward(MIX, 0, 1)

        @pl.when(s == 3)
        def _():
            forward(MIX, 1, 1)

        left = nbuf[s].reshape(rows, width)
        total = jnp.dot(left, rec_w[...].reshape(width, chans), preferred_element_type=F32)
        for b in range(chans // block):
            here = slice(b * block, (b + 1) * block)
            number = q * (chans // block) + b
            ri[:, here] = (total[:, here] * rec_scale[pl.ds(number, 1), :]).astype(LOW)
        ecol[...] = jnp.broadcast_to(ext[s, 0:1, :], (block, rows)).T
        for b in range(chans // block):
            here = slice(b * block, (b + 1) * block)
            lanes = pl.ds(pl.multiple_of(at_chans + b * block, block), block)
            number = q * (chans // block) + b
            values = ri[:, here].astype(F32)
            places = lax.broadcasted_iota(jnp.int32, values.shape, 0)
            conv_out = taps[tap_count - 1 : tap_count, lanes] * values
            for back in range(1, tap_count):
                moved = jnp.where(places >= back, pltpu.roll(values, back, 0), 0.0)
                tap = tap_count - 1 - back
                conv_out = conv_out + taps[tap : tap + 1, lanes] * moved
            conv_low = conv_out.astype(LOW)
            recur_gate = jax.nn.sigmoid(
                jnp.dot(conv_low, recur_blocks[number], preferred_element_type=F32)
            )
            input_gate = jax.nn.sigmoid(
                jnp.dot(conv_low, input_blocks[number], preferred_element_type=F32)
            )
            param = -decay_param[pl.ds(number, 1), :]
            soft = jnp.maximum(param, 0.0) + jnp.log1p(jnp.exp(-jnp.abs(param)))
            log_decay = -DECAY_FACTOR * recur_gate * soft + ecol[...]
            decay = jnp.exp(log_decay)
            drive = jnp.sqrt(-jnp.tanh(log_decay) * (1.0 + decay * decay)) * input_gate * conv_out
            step = 1
            while step < rows:
                keep = places >= step
                drive = drive + decay * jnp.where(keep, pltpu.roll(drive, step, 0), 0.0)
                if step * 2 < rows:
                    decay = decay * jnp.where(keep, pltpu.roll(decay, step, 0), 1.0)
                step *= 2
            state = drive.astype(LOW)
            st[s, 0, :, here] = state[:half]
            st[s, 1, :, here] = state[half:]
        return carry

    lax.fori_loop(0, 4, recur, 0)

    products(0, 0, st, mix_w, MIX)
    products(0, 1, st, mix_w, MIX)
    pair_sums(0, 0)
    send_own(GU, 1)
    pair_sums(0, 1)
    products(0, 2, st, mix_w, MIX)
    line_sums(0, 0)
    pair_sums(0, 2)
    line_sums(0, 1)
    products(0, 3, st, mix_w, MIX)
    mix_done(0)
    pair_sums(0, 3)
    forward(GU, 0, 0)
    line_sums(0, 2)
    mix_done(1)
    forward(GU, 1, 0)
    line_sums(0, 3)
    mix_done(2)
    mix_done(3)

    norm_rows(mx, gain_two)
    gather_start(1)
    gather_first(1)
    wait_block(DOWN, fp)
    forward(GU, 0, 1)
    gather_second(1)
    forward(GU, 1, 1)
    gather_last(1)
    send_own(DOWN, 0)
    send_own(DOWN, 1)
    for p in range(1, 4):
        need(GU, p)

    unit_rows = units // block

    def unit_scales(scale):
        first = q * unit_rows
        return jnp.concatenate([scale[pl.ds(first + i, 1), :] for i in range(unit_rows)], 1)

    def hidden(s, carry):
        left = nbuf[s].reshape(rows, width)
        total = jnp.dot(left, gu_w[...].reshape(width, 2 * units), preferred_element_type=F32)
        gate = total[:, :units] * unit_scales(gate_scale)
        up = total[:, units:] * unit_scales(up_scale)
        value = (gate * jax.nn.sigmoid(gate) * up).astype(LOW)
        hid[s, 0] = value[:half]
        hid[s, 1] = value[half:]
        return carry

    lax.fori_loop(0, 4, hidden, 0)

    products(1, 0, hid, down_w, DOWN)
    products(1, 1, hid, down_w, DOWN)
    pair_sums(1, 0)
    pair_sums(1, 1)
    forward(DOWN, 0, 0)
    forward(DOWN, 0, 1)
    line_sums(1, 0)
    line_sums(1, 1)
    down_done(0)
    forward(DOWN, 1, 0)
    forward(DOWN, 1, 1)
    down_done(1)
    products(1, 2, hid, down_w, DOWN)
    pair_sums(1, 2)
    products(1, 3, hid, down_w, DOWN, (0,))
    line_sums(1, 2)
    pair_sums(1, 3, (0,))
    down_done(2)
    products(1, 3, hid, down_w, DOWN, (1,))
    line_sums(1, 3, (0,))
    pair_sums(1, 3, (1,))
    down_done(3, (0,))
    line_sums(1, 3, (1,))
    down_done(3, (1,))

    for p, blocks in ((0, (0, 1)), (1, (0, 1)), (2, (0, 1)), (3, (0,)), (3, (1,))):
        local = lax.div(planes[p], 2) == t

        @pl.when(local)
        def _():
            out_copy(p, blocks).wait_recv()

        @pl.when(jnp.logical_not(local))
        def _():
            out_copy(p, blocks).wait_send()

    result = pltpu.make_async_copy(ob, out, out_sem)
    result.start()
    for k in range(4):
        y_copy(k).wait_send()
        for j in range(2):
            for i, device in enumerate(near):
                block_copy(k, own_place(k, j), wo_send.at[k, j, i], device).wait_send()

        @pl.when(inner)
        def _():
            for far in range(2):
                for j in range(2):
                    forward_copy(k, far, j)[1].wait_send()

    for copy in ext_copies:
        copy.wait_send()
    result.wait()


def team_body(
    tokens,
    mixing_norm_gain,
    recurrent_input_weight,
    recurrent_input_scale,
    convolution_kernel_taps,
    recurrence_gate_weight_blocks,
    input_gate_weight_blocks,
    channel_decay_parameter,
    token_extra_log_decay,
    mixing_output_weight,
    mixing_output_scale,
    feedforward_norm_gain,
    feedforward_gate_weight,
    feedforward_gate_scale,
    feedforward_up_weight,
    feedforward_up_scale,
    feedforward_down_weight,
    feedforward_down_scale,
):
    rows, half_width = tokens.shape
    half, part = rows // 2, rows // 4
    width = half_width * 2
    depth = recurrent_input_weight.shape[0]
    chans = recurrent_input_weight.shape[1] // 4
    units = feedforward_gate_weight.shape[1] // 4
    cols = mixing_output_weight.shape[1]
    block = recurrence_gate_weight_blocks.shape[1]
    planes = width // depth
    any_spec = pl.BlockSpec(memory_space=pl.ANY)
    vmem_spec = pl.BlockSpec(memory_space=pltpu.VMEM)
    vmem = pltpu.VMEM
    dma = pltpu.SemaphoreType.DMA

    def row(vector):
        return vector.reshape(1, -1)

    def lines(vector):
        return vector.reshape(-1, block)

    out = pl.pallas_call(
        layer_kernel,
        out_shape=jax.ShapeDtypeStruct((2, half, half_width), LOW),
        in_specs=[any_spec] * 6 + [vmem_spec] * 12,
        out_specs=any_spec,
        scratch_shapes=[
            vmem((4, 2, half, width), LOW),
            vmem((planes, depth, chans), LOW),
            vmem((planes, chans, cols), LOW),
            vmem((planes, depth, 2 * units), LOW),
            vmem((planes, units, cols), LOW),
            vmem((2, depth, chans), F32),
            vmem((2, chans, cols), F32),
            vmem((2, 2, depth, units), F32),
            vmem((2, units, cols), F32),
            vmem((depth, chans), LOW),
            vmem((chans, cols), LOW),
            vmem((depth, 2 * units), LOW),
            vmem((units, cols), LOW),
            vmem((half, width), LOW),
            vmem((half, width), LOW),
            vmem((4, 2, half, chans), LOW),
            vmem((4, 2, half, units), LOW),
            vmem((rows, chans), LOW),
            vmem((4, 8, rows), F32),
            vmem((rows, block), F32),
            vmem((4, 4, half, 2 * cols), LOW),
            vmem((4, 2, 2, half, 2 * cols), LOW),
            vmem((2, 4, 4, half, 2 * cols), LOW),
            vmem((2, 4, 2, 2, part, 2 * cols), LOW),
            vmem((2, 4, 2, part, 2 * cols), LOW),
            vmem((4, half, 2 * cols), LOW),
            vmem((2, half, half_width), LOW),
            dma((11,)),
            dma,
            dma((4,)),
            dma((4, 2, 2)),
            dma((4, 2, 2)),
            dma((4, planes)),
            dma((2, 13)),
            dma((2, 13)),
            dma((2,)),
            dma((3,)),
            dma((3,)),
            dma((2, 4, 10)),
            dma((2, 4, 10)),
            dma((4, 2)),
            dma((4, 2)),
        ],
        compiler_params=pltpu.CompilerParams(
            collective_id=0, has_side_effects=True, vmem_limit_bytes=VMEM_BYTES
        ),
    )(
        tokens,
        recurrent_input_weight,
        mixing_output_weight,
        feedforward_gate_weight,
        feedforward_up_weight,
        feedforward_down_weight,
        row(mixing_norm_gain),
        lines(recurrent_input_scale),
        convolution_kernel_taps,
        recurrence_gate_weight_blocks,
        input_gate_weight_blocks,
        lines(channel_decay_parameter),
        lines(token_extra_log_decay),
        row(mixing_output_scale),
        row(feedforward_norm_gain),
        lines(feedforward_gate_scale),
        lines(feedforward_up_scale),
        row(feedforward_down_scale),
    )
    return out.reshape(rows, half_width)


VMEM_BYTES = 66_000_000


def team_fits(mesh):
    sizes = mesh.shape
    return sizes["rep"] == 2 and sizes["tp"] == 2 and sizes["fs"] == 8


def solution(mesh):
    placed = (
        P(("rep", "fs"), "tp"),
        P(),
        P("fs", "tp"),
        P("tp"),
        P(None, "tp"),
        P("tp", None, None),
        P("tp", None, None),
        P("tp"),
        P(("rep", "fs")),
        P("tp", "fs"),
        P("fs"),
        P(),
        P("fs", "tp"),
        P("tp"),
        P("fs", "tp"),
        P("tp"),
        P("tp", "fs"),
        P("fs"),
    )

    def body(*args):
        blocks, hidden, rows = args[5].shape[0], args[12].shape[1], args[0].shape[0]
        if not team_fits(mesh) or blocks % 4 or hidden % 512 or rows % 64:
            return plain_body(*args)
        return team_body(*args)

    return jax.shard_map(
        body, mesh=mesh, in_specs=placed, out_specs=P(("rep", "fs"), "tp"), check_vma=False
    )
```

```python
import jax
import jax.numpy as jnp
from jax import lax
from jax.experimental import pallas as pl
from jax.experimental.pallas import tpu as pltpu
from jax.sharding import PartitionSpec as P

EPS = 1e-06
DECAY_FACTOR = 8.0


def row_norm(rows, gain_vec):
    values = rows.astype(jnp.float32)
    inverse = lax.rsqrt(jnp.mean(values * values, axis=-1, keepdims=True) + EPS)
    return (values * inverse * gain_vec).astype(jnp.bfloat16)


def gather_normed(rows, gain_vec):
    whole_rows = lax.all_gather(rows, "tp", axis=1, tiled=True)
    return row_norm(whole_rows, gain_vec)


def share_sums(terms):
    return lax.psum_scatter(
        terms.astype(jnp.bfloat16), "tp", scatter_dimension=1, tiled=True
    ).astype(jnp.float32)


def combine_pairs(earlier, later):
    decay_one, value_one = earlier
    decay_two, value_two = later
    return (decay_one * decay_two, decay_two * value_one + value_two)


def add_one(left_rows, weight_piece):
    return jnp.dot(left_rows, weight_piece, preferred_element_type=jnp.float32)


def place_columns(left_rows, total_now, pieces, start_row):
    weight_piece, scale_piece = pieces
    product = jnp.dot(left_rows, weight_piece, preferred_element_type=jnp.float32) * scale_piece
    return lax.dynamic_update_slice_in_dim(total_now, product, start_row, 1)


def plain_body(
    tokens,
    mixing_norm_gain,
    recurrent_input_weight,
    recurrent_input_scale,
    convolution_kernel_taps,
    recurrence_gate_weight_blocks,
    input_gate_weight_blocks,
    channel_decay_parameter,
    token_extra_log_decay,
    mixing_output_weight,
    mixing_output_scale,
    feedforward_norm_gain,
    feedforward_gate_weight,
    feedforward_gate_scale,
    feedforward_up_weight,
    feedforward_up_scale,
    feedforward_down_weight,
    feedforward_down_scale,
):
    normed = gather_normed(tokens, mixing_norm_gain)
    seq_rows = normed.shape[0]
    model_width = normed.shape[1]
    width_dev = recurrent_input_weight.shape[1]
    rec_sum = add_one(
        normed,
        lax.all_gather(recurrent_input_weight.astype(jnp.bfloat16), "fs", axis=0, tiled=True),
    )
    rec_input = (rec_sum * recurrent_input_scale).astype(jnp.bfloat16)
    rec_f32 = rec_input.astype(jnp.float32)
    tap_count = convolution_kernel_taps.shape[0]
    padded = jnp.pad(rec_f32, ((tap_count - 1, 0), (0, 0)))
    conv_out = jnp.zeros((seq_rows, width_dev), jnp.float32)
    for tap_index in range(tap_count):
        conv_out = (
            conv_out + convolution_kernel_taps[tap_index] * padded[tap_index : tap_index + seq_rows]
        )
    block_count = recurrence_gate_weight_blocks.shape[0]
    block_size = recurrence_gate_weight_blocks.shape[1]
    blocks = conv_out.astype(jnp.bfloat16).reshape(seq_rows, block_count, block_size)
    recurrence_gate_values = jax.nn.sigmoid(
        jnp.einsum(
            "lni,nij->lnj",
            blocks,
            recurrence_gate_weight_blocks,
            preferred_element_type=jnp.float32,
        ).reshape(seq_rows, width_dev)
    )
    input_gate = jax.nn.sigmoid(
        jnp.einsum(
            "lni,nij->lnj", blocks, input_gate_weight_blocks, preferred_element_type=jnp.float32
        ).reshape(seq_rows, width_dev)
    )
    decay_logarithm = (
        -DECAY_FACTOR * recurrence_gate_values * jax.nn.softplus(-channel_decay_parameter)
        + token_extra_log_decay[:, None]
    )
    decay = jnp.exp(decay_logarithm)
    drive = jnp.sqrt(-jnp.expm1(2.0 * decay_logarithm)) * input_gate * conv_out
    _, state = lax.associative_scan(combine_pairs, (decay, drive), axis=0)
    state_low = state.astype(jnp.bfloat16)
    mix_terms = place_columns(
        state_low,
        jnp.zeros((seq_rows, model_width), jnp.float32),
        (
            lax.all_gather(mixing_output_weight.astype(jnp.bfloat16), "fs", axis=1, tiled=True),
            lax.all_gather(
                mixing_output_scale.reshape(1, -1).astype(jnp.bfloat16), "fs", axis=1, tiled=True
            ).astype(jnp.float32),
        ),
        jnp.int32(0),
    )
    mixed = (tokens.astype(jnp.float32) + share_sums(mix_terms)).astype(jnp.bfloat16)
    normed_ffn = gather_normed(mixed, feedforward_norm_gain)
    gate_sum = add_one(
        normed_ffn,
        lax.all_gather(feedforward_gate_weight.astype(jnp.bfloat16), "fs", axis=0, tiled=True),
    )
    up_sum = add_one(
        normed_ffn,
        lax.all_gather(feedforward_up_weight.astype(jnp.bfloat16), "fs", axis=0, tiled=True),
    )
    hidden = (
        jax.nn.silu(gate_sum * feedforward_gate_scale) * (up_sum * feedforward_up_scale)
    ).astype(jnp.bfloat16)
    down_terms = place_columns(
        hidden,
        jnp.zeros((seq_rows, model_width), jnp.float32),
        (
            lax.all_gather(feedforward_down_weight.astype(jnp.bfloat16), "fs", axis=1, tiled=True),
            lax.all_gather(
                feedforward_down_scale.reshape(1, -1).astype(jnp.bfloat16), "fs", axis=1, tiled=True
            ).astype(jnp.float32),
        ),
        jnp.int32(0),
    )
    return (mixed.astype(jnp.float32) + share_sums(down_terms)).astype(jnp.bfloat16)


REC, MIX, GU, DOWN = range(4)
PIECE_PLACE = {0: 0, 2: 1, 3: 2}
LOW = jnp.bfloat16
F32 = jnp.float32


def remote(src, dst, send_sem, recv_sem, device):
    return pltpu.make_async_remote_copy(
        src_ref=src,
        dst_ref=dst,
        send_sem=send_sem,
        recv_sem=recv_sem,
        device_id=device,
        device_id_type=pl.DeviceIdType.MESH,
    )


def layer_kernel(
    tokens,
    w_rec,
    w_mix,
    w_gate,
    w_up,
    w_down,
    gain_one,
    rec_scale,
    taps,
    w_recur,
    w_input,
    decay_param,
    extra,
    mix_scale,
    gain_two,
    gate_scale,
    up_scale,
    down_scale,
    out,
    nbuf,
    rec_w,
    mix_w,
    gu_w,
    down_w,
    f_rec,
    f_mix,
    f_gu,
    f_down,
    y_rec,
    y_mix,
    y_gu,
    y_down,
    tk,
    mx,
    st,
    hid,
    ri,
    ext,
    ecol,
    oth,
    kept,
    rt,
    r1,
    r2,
    oo,
    recur_blocks,
    input_blocks,
    load_sem,
    wl_send,
    wl_recv,
    wy_send,
    wo_send,
    wf_send,
    w_recv,
    g_send,
    g_recv,
    tt_sem,
    ex_send,
    ex_recv,
    m_send,
    m_recv,
    o_send,
    o_recv,
):
    rows, half_width = tokens.shape
    half, part = rows // 2, rows // 4
    width = half_width * 2
    chans = rec_w.shape[2]
    units = down_w.shape[1]
    cols = mix_w.shape[2]
    unit = cols // 2
    block = recur_blocks.shape[1]
    tap_count = taps.shape[0]

    r, f, t = lax.axis_index("rep"), lax.axis_index("fs"), lax.axis_index("tp")
    y, z = lax.rem(f, 2), lax.div(f, 2)
    fp = f + 1 - 2 * y
    q = r * 2 + y
    own, own_x, own_y, own_d = q, (1 - r) * 2 + y, r * 2 + 1 - y, (1 - r) * 2 + 1 - y
    x_dev, y_dev, t_dev = {"rep": 1 - r}, {"fs": fp}, {"tp": 1 - t}
    d_dev = {"rep": 1 - r, "fs": fp}
    inner = lax.div(z + 1, 2) == 1
    near = (1 + lax.rem(z, 2), lax.rem(2 + 3 * z, 5))
    near = tuple({"fs": plane * 2 + y} for plane in near)
    planes = (z, z + 1 - 2 * lax.rem(z, 2), z + 2 - 4 * lax.div(z, 2), 3 - z)
    mats = (rec_w, mix_w, gu_w, down_w)
    top, low = pl.ds(0, part), pl.ds(part, part)

    quarters = (q, r * 2 + 1 - y)
    loads = {}

    def load(name, number, src, dst):
        copy = pltpu.make_async_copy(src, dst, load_sem.at[number])
        copy.start()
        loads[name] = copy

    mine = pl.ds(pl.multiple_of(t * half, half), half)
    theirs = pl.ds(pl.multiple_of((1 - t) * half, half), half)
    side = pl.ds(pl.multiple_of(t * half_width, half_width), half_width)
    load("tok", 0, tokens.at[mine, :], tk.at[:, side])
    for i, piece in enumerate(quarters):
        at = pl.ds(pl.multiple_of(piece * chans, chans), chans)
        load(("rec", i), 1 + i, w_rec.at[:, at], f_rec.at[i])
    for i, piece in enumerate(quarters):
        at = pl.ds(pl.multiple_of(piece * chans, chans), chans)
        load(("mix", i), 3 + i, w_mix.at[at, :], f_mix.at[i])
    for i, piece in enumerate(quarters):
        at = pl.ds(pl.multiple_of(piece * units, units), units)
        load(("gate", i), 5 + i, w_gate.at[:, at], f_gu.at[i, 0])
        load(("up", i), 7 + i, w_up.at[:, at], f_gu.at[i, 1])
        load(("down", i), 9 + i, w_down.at[at, :], f_down.at[i])
    gate_blocks = pl.ds(q * (chans // block), chans // block)
    load("recur", 11, w_recur.at[gate_blocks], recur_blocks)
    load("input", 12, w_input.at[gate_blocks], input_blocks)

    barrier = pltpu.get_barrier_semaphore()
    peers = [x_dev, y_dev, t_dev, d_dev]
    peers += [{"fs": plane * 2 + y} for plane in planes[1:]]
    for device in peers:
        pl.semaphore_signal(barrier, inc=1, device_id=device, device_id_type=pl.DeviceIdType.MESH)

    token_swap = remote(tokens.at[theirs, :], tk.at[:, side], tt_sem.at[0], tt_sem.at[1], t_dev)

    def block_copy(k, place, send_sem, device):
        view = mats[k].at[place]
        return remote(view, view, send_sem, w_recv.at[k, place], device)

    def wait_block(k, place):
        block_copy(k, place, wo_send.at[0, 0, 0], y_dev).wait_recv()

    def own_place(k, j):
        return z * 2 + j if k == DOWN else (f if j == 0 else fp)

    def send_own(k, j):
        if j == 1 and k != DOWN:
            wait_block(k, fp)
        for i in range(2):
            send_one(k, j, i)

    def send_one(k, j, i):
        block_copy(k, own_place(k, j), wo_send.at[k, j, i], near[i]).start()

    y_bufs = (y_rec, y_mix, y_gu, y_down)

    def y_copy(k):
        return remote(y_bufs[k], mats[k].at[f], wy_send.at[k], w_recv.at[k, f], y_dev)

    def forward_copy(k, far, j):
        plane = 3 * (2 - z) if far else 3 - z
        place = plane * 2 + (j if k == DOWN else (y if j == 0 else 1 - y))
        edge = 3 * (z - 1)
        return place, block_copy(k, place, wf_send.at[k, far, j], {"fs": edge * 2 + y})

    def forward_copies(k, far, j):
        place, copy = forward_copy(k, far, j)
        if k == DOWN and far and j:
            return place, last_copies(place, {"fs": 3 * (z - 1) * 2 + y})
        return place, [copy]

    def forward(k, far, j):
        @pl.when(inner)
        def _():
            place, copies = forward_copies(k, far, j)
            wait_block(k, place)
            for copy in copies:
                copy.start()

    def last_copies(place, device):
        view = down_w.at[place]
        return [
            remote(
                view.at[:, pl.ds(i * unit, unit)],
                view.at[:, pl.ds(i * unit, unit)],
                wl_send.at[i],
                wl_recv.at[i],
                device,
            )
            for i in range(2)
        ]

    def need(k, p, piece=(0, 4)):
        def wait():
            for j in range(2):
                if k == DOWN and p == 3 and j == 1:
                    for i, copy in enumerate(last_copies(planes[p] * 2 + j, y_dev)):
                        if piece[0] <= 2 + i < sum(piece):
                            copy.wait_recv()
                elif piece[0] <= 2 * j < sum(piece):
                    wait_block(k, planes[p] * 2 + j)

        if p == 1:
            wait()
        elif p > 1:
            pl.when(jnp.logical_not(inner))(wait)

    def norm_rows(src, gain):
        def step(i, carry):
            at = pl.ds(pl.multiple_of(i * 16, 16), 16)
            v = src[at, :].astype(F32)
            inverse = lax.rsqrt(jnp.mean(v * v, axis=-1, keepdims=True) + EPS)
            nbuf[own, t, at, :] = (v * inverse * gain[...]).astype(LOW)
            return carry

        lax.fori_loop(0, half // 16, step, 0)

    def rows_copy(phase, role):
        seq, at, device = (
            (own, top, x_dev),
            (own, low, x_dev),
            (own, top, y_dev),
            (own, low, y_dev),
            (own_y, top, x_dev),
            (own_x, low, y_dev),
            (own, pl.ds(0, half), t_dev),
            (own_x, top, t_dev),
            (own_x, low, t_dev),
            (own_y, top, t_dev),
            (own_y, low, t_dev),
            (own_d, top, t_dev),
            (own_d, low, t_dev),
        )[role]
        view = nbuf.at[seq, t, at, :]
        return remote(view, view, g_send.at[role], g_recv.at[role], device)

    def rows_wait(phase, role):
        seq, side_at, at = (
            (own_x, t, top),
            (own_x, t, low),
            (own_y, t, top),
            (own_y, t, low),
            (own_d, t, top),
            (own_d, t, low),
            (own, 1 - t, pl.ds(0, half)),
            (own_x, 1 - t, top),
            (own_x, 1 - t, low),
            (own_y, 1 - t, top),
            (own_y, 1 - t, low),
            (own_d, 1 - t, top),
            (own_d, 1 - t, low),
        )[role]
        view = nbuf.at[seq, side_at, at, :]
        remote(view, view, g_send.at[role], g_recv.at[role], t_dev).wait_recv()

    def gather_start(phase):
        for role in (1, 2, 0, 3, 6):
            rows_copy(phase, role).start()

    def gather_first(phase):
        rows_wait(phase, 2)
        rows_copy(phase, 4).start()
        rows_wait(phase, 1)
        rows_copy(phase, 5).start()
        rows_copy(phase, 9).start()
        rows_copy(phase, 8).start()

    def gather_second(phase):
        rows_wait(phase, 0)
        rows_copy(phase, 7).start()
        rows_wait(phase, 3)
        rows_copy(phase, 10).start()

    def gather_last(phase):
        rows_wait(phase, 4)
        rows_copy(phase, 11).start()
        rows_wait(phase, 5)
        rows_copy(phase, 12).start()
        for role in range(6, 13):
            rows_wait(phase, role)
        for role in range(13):
            rows_copy(phase, role).wait_send()

    def products(phase, p, left, weights, k, piece=(0, 4)):
        need(k, p, piece)
        first, size = planes[p] * 2, min(piece[1], 2)

        def product(side, start):
            rows_now = left[:, side].reshape(4 * half, left.shape[-1])
            column = start % 2 * unit
            weight = weights[first + start // 2, :, column : column + size * unit]
            value = jnp.dot(rows_now, weight, preferred_element_type=F32)
            return value.astype(LOW).reshape(4, half, size * unit)

        starts = range(piece[0], sum(piece), size)
        for start in starts:
            oth[p, :, :, start * unit : (start + size) * unit] = product(1 - t, start)
        sum_copies(phase, p, 0, piece).start()
        for start in starts:
            value = product(t, start).reshape(2, 2, half, size * unit)
            kept[p, :, :, :, start * unit : (start + size) * unit] = value

    def span_of(piece):
        return pl.ds(piece[0] * unit, piece[1] * unit)

    def sum_copies(phase, p, number, piece):
        at = span_of(piece)
        src, dst, device = (
            (oth.at[p, :, :, at], rt.at[phase, p, :, :, at], t_dev),
            (kept.at[p, 1 - r, :, top, at], r1.at[phase, p, 0, :, :, at], x_dev),
            (kept.at[p, :, 1 - y, low, at], r1.at[phase, p, 1, :, :, at], y_dev),
            (kept.at[p, r, 1 - y, top, at], r2.at[phase, p, 0, :, at], y_dev),
            (kept.at[p, 1 - r, y, low, at], r2.at[phase, p, 1, :, at], x_dev),
        )[number]
        send, land = p + PIECE_PLACE[piece[0]], p + PIECE_PLACE[piece[0]] + 4 * phase
        return remote(src, dst, m_send.at[send, number], m_recv.at[land, number], device)

    def pair_sums(phase, p, piece=(0, 4)):
        sum_copies(phase, p, 0, piece).wait_recv()
        at = span_of(piece)

        def step(s, carry):
            a, b = lax.div(s, 2), lax.rem(s, 2)
            value = kept[p, a, b, :, at].astype(F32) + rt[phase, p, s, :, at].astype(F32)
            kept[p, a, b, :, at] = value.astype(LOW)
            return carry

        lax.fori_loop(0, 4, step, 0)
        sum_copies(phase, p, 1, piece).start()
        sum_copies(phase, p, 2, piece).start()

    def line_sums(phase, p, piece=(0, 4)):
        at = span_of(piece)
        sum_copies(phase, p, 1, piece).wait_recv()
        for i in range(2):
            value = kept[p, r, i, top, at].astype(F32) + r1[phase, p, 0, i, :, at].astype(F32)
            kept[p, r, i, top, at] = value.astype(LOW)
        sum_copies(phase, p, 3, piece).start()
        sum_copies(phase, p, 2, piece).wait_recv()
        for i in range(2):
            value = kept[p, i, y, low, at].astype(F32) + r1[phase, p, 1, i, :, at].astype(F32)
            kept[p, i, y, low, at] = value.astype(LOW)
        sum_copies(phase, p, 4, piece).start()

    def columns_of(plane, piece):
        start = pl.multiple_of((plane * 4 + piece[0]) * unit, unit)
        return pl.ds(start, piece[1] * unit)

    def last_sums(phase, p, base, piece):
        at, inside = columns_of(planes[p], piece), span_of(piece)
        values = []
        for i, number in enumerate((3, 4)):
            span = slice(i * part, (i + 1) * part)
            sum_copies(phase, p, number, piece).wait_recv()
            value = kept[p, r, y, span, inside].astype(F32) + r2[phase, p, i, :, inside].astype(F32)
            values.append((base[span, at].astype(F32) + value).astype(LOW))
        for number in range(5):
            sum_copies(phase, p, number, piece).wait_send()
        return at, values

    def mix_done(p):
        at, values = last_sums(0, p, tk, (0, 4))
        for i, value in enumerate(values):
            mx[i * part : (i + 1) * part, at] = value

    def out_copy(p, piece):
        at = columns_of(lax.rem(planes[p], 2), piece)
        src = oo.at[p, :, span_of(piece)]
        return remote(src, out.at[t, :, at], o_send.at[p + PIECE_PLACE[piece[0]]], o_recv.at[p + PIECE_PLACE[piece[0]]], t_dev)

    def down_done(p, piece=(0, 4)):
        _, values = last_sums(1, p, mx, piece)
        local = lax.div(planes[p], 2) == t
        at = columns_of(lax.rem(planes[p], 2), piece)

        @pl.when(local)
        def _():
            for i, value in enumerate(values):
                out[t, i * part : (i + 1) * part, at] = value

        @pl.when(jnp.logical_not(local))
        def _():
            for i, value in enumerate(values):
                oo[p, i * part : (i + 1) * part, span_of(piece)] = value
            out_copy(p, piece).start()

    for i in range(2):
        loads["rec", i].wait()
    y_rec[...] = f_rec[1].astype(LOW)
    rec_w[f] = f_rec[0].astype(LOW)
    pl.semaphore_wait(barrier, len(peers))
    token_swap.start()
    y_copy(REC).start()
    send_own(REC, 0)
    loads["tok"].wait()
    token_swap.wait()
    norm_rows(tk, gain_one)
    gather_start(0)

    for i in range(2):
        loads["mix", i].wait()
    y_mix[...] = (f_mix[1] * mix_scale[...]).astype(LOW)
    mix_w[f] = (f_mix[0] * mix_scale[...]).astype(LOW)


    @pl.when(inner)
    def _():
        send_one(MIX, 0, 1)

    send_own(REC, 1)
    for i in range(extra.shape[0]):
        lanes = slice(i * block, (i + 1) * block)
        ext[own, :, lanes] = jnp.broadcast_to(extra[i : i + 1, :], (ext.shape[1], block))
    ext_copies = [
        remote(ext.at[own], ext.at[own], ex_send.at[i], ex_recv.at[i], device)
        for i, device in enumerate((x_dev, y_dev, d_dev))
    ]
    for copy in ext_copies:
        copy.start()
    for i in range(2):
        for name in ("gate", "up", "down"):
            loads[name, i].wait()
    for i in range(2):
        y_gu[:, i * units : (i + 1) * units] = f_gu[1, i].astype(LOW)
        gu_w[f, :, i * units : (i + 1) * units] = f_gu[0, i].astype(LOW)
    y_down[...] = (f_down[1] * down_scale[...]).astype(LOW)
    down_w[f] = (f_down[0] * down_scale[...]).astype(LOW)

    send_one(MIX, 0, 0)

    @pl.when(jnp.logical_not(inner))
    def _():
        send_one(MIX, 0, 1)

    forward(REC, 0, 0)
    forward(REC, 1, 0)
    gather_first(0)
    y_copy(MIX).start()
    y_copy(GU).start()
    y_copy(DOWN).start()
    forward(REC, 0, 1)
    forward(REC, 1, 1)
    gather_second(0)
    forward(MIX, 0, 0)
    forward(MIX, 1, 0)
    gather_last(0)
    for i, seq in enumerate((own_x, own_y, own_d)):
        remote(ext.at[seq], ext.at[seq], ex_send.at[i], ex_recv.at[i], t_dev).wait_recv()
    for p in range(1, 4):
        need(REC, p)
    loads["recur"].wait()
    loads["input"].wait()

    at_chans = pl.multiple_of(q * chans, chans)

    def recur(s, carry):
        @pl.when(s == 1)
        def _():
            send_own(MIX, 1)
            send_own(GU, 0)

        @pl.when(s == 2)
        def _():
            forward(MIX, 0, 1)

        @pl.when(s == 3)
        def _():
            forward(MIX, 1, 1)

        left = nbuf[s].reshape(rows, width)
        total = jnp.dot(left, rec_w[...].reshape(width, chans), preferred_element_type=F32)
        for b in range(chans // block):
            here = slice(b * block, (b + 1) * block)
            number = q * (chans // block) + b
            ri[:, here] = (total[:, here] * rec_scale[pl.ds(number, 1), :]).astype(LOW)
        ecol[...] = jnp.broadcast_to(ext[s, 0:1, :], (block, rows)).T
        for b in range(chans // block):
            here = slice(b * block, (b + 1) * block)
            lanes = pl.ds(pl.multiple_of(at_chans + b * block, block), block)
            number = q * (chans // block) + b
            values = ri[:, here].astype(F32)
            places = lax.broadcasted_iota(jnp.int32, values.shape, 0)
            conv_out = taps[tap_count - 1 : tap_count, lanes] * values
            for back in range(1, tap_count):
                moved = jnp.where(places >= back, pltpu.roll(values, back, 0), 0.0)
                tap = tap_count - 1 - back
                conv_out = conv_out + taps[tap : tap + 1, lanes] * moved
            conv_low = conv_out.astype(LOW)
            recur_gate = jax.nn.sigmoid(
                jnp.dot(conv_low, recur_blocks[b], preferred_element_type=F32)
            )
            input_gate = jax.nn.sigmoid(
                jnp.dot(conv_low, input_blocks[b], preferred_element_type=F32)
            )
            param = -decay_param[pl.ds(number, 1), :]
            soft = jnp.maximum(param, 0.0) + jnp.log1p(jnp.exp(-jnp.abs(param)))
            log_decay = -DECAY_FACTOR * recur_gate * soft + ecol[...]
            decay = jnp.exp(log_decay)
            drive = jnp.sqrt(-jnp.tanh(log_decay) * (1.0 + decay * decay)) * input_gate * conv_out
            step = 1
            while step < rows:
                keep = places >= step
                drive = drive + decay * jnp.where(keep, pltpu.roll(drive, step, 0), 0.0)
                if step * 2 < rows:
                    decay = decay * jnp.where(keep, pltpu.roll(decay, step, 0), 1.0)
                step *= 2
            state = drive.astype(LOW)
            st[s, 0, :, here] = state[:half]
            st[s, 1, :, here] = state[half:]
        return carry

    lax.fori_loop(0, 4, recur, 0)

    products(0, 0, st, mix_w, MIX)
    products(0, 1, st, mix_w, MIX)
    pair_sums(0, 0)
    send_own(GU, 1)
    pair_sums(0, 1)
    products(0, 2, st, mix_w, MIX)
    line_sums(0, 0)
    pair_sums(0, 2)
    line_sums(0, 1)
    products(0, 3, st, mix_w, MIX)
    mix_done(0)
    pair_sums(0, 3)
    forward(GU, 0, 0)
    line_sums(0, 2)
    mix_done(1)
    forward(GU, 1, 0)
    line_sums(0, 3)
    mix_done(2)
    mix_done(3)

    norm_rows(mx, gain_two)
    gather_start(1)
    gather_first(1)
    wait_block(DOWN, fp)
    forward(GU, 0, 1)
    gather_second(1)
    forward(GU, 1, 1)
    gather_last(1)
    send_own(DOWN, 0)
    send_own(DOWN, 1)
    for p in range(1, 4):
        need(GU, p)

    unit_rows = units // block

    def unit_scales(scale):
        first = q * unit_rows
        return jnp.concatenate([scale[pl.ds(first + i, 1), :] for i in range(unit_rows)], 1)

    def hidden(s, carry):
        left = nbuf[s].reshape(rows, width)
        total = jnp.dot(left, gu_w[...].reshape(width, 2 * units), preferred_element_type=F32)
        gate = total[:, :units] * unit_scales(gate_scale)
        up = total[:, units:] * unit_scales(up_scale)
        value = (gate * jax.nn.sigmoid(gate) * up).astype(LOW)
        hid[s, 0] = value[:half]
        hid[s, 1] = value[half:]
        return carry

    lax.fori_loop(0, 4, hidden, 0)

    last_pieces = ((0, 2), (2, 1), (3, 1))
    products(1, 0, hid, down_w, DOWN)
    pair_sums(1, 0)
    products(1, 1, hid, down_w, DOWN)
    forward(DOWN, 0, 0)
    line_sums(1, 0)
    pair_sums(1, 1)
    forward(DOWN, 0, 1)
    down_done(0)
    forward(DOWN, 1, 0)
    line_sums(1, 1)
    forward(DOWN, 1, 1)
    down_done(1)
    products(1, 2, hid, down_w, DOWN)
    pair_sums(1, 2)
    products(1, 3, hid, down_w, DOWN, last_pieces[0])
    line_sums(1, 2)
    pair_sums(1, 3, last_pieces[0])
    products(1, 3, hid, down_w, DOWN, last_pieces[1])
    down_done(2)
    pair_sums(1, 3, last_pieces[1])
    line_sums(1, 3, last_pieces[0])
    products(1, 3, hid, down_w, DOWN, last_pieces[2])
    pair_sums(1, 3, last_pieces[2])
    line_sums(1, 3, last_pieces[1])
    down_done(3, last_pieces[0])
    line_sums(1, 3, last_pieces[2])
    down_done(3, last_pieces[1])
    down_done(3, last_pieces[2])

    for p, piece in ((0, (0, 4)), (1, (0, 4)), (2, (0, 4)), (3, (0, 2)), (3, (2, 1)), (3, (3, 1))):
        local = lax.div(planes[p], 2) == t

        @pl.when(local)
        def _():
            out_copy(p, piece).wait_recv()

        @pl.when(jnp.logical_not(local))
        def _():
            out_copy(p, piece).wait_send()

    for k in range(4):
        y_copy(k).wait_send()
        for j in range(2):
            for i, device in enumerate(near):
                block_copy(k, own_place(k, j), wo_send.at[k, j, i], device).wait_send()

        @pl.when(inner)
        def _():
            for far in range(2):
                for j in range(2):
                    for copy in forward_copies(k, far, j)[1]:
                        copy.wait_send()

    for copy in ext_copies:
        copy.wait_send()


def team_body(
    tokens,
    mixing_norm_gain,
    recurrent_input_weight,
    recurrent_input_scale,
    convolution_kernel_taps,
    recurrence_gate_weight_blocks,
    input_gate_weight_blocks,
    channel_decay_parameter,
    token_extra_log_decay,
    mixing_output_weight,
    mixing_output_scale,
    feedforward_norm_gain,
    feedforward_gate_weight,
    feedforward_gate_scale,
    feedforward_up_weight,
    feedforward_up_scale,
    feedforward_down_weight,
    feedforward_down_scale,
):
    rows, half_width = tokens.shape
    half, part = rows // 2, rows // 4
    width = half_width * 2
    depth = recurrent_input_weight.shape[0]
    chans = recurrent_input_weight.shape[1] // 4
    units = feedforward_gate_weight.shape[1] // 4
    cols = mixing_output_weight.shape[1]
    block = recurrence_gate_weight_blocks.shape[1]
    planes = width // depth
    any_spec = pl.BlockSpec(memory_space=pl.ANY)
    vmem_spec = pl.BlockSpec(memory_space=pltpu.VMEM)
    vmem = pltpu.VMEM
    dma = pltpu.SemaphoreType.DMA

    def row(vector):
        return vector.reshape(1, -1)

    def lines(vector):
        return vector.reshape(-1, block)

    out = pl.pallas_call(
        layer_kernel,
        out_shape=vmem((2, half, half_width), LOW),
        in_specs=[any_spec] * 6 + [vmem_spec] * 3 + [any_spec] * 2 + [vmem_spec] * 7,
        out_specs=vmem_spec,
        scratch_shapes=[
            vmem((4, 2, half, width), LOW),
            vmem((planes, depth, chans), LOW),
            vmem((planes, chans, cols), LOW),
            vmem((planes, depth, 2 * units), LOW),
            vmem((planes, units, cols), LOW),
            vmem((2, depth, chans), F32),
            vmem((2, chans, cols), F32),
            vmem((2, 2, depth, units), F32),
            vmem((2, units, cols), F32),
            vmem((depth, chans), LOW),
            vmem((chans, cols), LOW),
            vmem((depth, 2 * units), LOW),
            vmem((units, cols), LOW),
            vmem((half, width), LOW),
            vmem((half, width), LOW),
            vmem((4, 2, half, chans), LOW),
            vmem((4, 2, half, units), LOW),
            vmem((rows, chans), LOW),
            vmem((4, 8, rows), F32),
            vmem((rows, block), F32),
            vmem((4, 4, half, 2 * cols), LOW),
            vmem((4, 2, 2, half, 2 * cols), LOW),
            vmem((2, 4, 4, half, 2 * cols), LOW),
            vmem((2, 4, 2, 2, part, 2 * cols), LOW),
            vmem((2, 4, 2, part, 2 * cols), LOW),
            vmem((4, half, 2 * cols), LOW),
            vmem((chans // block, block, block), LOW),
            vmem((chans // block, block, block), LOW),
            dma((13,)),
            dma((2,)),
            dma((2,)),
            dma((4,)),
            dma((4, 2, 2)),
            dma((4, 2, 2)),
            dma((4, planes)),
            dma((13,)),
            dma((13,)),
            dma((2,)),
            dma((3,)),
            dma((3,)),
            dma((6, 5)),
            dma((10, 5)),
            dma((6,)),
            dma((6,)),
        ],
        compiler_params=pltpu.CompilerParams(
            collective_id=0, has_side_effects=True, vmem_limit_bytes=VMEM_BYTES
        ),
    )(
        tokens,
        recurrent_input_weight,
        mixing_output_weight,
        feedforward_gate_weight,
        feedforward_up_weight,
        feedforward_down_weight,
        row(mixing_norm_gain),
        lines(recurrent_input_scale),
        convolution_kernel_taps,
        recurrence_gate_weight_blocks,
        input_gate_weight_blocks,
        lines(channel_decay_parameter),
        lines(token_extra_log_decay),
        row(mixing_output_scale),
        row(feedforward_norm_gain),
        lines(feedforward_gate_scale),
        lines(feedforward_up_scale),
        row(feedforward_down_scale),
    )
    return out.reshape(rows, half_width)


VMEM_BYTES = 60_000_000


def team_fits(mesh):
    sizes = mesh.shape
    return sizes["rep"] == 2 and sizes["tp"] == 2 and sizes["fs"] == 8


def solution(mesh):
    placed = (
        P(("rep", "fs"), "tp"),
        P(),
        P("fs", "tp"),
        P("tp"),
        P(None, "tp"),
        P("tp", None, None),
        P("tp", None, None),
        P("tp"),
        P(("rep", "fs")),
        P("tp", "fs"),
        P("fs"),
        P(),
        P("fs", "tp"),
        P("tp"),
        P("fs", "tp"),
        P("tp"),
        P("tp", "fs"),
        P("fs"),
    )

    def body(*args):
        blocks, hidden, rows = args[5].shape[0], args[12].shape[1], args[0].shape[0]
        if not team_fits(mesh) or blocks % 4 or hidden % 512 or rows % 64 or args[9].shape[1] % 256:
            return plain_body(*args)
        return team_body(*args)

    return jax.shard_map(
        body, mesh=mesh, in_specs=placed, out_specs=P(("rep", "fs"), "tp"), check_vma=False
    )
```

```python
import jax
import jax.numpy as jnp
from jax import lax
from jax.experimental import pallas as pl
from jax.experimental.pallas import tpu as pltpu
from jax.sharding import PartitionSpec as P

EPS = 1e-06
DECAY_FACTOR = 8.0


def row_norm(rows, gain_vec):
    values = rows.astype(jnp.float32)
    inverse = lax.rsqrt(jnp.mean(values * values, axis=-1, keepdims=True) + EPS)
    return (values * inverse * gain_vec).astype(jnp.bfloat16)


def gather_normed(rows, gain_vec):
    whole_rows = lax.all_gather(rows, "tp", axis=1, tiled=True)
    return row_norm(whole_rows, gain_vec)


def share_sums(terms):
    return lax.psum_scatter(
        terms.astype(jnp.bfloat16), "tp", scatter_dimension=1, tiled=True
    ).astype(jnp.float32)


def combine_pairs(earlier, later):
    decay_one, value_one = earlier
    decay_two, value_two = later
    return (decay_one * decay_two, decay_two * value_one + value_two)


def add_one(left_rows, weight_piece):
    return jnp.dot(left_rows, weight_piece, preferred_element_type=jnp.float32)


def place_columns(left_rows, total_now, pieces, start_row):
    weight_piece, scale_piece = pieces
    product = jnp.dot(left_rows, weight_piece, preferred_element_type=jnp.float32) * scale_piece
    return lax.dynamic_update_slice_in_dim(total_now, product, start_row, 1)


def plain_body(
    tokens,
    mixing_norm_gain,
    recurrent_input_weight,
    recurrent_input_scale,
    convolution_kernel_taps,
    recurrence_gate_weight_blocks,
    input_gate_weight_blocks,
    channel_decay_parameter,
    token_extra_log_decay,
    mixing_output_weight,
    mixing_output_scale,
    feedforward_norm_gain,
    feedforward_gate_weight,
    feedforward_gate_scale,
    feedforward_up_weight,
    feedforward_up_scale,
    feedforward_down_weight,
    feedforward_down_scale,
):
    normed = gather_normed(tokens, mixing_norm_gain)
    seq_rows = normed.shape[0]
    model_width = normed.shape[1]
    width_dev = recurrent_input_weight.shape[1]
    rec_sum = add_one(
        normed,
        lax.all_gather(recurrent_input_weight.astype(jnp.bfloat16), "fs", axis=0, tiled=True),
    )
    rec_input = (rec_sum * recurrent_input_scale).astype(jnp.bfloat16)
    rec_f32 = rec_input.astype(jnp.float32)
    tap_count = convolution_kernel_taps.shape[0]
    padded = jnp.pad(rec_f32, ((tap_count - 1, 0), (0, 0)))
    conv_out = jnp.zeros((seq_rows, width_dev), jnp.float32)
    for tap_index in range(tap_count):
        conv_out = (
            conv_out + convolution_kernel_taps[tap_index] * padded[tap_index : tap_index + seq_rows]
        )
    block_count = recurrence_gate_weight_blocks.shape[0]
    block_size = recurrence_gate_weight_blocks.shape[1]
    blocks = conv_out.astype(jnp.bfloat16).reshape(seq_rows, block_count, block_size)
    recurrence_gate_values = jax.nn.sigmoid(
        jnp.einsum(
            "lni,nij->lnj",
            blocks,
            recurrence_gate_weight_blocks,
            preferred_element_type=jnp.float32,
        ).reshape(seq_rows, width_dev)
    )
    input_gate = jax.nn.sigmoid(
        jnp.einsum(
            "lni,nij->lnj", blocks, input_gate_weight_blocks, preferred_element_type=jnp.float32
        ).reshape(seq_rows, width_dev)
    )
    decay_logarithm = (
        -DECAY_FACTOR * recurrence_gate_values * jax.nn.softplus(-channel_decay_parameter)
        + token_extra_log_decay[:, None]
    )
    decay = jnp.exp(decay_logarithm)
    drive = jnp.sqrt(-jnp.expm1(2.0 * decay_logarithm)) * input_gate * conv_out
    _, state = lax.associative_scan(combine_pairs, (decay, drive), axis=0)
    state_low = state.astype(jnp.bfloat16)
    mix_terms = place_columns(
        state_low,
        jnp.zeros((seq_rows, model_width), jnp.float32),
        (
            lax.all_gather(mixing_output_weight.astype(jnp.bfloat16), "fs", axis=1, tiled=True),
            lax.all_gather(
                mixing_output_scale.reshape(1, -1).astype(jnp.bfloat16), "fs", axis=1, tiled=True
            ).astype(jnp.float32),
        ),
        jnp.int32(0),
    )
    mixed = (tokens.astype(jnp.float32) + share_sums(mix_terms)).astype(jnp.bfloat16)
    normed_ffn = gather_normed(mixed, feedforward_norm_gain)
    gate_sum = add_one(
        normed_ffn,
        lax.all_gather(feedforward_gate_weight.astype(jnp.bfloat16), "fs", axis=0, tiled=True),
    )
    up_sum = add_one(
        normed_ffn,
        lax.all_gather(feedforward_up_weight.astype(jnp.bfloat16), "fs", axis=0, tiled=True),
    )
    hidden = (
        jax.nn.silu(gate_sum * feedforward_gate_scale) * (up_sum * feedforward_up_scale)
    ).astype(jnp.bfloat16)
    down_terms = place_columns(
        hidden,
        jnp.zeros((seq_rows, model_width), jnp.float32),
        (
            lax.all_gather(feedforward_down_weight.astype(jnp.bfloat16), "fs", axis=1, tiled=True),
            lax.all_gather(
                feedforward_down_scale.reshape(1, -1).astype(jnp.bfloat16), "fs", axis=1, tiled=True
            ).astype(jnp.float32),
        ),
        jnp.int32(0),
    )
    return (mixed.astype(jnp.float32) + share_sums(down_terms)).astype(jnp.bfloat16)


REC, MIX, GU, DOWN = range(4)
PIECES = ((0, 0), (1, 0), (2, 0), (2, 2), (3, 0), (3, 2), (3, 3))
LOW = jnp.bfloat16
F32 = jnp.float32


def remote(src, dst, send_sem, recv_sem, device):
    return pltpu.make_async_remote_copy(
        src_ref=src,
        dst_ref=dst,
        send_sem=send_sem,
        recv_sem=recv_sem,
        device_id=device,
        device_id_type=pl.DeviceIdType.MESH,
    )


def layer_kernel(
    tokens,
    w_rec,
    w_mix,
    w_gate,
    w_up,
    w_down,
    gain_one,
    rec_scale,
    taps,
    w_recur,
    w_input,
    decay_param,
    extra,
    mix_scale,
    gain_two,
    gate_scale,
    up_scale,
    down_scale,
    out,
    nbuf,
    rec_w,
    mix_w,
    gu_w,
    down_w,
    f_rec,
    f_mix,
    f_gu,
    f_down,
    y_rec,
    y_mix,
    y_gu,
    y_down,
    tk,
    mx,
    st,
    hid,
    ri,
    ext,
    ecol,
    oth,
    kept,
    rt,
    r1,
    r2,
    rd,
    oo,
    recur_blocks,
    input_blocks,
    load_sem,
    wl_send,
    wl_recv,
    wy_send,
    wo_send,
    wf_send,
    w_recv,
    g_send,
    g_recv,
    tt_sem,
    ex_send,
    ex_recv,
    m_send,
    m_recv,
    o_send,
    o_recv,
):
    rows, half_width = tokens.shape
    half, part = rows // 2, rows // 4
    width = half_width * 2
    chans = rec_w.shape[2]
    units = down_w.shape[1]
    cols = mix_w.shape[2]
    unit = cols // 2
    block = recur_blocks.shape[1]
    tap_count = taps.shape[0]

    r, f, t = lax.axis_index("rep"), lax.axis_index("fs"), lax.axis_index("tp")
    y, z = lax.rem(f, 2), lax.div(f, 2)
    fp = f + 1 - 2 * y
    q = r * 2 + y
    own, own_x, own_y, own_d = q, (1 - r) * 2 + y, r * 2 + 1 - y, (1 - r) * 2 + 1 - y
    x_dev, y_dev, t_dev = {"rep": 1 - r}, {"fs": fp}, {"tp": 1 - t}
    d_dev = {"rep": 1 - r, "fs": fp}
    inner = lax.div(z + 1, 2) == 1
    near = (1 + lax.rem(z, 2), lax.rem(2 + 3 * z, 5))
    near = tuple({"fs": plane * 2 + y} for plane in near)
    planes = (z, z + 1 - 2 * lax.rem(z, 2), z + 2 - 4 * lax.div(z, 2), 3 - z)
    mats = (rec_w, mix_w, gu_w, down_w)
    top, low = pl.ds(0, part), pl.ds(part, part)

    quarters = (q, r * 2 + 1 - y)
    loads = {}

    def load(name, number, src, dst):
        copy = pltpu.make_async_copy(src, dst, load_sem.at[number])
        copy.start()
        loads[name] = copy

    mine = pl.ds(pl.multiple_of(t * half, half), half)
    theirs = pl.ds(pl.multiple_of((1 - t) * half, half), half)
    side = pl.ds(pl.multiple_of(t * half_width, half_width), half_width)
    load("tok", 0, tokens.at[mine, :], tk.at[:, side])
    for i, piece in enumerate(quarters):
        at = pl.ds(pl.multiple_of(piece * chans, chans), chans)
        load(("rec", i), 1 + i, w_rec.at[:, at], f_rec.at[i])
    for i, piece in enumerate(quarters):
        at = pl.ds(pl.multiple_of(piece * chans, chans), chans)
        load(("mix", i), 3 + i, w_mix.at[at, :], f_mix.at[i])
    for i, piece in enumerate(quarters):
        at = pl.ds(pl.multiple_of(piece * units, units), units)
        load(("gate", i), 5 + i, w_gate.at[:, at], f_gu.at[i, 0])
        load(("up", i), 7 + i, w_up.at[:, at], f_gu.at[i, 1])
        load(("down", i), 9 + i, w_down.at[at, :], f_down.at[i])
    gate_blocks = pl.ds(q * (chans // block), chans // block)
    load("recur", 11, w_recur.at[gate_blocks], recur_blocks)
    load("input", 12, w_input.at[gate_blocks], input_blocks)

    barrier = pltpu.get_barrier_semaphore()
    peers = [x_dev, y_dev, t_dev, d_dev]
    peers += [{"fs": plane * 2 + y} for plane in planes[1:]]
    for device in peers:
        pl.semaphore_signal(barrier, inc=1, device_id=device, device_id_type=pl.DeviceIdType.MESH)

    token_swap = remote(tokens.at[theirs, :], tk.at[:, side], tt_sem.at[0], tt_sem.at[1], t_dev)

    def block_copy(k, place, send_sem, device):
        view = mats[k].at[place]
        return remote(view, view, send_sem, w_recv.at[k, place], device)

    def wait_block(k, place):
        block_copy(k, place, wo_send.at[0, 0, 0], y_dev).wait_recv()

    def own_place(k, j):
        return z * 2 + j if k == DOWN else (f if j == 0 else fp)

    def send_own(k, j):
        if j == 1 and k != DOWN:
            wait_block(k, fp)
        for i in range(2):
            send_one(k, j, i)

    def send_one(k, j, i):
        block_copy(k, own_place(k, j), wo_send.at[k, j, i], near[i]).start()

    y_bufs = (y_rec, y_mix, y_gu, y_down)

    def y_copy(k):
        return remote(y_bufs[k], mats[k].at[f], wy_send.at[k], w_recv.at[k, f], y_dev)

    def forward_copy(k, far, j):
        plane = 3 * (2 - z) if far else 3 - z
        place = plane * 2 + (j if k == DOWN else (y if j == 0 else 1 - y))
        edge = 3 * (z - 1)
        return place, block_copy(k, place, wf_send.at[k, far, j], {"fs": edge * 2 + y})

    def forward_copies(k, far, j):
        place, copy = forward_copy(k, far, j)
        if k == DOWN and far and j:
            return place, last_copies(place, {"fs": 3 * (z - 1) * 2 + y})
        return place, [copy]

    def forward(k, far, j):
        @pl.when(inner)
        def _():
            place, copies = forward_copies(k, far, j)
            wait_block(k, place)
            for copy in copies:
                copy.start()

    def last_copies(place, device):
        view = down_w.at[place]
        return [
            remote(
                view.at[:, pl.ds(i * unit, unit)],
                view.at[:, pl.ds(i * unit, unit)],
                wl_send.at[i],
                wl_recv.at[i],
                device,
            )
            for i in range(2)
        ]

    def need(k, p, piece=(0, 4)):
        def wait():
            for j in range(2):
                if k == DOWN and p == 3 and j == 1:
                    for i, copy in enumerate(last_copies(planes[p] * 2 + j, y_dev)):
                        if piece[0] <= 2 + i < sum(piece):
                            copy.wait_recv()
                elif piece[0] <= 2 * j < sum(piece):
                    wait_block(k, planes[p] * 2 + j)

        if p == 1:
            wait()
        elif p > 1:
            pl.when(jnp.logical_not(inner))(wait)

    def norm_rows(src, gain):
        def step(i, carry):
            at = pl.ds(pl.multiple_of(i * 16, 16), 16)
            v = src[at, :].astype(F32)
            inverse = lax.rsqrt(jnp.mean(v * v, axis=-1, keepdims=True) + EPS)
            nbuf[own, t, at, :] = (v * inverse * gain[...]).astype(LOW)
            return carry

        lax.fori_loop(0, half // 16, step, 0)

    def rows_copy(phase, role):
        seq, at, device = (
            (own, top, x_dev),
            (own, low, x_dev),
            (own, top, y_dev),
            (own, low, y_dev),
            (own_y, top, x_dev),
            (own_x, low, y_dev),
            (own, pl.ds(0, half), t_dev),
            (own_x, top, t_dev),
            (own_x, low, t_dev),
            (own_y, top, t_dev),
            (own_y, low, t_dev),
            (own_d, top, t_dev),
            (own_d, low, t_dev),
        )[role]
        view = nbuf.at[seq, t, at, :]
        return remote(view, view, g_send.at[role], g_recv.at[role], device)

    def rows_wait(phase, role):
        seq, side_at, at = (
            (own_x, t, top),
            (own_x, t, low),
            (own_y, t, top),
            (own_y, t, low),
            (own_d, t, top),
            (own_d, t, low),
            (own, 1 - t, pl.ds(0, half)),
            (own_x, 1 - t, top),
            (own_x, 1 - t, low),
            (own_y, 1 - t, top),
            (own_y, 1 - t, low),
            (own_d, 1 - t, top),
            (own_d, 1 - t, low),
        )[role]
        view = nbuf.at[seq, side_at, at, :]
        remote(view, view, g_send.at[role], g_recv.at[role], t_dev).wait_recv()

    def gather_start(phase):
        for role in (1, 2, 0, 3, 6):
            rows_copy(phase, role).start()

    def gather_first(phase):
        rows_wait(phase, 2)
        rows_copy(phase, 4).start()
        rows_wait(phase, 1)
        rows_copy(phase, 5).start()
        rows_copy(phase, 9).start()
        rows_copy(phase, 8).start()

    def gather_second(phase):
        rows_wait(phase, 0)
        rows_copy(phase, 7).start()
        rows_wait(phase, 3)
        rows_copy(phase, 10).start()

    def gather_last(phase):
        rows_wait(phase, 4)
        rows_copy(phase, 11).start()
        rows_wait(phase, 5)
        rows_copy(phase, 12).start()
        for role in range(6, 13):
            rows_wait(phase, role)
        for role in range(13):
            rows_copy(phase, role).wait_send()

    def products(phase, p, left, weights, k, piece=(0, 4)):
        need(k, p, piece)
        first, size = planes[p] * 2, min(piece[1], 2)

        def product(side, start):
            rows_now = left[:, side].reshape(4 * half, left.shape[-1])
            column = start % 2 * unit
            weight = weights[first + start // 2, :, column : column + size * unit]
            value = jnp.dot(rows_now, weight, preferred_element_type=F32)
            return value.astype(LOW).reshape(4, half, size * unit)

        starts = range(piece[0], sum(piece), size)
        for start in starts:
            oth[p, :, :, start * unit : (start + size) * unit] = product(1 - t, start)
        sum_copies(phase, p, 0, piece).start()
        for start in starts:
            value = product(t, start).reshape(2, 2, half, size * unit)
            kept[p, :, :, :, start * unit : (start + size) * unit] = value

    def span_of(piece):
        return pl.ds(piece[0] * unit, piece[1] * unit)

    def sum_copies(phase, p, number, piece):
        at = span_of(piece)
        src, dst, device = (
            (oth.at[p, :, :, at], rt.at[phase, p, :, :, at], t_dev),
            (kept.at[p, 1 - r, :, top, at], r1.at[phase, p, 0, :, :, at], x_dev),
            (kept.at[p, :, 1 - y, low, at], r1.at[phase, p, 1, :, :, at], y_dev),
            (kept.at[p, r, 1 - y, top, at], r2.at[phase, p, 0, :, at], y_dev),
            (kept.at[p, 1 - r, y, low, at], r2.at[phase, p, 1, :, at], x_dev),
        )[number]
        return remote(src, dst, *sum_sems(phase, p, number, piece), device)

    def sum_sems(phase, p, number, piece):
        place = PIECES.index((p, piece[0])) if phase else p
        return m_send.at[place, number], m_recv.at[4 * phase + place, number]

    def direct_copy(p, number, piece):
        at, device = span_of(piece), (x_dev, y_dev, d_dev)[number]
        a, b = ((1 - r, y), (r, 1 - y), (1 - r, 1 - y))[number]
        src, dst = kept.at[p, a, b, :, at], rd.at[piece[0] % 2, number]
        return remote(src, dst, *sum_sems(1, p, 1 + number, piece), device)

    def pair_sums(phase, p, piece=(0, 4)):
        sum_copies(phase, p, 0, piece).wait_recv()
        at = span_of(piece)

        def step(s, carry):
            a, b = lax.div(s, 2), lax.rem(s, 2)
            value = kept[p, a, b, :, at].astype(F32) + rt[phase, p, s, :, at].astype(F32)
            kept[p, a, b, :, at] = value.astype(LOW)
            return carry

        lax.fori_loop(0, 4, step, 0)
        if piece[1] == 1:
            for number in (2, 0, 1):
                direct_copy(p, number, piece).start()
        else:
            sum_copies(phase, p, 1, piece).start()
            sum_copies(phase, p, 2, piece).start()

    def line_sums(phase, p, piece=(0, 4)):
        at = span_of(piece)
        sum_copies(phase, p, 1, piece).wait_recv()
        for i in range(2):
            value = kept[p, r, i, top, at].astype(F32) + r1[phase, p, 0, i, :, at].astype(F32)
            kept[p, r, i, top, at] = value.astype(LOW)
        sum_copies(phase, p, 3, piece).start()
        sum_copies(phase, p, 2, piece).wait_recv()
        for i in range(2):
            value = kept[p, i, y, low, at].astype(F32) + r1[phase, p, 1, i, :, at].astype(F32)
            kept[p, i, y, low, at] = value.astype(LOW)
        sum_copies(phase, p, 4, piece).start()

    def columns_of(plane, piece):
        start = pl.multiple_of((plane * 4 + piece[0]) * unit, unit)
        return pl.ds(start, piece[1] * unit)

    def last_sums(phase, p, base, piece):
        at, inside = columns_of(planes[p], piece), span_of(piece)
        if piece[1] == 1:
            total = kept[p, r, y, :, inside].astype(F32)
            for number in range(3):
                direct_copy(p, number, piece).wait_recv()
                total = total + rd[piece[0] % 2, number].astype(F32)
            value = (base[:, at].astype(F32) + total).astype(LOW)
            sum_copies(phase, p, 0, piece).wait_send()
            for number in range(3):
                direct_copy(p, number, piece).wait_send()
            return at, [value[:part], value[part:]]
        values = []
        for i, number in enumerate((3, 4)):
            span = slice(i * part, (i + 1) * part)
            sum_copies(phase, p, number, piece).wait_recv()
            value = kept[p, r, y, span, inside].astype(F32) + r2[phase, p, i, :, inside].astype(F32)
            values.append((base[span, at].astype(F32) + value).astype(LOW))
        for number in range(5):
            sum_copies(phase, p, number, piece).wait_send()
        return at, values

    def mix_done(p):
        at, values = last_sums(0, p, tk, (0, 4))
        for i, value in enumerate(values):
            mx[i * part : (i + 1) * part, at] = value

    def out_copy(p, piece):
        at = columns_of(lax.rem(planes[p], 2), piece)
        src, place = oo.at[p, :, span_of(piece)], PIECES.index((p, piece[0]))
        return remote(src, out.at[t, :, at], o_send.at[place], o_recv.at[place], t_dev)

    def down_done(p, piece=(0, 4)):
        _, values = last_sums(1, p, mx, piece)
        local = lax.div(planes[p], 2) == t
        at = columns_of(lax.rem(planes[p], 2), piece)

        @pl.when(local)
        def _():
            for i, value in enumerate(values):
                out[t, i * part : (i + 1) * part, at] = value

        @pl.when(jnp.logical_not(local))
        def _():
            for i, value in enumerate(values):
                oo[p, i * part : (i + 1) * part, span_of(piece)] = value
            out_copy(p, piece).start()

    for i in range(2):
        loads["rec", i].wait()
    y_rec[...] = f_rec[1].astype(LOW)
    rec_w[f] = f_rec[0].astype(LOW)
    pl.semaphore_wait(barrier, len(peers))
    token_swap.start()
    y_copy(REC).start()
    send_own(REC, 0)
    loads["tok"].wait()
    token_swap.wait()
    norm_rows(tk, gain_one)
    gather_start(0)

    for i in range(2):
        loads["mix", i].wait()
    y_mix[...] = (f_mix[1] * mix_scale[...]).astype(LOW)
    mix_w[f] = (f_mix[0] * mix_scale[...]).astype(LOW)


    @pl.when(inner)
    def _():
        send_one(MIX, 0, 1)

    send_own(REC, 1)
    for i in range(extra.shape[0]):
        lanes = slice(i * block, (i + 1) * block)
        ext[own, :, lanes] = jnp.broadcast_to(extra[i : i + 1, :], (ext.shape[1], block))
    ext_copies = [
        remote(ext.at[own], ext.at[own], ex_send.at[i], ex_recv.at[i], device)
        for i, device in enumerate((x_dev, y_dev, d_dev))
    ]
    for copy in ext_copies:
        copy.start()
    for i in range(2):
        for name in ("gate", "up", "down"):
            loads[name, i].wait()
    for i in range(2):
        y_gu[:, i * units : (i + 1) * units] = f_gu[1, i].astype(LOW)
        gu_w[f, :, i * units : (i + 1) * units] = f_gu[0, i].astype(LOW)
    y_down[...] = (f_down[1] * down_scale[...]).astype(LOW)
    down_w[f] = (f_down[0] * down_scale[...]).astype(LOW)

    send_one(MIX, 0, 0)

    @pl.when(jnp.logical_not(inner))
    def _():
        send_one(MIX, 0, 1)

    forward(REC, 0, 0)
    forward(REC, 1, 0)
    gather_first(0)
    y_copy(MIX).start()
    y_copy(GU).start()
    y_copy(DOWN).start()
    forward(REC, 0, 1)
    forward(REC, 1, 1)
    gather_second(0)
    forward(MIX, 0, 0)
    forward(MIX, 1, 0)
    gather_last(0)
    for i, seq in enumerate((own_x, own_y, own_d)):
        remote(ext.at[seq], ext.at[seq], ex_send.at[i], ex_recv.at[i], t_dev).wait_recv()
    for p in range(1, 4):
        need(REC, p)
    loads["recur"].wait()
    loads["input"].wait()

    at_chans = pl.multiple_of(q * chans, chans)

    def recur(s, carry):
        @pl.when(s == 1)
        def _():
            send_own(MIX, 1)
            send_own(GU, 0)

        @pl.when(s == 2)
        def _():
            forward(MIX, 0, 1)

        @pl.when(s == 3)
        def _():
            forward(MIX, 1, 1)

        left = nbuf[s].reshape(rows, width)
        total = jnp.dot(left, rec_w[...].reshape(width, chans), preferred_element_type=F32)
        for b in range(chans // block):
            here = slice(b * block, (b + 1) * block)
            number = q * (chans // block) + b
            ri[:, here] = (total[:, here] * rec_scale[pl.ds(number, 1), :]).astype(LOW)
        ecol[...] = jnp.broadcast_to(ext[s, 0:1, :], (block, rows)).T
        for b in range(chans // block):
            here = slice(b * block, (b + 1) * block)
            lanes = pl.ds(pl.multiple_of(at_chans + b * block, block), block)
            number = q * (chans // block) + b
            values = ri[:, here].astype(F32)
            places = lax.broadcasted_iota(jnp.int32, values.shape, 0)
            conv_out = taps[tap_count - 1 : tap_count, lanes] * values
            for back in range(1, tap_count):
                moved = jnp.where(places >= back, pltpu.roll(values, back, 0), 0.0)
                tap = tap_count - 1 - back
                conv_out = conv_out + taps[tap : tap + 1, lanes] * moved
            conv_low = conv_out.astype(LOW)
            recur_gate = jax.nn.sigmoid(
                jnp.dot(conv_low, recur_blocks[b], preferred_element_type=F32)
            )
            input_gate = jax.nn.sigmoid(
                jnp.dot(conv_low, input_blocks[b], preferred_element_type=F32)
            )
            param = -decay_param[pl.ds(number, 1), :]
            soft = jnp.maximum(param, 0.0) + jnp.log1p(jnp.exp(-jnp.abs(param)))
            log_decay = -DECAY_FACTOR * recur_gate * soft + ecol[...]
            decay = jnp.exp(log_decay)
            drive = jnp.sqrt(-jnp.tanh(log_decay) * (1.0 + decay * decay)) * input_gate * conv_out
            step = 1
            while step < rows:
                keep = places >= step
                drive = drive + decay * jnp.where(keep, pltpu.roll(drive, step, 0), 0.0)
                if step * 2 < rows:
                    decay = decay * jnp.where(keep, pltpu.roll(decay, step, 0), 1.0)
                step *= 2
            state = drive.astype(LOW)
            st[s, 0, :, here] = state[:half]
            st[s, 1, :, here] = state[half:]
        return carry

    lax.fori_loop(0, 4, recur, 0)

    products(0, 0, st, mix_w, MIX)
    products(0, 1, st, mix_w, MIX)
    pair_sums(0, 0)
    send_own(GU, 1)
    pair_sums(0, 1)
    products(0, 2, st, mix_w, MIX)
    line_sums(0, 0)
    pair_sums(0, 2)
    line_sums(0, 1)
    products(0, 3, st, mix_w, MIX)
    mix_done(0)
    pair_sums(0, 3)
    forward(GU, 0, 0)
    line_sums(0, 2)
    mix_done(1)
    forward(GU, 1, 0)
    line_sums(0, 3)
    mix_done(2)
    mix_done(3)

    norm_rows(mx, gain_two)
    gather_start(1)
    gather_first(1)
    wait_block(DOWN, fp)
    forward(GU, 0, 1)
    gather_second(1)
    forward(GU, 1, 1)
    gather_last(1)
    send_own(DOWN, 0)
    send_own(DOWN, 1)
    for p in range(1, 4):
        need(GU, p)

    unit_rows = units // block

    def unit_scales(scale):
        first = q * unit_rows
        return jnp.concatenate([scale[pl.ds(first + i, 1), :] for i in range(unit_rows)], 1)

    def hidden(s, carry):
        left = nbuf[s].reshape(rows, width)
        total = jnp.dot(left, gu_w[...].reshape(width, 2 * units), preferred_element_type=F32)
        gate = total[:, :units] * unit_scales(gate_scale)
        up = total[:, units:] * unit_scales(up_scale)
        value = (gate * jax.nn.sigmoid(gate) * up).astype(LOW)
        hid[s, 0] = value[:half]
        hid[s, 1] = value[half:]
        return carry

    lax.fori_loop(0, 4, hidden, 0)

    first, second, third, fourth = (0, 2), (2, 2), (2, 1), (3, 1)

    def down_products(p, piece=(0, 4)):
        products(1, p, hid, down_w, DOWN, piece)

    down_products(0)
    pair_sums(1, 0)
    down_products(1)
    forward(DOWN, 0, 0)
    pair_sums(1, 1)
    line_sums(1, 0)
    forward(DOWN, 0, 1)
    forward(DOWN, 1, 0)
    down_products(2, first)
    pair_sums(1, 2, first)
    down_done(0)
    line_sums(1, 1)
    line_sums(1, 2, first)
    forward(DOWN, 1, 1)
    down_products(2, second)
    pair_sums(1, 2, second)
    down_done(1)
    down_done(2, first)
    line_sums(1, 2, second)
    down_products(3, first)
    pair_sums(1, 3, first)
    down_products(3, third)
    down_done(2, second)
    pair_sums(1, 3, third)
    line_sums(1, 3, first)
    down_products(3, fourth)
    pair_sums(1, 3, fourth)
    down_done(3, first)
    down_done(3, third)
    down_done(3, fourth)

    for p, piece in ((0, (0, 4)), (1, (0, 4)), (2, first), (2, second), (3, first), (3, third), (3, fourth)):
        local = lax.div(planes[p], 2) == t

        @pl.when(local)
        def _():
            out_copy(p, piece).wait_recv()

        @pl.when(jnp.logical_not(local))
        def _():
            out_copy(p, piece).wait_send()

    for k in range(4):
        y_copy(k).wait_send()
        for j in range(2):
            for i, device in enumerate(near):
                block_copy(k, own_place(k, j), wo_send.at[k, j, i], device).wait_send()

        @pl.when(inner)
        def _():
            for far in range(2):
                for j in range(2):
                    for copy in forward_copies(k, far, j)[1]:
                        copy.wait_send()

    for copy in ext_copies:
        copy.wait_send()


def team_body(
    tokens,
    mixing_norm_gain,
    recurrent_input_weight,
    recurrent_input_scale,
    convolution_kernel_taps,
    recurrence_gate_weight_blocks,
    input_gate_weight_blocks,
    channel_decay_parameter,
    token_extra_log_decay,
    mixing_output_weight,
    mixing_output_scale,
    feedforward_norm_gain,
    feedforward_gate_weight,
    feedforward_gate_scale,
    feedforward_up_weight,
    feedforward_up_scale,
    feedforward_down_weight,
    feedforward_down_scale,
):
    rows, half_width = tokens.shape
    half, part = rows // 2, rows // 4
    width = half_width * 2
    depth = recurrent_input_weight.shape[0]
    chans = recurrent_input_weight.shape[1] // 4
    units = feedforward_gate_weight.shape[1] // 4
    cols = mixing_output_weight.shape[1]
    block = recurrence_gate_weight_blocks.shape[1]
    planes = width // depth
    any_spec = pl.BlockSpec(memory_space=pl.ANY)
    vmem_spec = pl.BlockSpec(memory_space=pltpu.VMEM)
    vmem = pltpu.VMEM
    dma = pltpu.SemaphoreType.DMA

    def row(vector):
        return vector.reshape(1, -1)

    def lines(vector):
        return vector.reshape(-1, block)

    out = pl.pallas_call(
        layer_kernel,
        out_shape=vmem((2, half, half_width), LOW),
        in_specs=[any_spec] * 6 + [vmem_spec] * 3 + [any_spec] * 2 + [vmem_spec] * 7,
        out_specs=vmem_spec,
        scratch_shapes=[
            vmem((4, 2, half, width), LOW),
            vmem((planes, depth, chans), LOW),
            vmem((planes, chans, cols), LOW),
            vmem((planes, depth, 2 * units), LOW),
            vmem((planes, units, cols), LOW),
            vmem((2, depth, chans), F32),
            vmem((2, chans, cols), F32),
            vmem((2, 2, depth, units), F32),
            vmem((2, units, cols), F32),
            vmem((depth, chans), LOW),
            vmem((chans, cols), LOW),
            vmem((depth, 2 * units), LOW),
            vmem((units, cols), LOW),
            vmem((half, width), LOW),
            vmem((half, width), LOW),
            vmem((4, 2, half, chans), LOW),
            vmem((4, 2, half, units), LOW),
            vmem((rows, chans), LOW),
            vmem((4, 8, rows), F32),
            vmem((rows, block), F32),
            vmem((4, 4, half, 2 * cols), LOW),
            vmem((4, 2, 2, half, 2 * cols), LOW),
            vmem((2, 4, 4, half, 2 * cols), LOW),
            vmem((2, 4, 2, 2, part, 2 * cols), LOW),
            vmem((2, 4, 2, part, 2 * cols), LOW),
            vmem((2, 3, half, cols // 2), LOW),
            vmem((4, half, 2 * cols), LOW),
            vmem((chans // block, block, block), LOW),
            vmem((chans // block, block, block), LOW),
            dma((13,)),
            dma((2,)),
            dma((2,)),
            dma((4,)),
            dma((4, 2, 2)),
            dma((4, 2, 2)),
            dma((4, planes)),
            dma((13,)),
            dma((13,)),
            dma((2,)),
            dma((3,)),
            dma((3,)),
            dma((len(PIECES), 5)),
            dma((4 + len(PIECES), 5)),
            dma((len(PIECES),)),
            dma((len(PIECES),)),
        ],
        compiler_params=pltpu.CompilerParams(
            collective_id=0, has_side_effects=True, vmem_limit_bytes=VMEM_BYTES
        ),
    )(
        tokens,
        recurrent_input_weight,
        mixing_output_weight,
        feedforward_gate_weight,
        feedforward_up_weight,
        feedforward_down_weight,
        row(mixing_norm_gain),
        lines(recurrent_input_scale),
        convolution_kernel_taps,
        recurrence_gate_weight_blocks,
        input_gate_weight_blocks,
        lines(channel_decay_parameter),
        lines(token_extra_log_decay),
        row(mixing_output_scale),
        row(feedforward_norm_gain),
        lines(feedforward_gate_scale),
        lines(feedforward_up_scale),
        row(feedforward_down_scale),
    )
    return out.reshape(rows, half_width)


VMEM_BYTES = 60_000_000


def team_fits(mesh):
    sizes = mesh.shape
    return sizes["rep"] == 2 and sizes["tp"] == 2 and sizes["fs"] == 8


def solution(mesh):
    placed = (
        P(("rep", "fs"), "tp"),
        P(),
        P("fs", "tp"),
        P("tp"),
        P(None, "tp"),
        P("tp", None, None),
        P("tp", None, None),
        P("tp"),
        P(("rep", "fs")),
        P("tp", "fs"),
        P("fs"),
        P(),
        P("fs", "tp"),
        P("tp"),
        P("fs", "tp"),
        P("tp"),
        P("tp", "fs"),
        P("fs"),
    )

    def body(*args):
        blocks, hidden, rows = args[5].shape[0], args[12].shape[1], args[0].shape[0]
        if not team_fits(mesh) or blocks % 4 or hidden % 512 or rows % 64 or args[9].shape[1] % 256:
            return plain_body(*args)
        return team_body(*args)

    return jax.shard_map(
        body, mesh=mesh, in_specs=placed, out_specs=P(("rep", "fs"), "tp"), check_vma=False
    )
```

```python
import jax
import jax.numpy as jnp
from jax import lax
from jax.experimental import pallas as pl
from jax.experimental.pallas import tpu as pltpu
from jax.sharding import PartitionSpec as P

EPS = 1e-06
DECAY_FACTOR = 8.0


def row_norm(rows, gain_vec):
    values = rows.astype(jnp.float32)
    inverse = lax.rsqrt(jnp.mean(values * values, axis=-1, keepdims=True) + EPS)
    return (values * inverse * gain_vec).astype(jnp.bfloat16)


def gather_normed(rows, gain_vec):
    whole_rows = lax.all_gather(rows, "tp", axis=1, tiled=True)
    return row_norm(whole_rows, gain_vec)


def share_sums(terms):
    return lax.psum_scatter(
        terms.astype(jnp.bfloat16), "tp", scatter_dimension=1, tiled=True
    ).astype(jnp.float32)


def combine_pairs(earlier, later):
    decay_one, value_one = earlier
    decay_two, value_two = later
    return (decay_one * decay_two, decay_two * value_one + value_two)


def add_one(left_rows, weight_piece):
    return jnp.dot(left_rows, weight_piece, preferred_element_type=jnp.float32)


def place_columns(left_rows, total_now, pieces, start_row):
    weight_piece, scale_piece = pieces
    product = jnp.dot(left_rows, weight_piece, preferred_element_type=jnp.float32) * scale_piece
    return lax.dynamic_update_slice_in_dim(total_now, product, start_row, 1)


def plain_body(
    tokens,
    mixing_norm_gain,
    recurrent_input_weight,
    recurrent_input_scale,
    convolution_kernel_taps,
    recurrence_gate_weight_blocks,
    input_gate_weight_blocks,
    channel_decay_parameter,
    token_extra_log_decay,
    mixing_output_weight,
    mixing_output_scale,
    feedforward_norm_gain,
    feedforward_gate_weight,
    feedforward_gate_scale,
    feedforward_up_weight,
    feedforward_up_scale,
    feedforward_down_weight,
    feedforward_down_scale,
):
    normed = gather_normed(tokens, mixing_norm_gain)
    seq_rows = normed.shape[0]
    model_width = normed.shape[1]
    width_dev = recurrent_input_weight.shape[1]
    rec_sum = add_one(
        normed,
        lax.all_gather(recurrent_input_weight.astype(jnp.bfloat16), "fs", axis=0, tiled=True),
    )
    rec_input = (rec_sum * recurrent_input_scale).astype(jnp.bfloat16)
    rec_f32 = rec_input.astype(jnp.float32)
    tap_count = convolution_kernel_taps.shape[0]
    padded = jnp.pad(rec_f32, ((tap_count - 1, 0), (0, 0)))
    conv_out = jnp.zeros((seq_rows, width_dev), jnp.float32)
    for tap_index in range(tap_count):
        conv_out = (
            conv_out + convolution_kernel_taps[tap_index] * padded[tap_index : tap_index + seq_rows]
        )
    block_count = recurrence_gate_weight_blocks.shape[0]
    block_size = recurrence_gate_weight_blocks.shape[1]
    blocks = conv_out.astype(jnp.bfloat16).reshape(seq_rows, block_count, block_size)
    recurrence_gate_values = jax.nn.sigmoid(
        jnp.einsum(
            "lni,nij->lnj",
            blocks,
            recurrence_gate_weight_blocks,
            preferred_element_type=jnp.float32,
        ).reshape(seq_rows, width_dev)
    )
    input_gate = jax.nn.sigmoid(
        jnp.einsum(
            "lni,nij->lnj", blocks, input_gate_weight_blocks, preferred_element_type=jnp.float32
        ).reshape(seq_rows, width_dev)
    )
    decay_logarithm = (
        -DECAY_FACTOR * recurrence_gate_values * jax.nn.softplus(-channel_decay_parameter)
        + token_extra_log_decay[:, None]
    )
    decay = jnp.exp(decay_logarithm)
    drive = jnp.sqrt(-jnp.expm1(2.0 * decay_logarithm)) * input_gate * conv_out
    _, state = lax.associative_scan(combine_pairs, (decay, drive), axis=0)
    state_low = state.astype(jnp.bfloat16)
    mix_terms = place_columns(
        state_low,
        jnp.zeros((seq_rows, model_width), jnp.float32),
        (
            lax.all_gather(mixing_output_weight.astype(jnp.bfloat16), "fs", axis=1, tiled=True),
            lax.all_gather(
                mixing_output_scale.reshape(1, -1).astype(jnp.bfloat16), "fs", axis=1, tiled=True
            ).astype(jnp.float32),
        ),
        jnp.int32(0),
    )
    mixed = (tokens.astype(jnp.float32) + share_sums(mix_terms)).astype(jnp.bfloat16)
    normed_ffn = gather_normed(mixed, feedforward_norm_gain)
    gate_sum = add_one(
        normed_ffn,
        lax.all_gather(feedforward_gate_weight.astype(jnp.bfloat16), "fs", axis=0, tiled=True),
    )
    up_sum = add_one(
        normed_ffn,
        lax.all_gather(feedforward_up_weight.astype(jnp.bfloat16), "fs", axis=0, tiled=True),
    )
    hidden = (
        jax.nn.silu(gate_sum * feedforward_gate_scale) * (up_sum * feedforward_up_scale)
    ).astype(jnp.bfloat16)
    down_terms = place_columns(
        hidden,
        jnp.zeros((seq_rows, model_width), jnp.float32),
        (
            lax.all_gather(feedforward_down_weight.astype(jnp.bfloat16), "fs", axis=1, tiled=True),
            lax.all_gather(
                feedforward_down_scale.reshape(1, -1).astype(jnp.bfloat16), "fs", axis=1, tiled=True
            ).astype(jnp.float32),
        ),
        jnp.int32(0),
    )
    return (mixed.astype(jnp.float32) + share_sums(down_terms)).astype(jnp.bfloat16)


REC, MIX, GU, DOWN = range(4)
PIECES = ((0, 0), (1, 0), (2, 0), (2, 2), (3, 0), (3, 2), (3, 3))
LOW = jnp.bfloat16
F32 = jnp.float32


def remote(src, dst, send_sem, recv_sem, device):
    return pltpu.make_async_remote_copy(
        src_ref=src,
        dst_ref=dst,
        send_sem=send_sem,
        recv_sem=recv_sem,
        device_id=device,
        device_id_type=pl.DeviceIdType.MESH,
    )


def layer_kernel(
    tokens,
    w_rec,
    w_mix,
    w_gate,
    w_up,
    w_down,
    gain_one,
    rec_scale,
    taps,
    w_recur,
    w_input,
    decay_param,
    extra,
    mix_scale,
    gain_two,
    gate_scale,
    up_scale,
    down_scale,
    out,
    nbuf,
    rec_w,
    mix_w,
    gu_w,
    down_w,
    f_rec,
    f_mix,
    f_gu,
    f_down,
    y_rec,
    y_mix,
    y_gu,
    y_down,
    tk,
    mx,
    st,
    hid,
    ri,
    ext,
    ecol,
    oth,
    kept,
    rt,
    r1,
    r2,
    rd,
    oo,
    recur_blocks,
    input_blocks,
    load_sem,
    wl_recv,
    wy_send,
    wo_send,
    wf_send,
    w_recv,
    g_send,
    g_recv,
    tt_sem,
    ex_sem,
    m_send,
    m_recv,
    o_sem,
):
    rows, half_width = tokens.shape
    half, part = rows // 2, rows // 4
    width = half_width * 2
    chans = rec_w.shape[2]
    units = down_w.shape[1]
    cols = mix_w.shape[2]
    unit = cols // 2
    block = recur_blocks.shape[1]
    tap_count = taps.shape[0]

    r, f, t = lax.axis_index("rep"), lax.axis_index("fs"), lax.axis_index("tp")
    y, z = lax.rem(f, 2), lax.div(f, 2)
    fp = f + 1 - 2 * y
    q = r * 2 + y
    own, own_x, own_y, own_d = q, (1 - r) * 2 + y, r * 2 + 1 - y, (1 - r) * 2 + 1 - y
    x_dev, y_dev, t_dev = {"rep": 1 - r}, {"fs": fp}, {"tp": 1 - t}
    d_dev = {"rep": 1 - r, "fs": fp}
    inner = lax.div(z + 1, 2) == 1
    near = (1 + lax.rem(z, 2), lax.rem(2 + 3 * z, 5))
    near = tuple({"fs": plane * 2 + y} for plane in near)
    planes = (z, z + 1 - 2 * lax.rem(z, 2), z + 2 - 4 * lax.div(z, 2), 3 - z)
    mats = (rec_w, mix_w, gu_w, down_w)
    top, low = pl.ds(0, part), pl.ds(part, part)

    barrier = pltpu.get_barrier_semaphore()

    def greet(device):
        pl.semaphore_signal(barrier, inc=1, device_id=device, device_id_type=pl.DeviceIdType.MESH)

    for device in (x_dev, y_dev, t_dev, d_dev, near[0]):
        greet(device)

    @pl.when(inner)
    def _():
        greet({"fs": y})
        greet({"fs": 6 + y})

    quarters = (q, r * 2 + 1 - y)

    def load(number, src, dst):
        pltpu.make_async_copy(src, dst, load_sem.at[number]).start()

    def loaded(number, whole):
        pltpu.make_async_copy(whole, whole, load_sem.at[number]).wait()

    mine = pl.ds(pl.multiple_of(t * half, half), half)
    theirs = pl.ds(pl.multiple_of((1 - t) * half, half), half)
    side = pl.ds(pl.multiple_of(t * half_width, half_width), half_width)
    for i, piece in enumerate(quarters):
        at = pl.ds(pl.multiple_of(piece * chans, chans), chans)
        load(REC, w_rec.at[:, at], f_rec.at[i])
    load(4, tokens.at[mine, :], tk.at[:, side])
    for i, piece in enumerate(quarters):
        at = pl.ds(pl.multiple_of(piece * chans, chans), chans)
        load(MIX, w_mix.at[at, :], f_mix.at[i])
    for i, piece in enumerate(quarters):
        at = pl.ds(pl.multiple_of(piece * units, units), units)
        load(GU, w_gate.at[:, at], f_gu.at[i, 0])
        load(GU, w_up.at[:, at], f_gu.at[i, 1])
        load(DOWN, w_down.at[at, :], f_down.at[i])
    gate_blocks = pl.ds(q * (chans // block), chans // block)
    load(5, w_recur.at[gate_blocks], recur_blocks)
    load(6, w_input.at[gate_blocks], input_blocks)

    token_swap = remote(tokens.at[theirs, :], tk.at[:, side], tt_sem.at[0], tt_sem.at[1], t_dev)

    def block_copy(k, place, send_sem, device):
        view = mats[k].at[place]
        return remote(view, view, send_sem, w_recv.at[k, place], device)

    def wait_block(k, place):
        block_copy(k, place, wo_send.at[0], y_dev).wait_recv()

    def own_place(k, j):
        return z * 2 + j if k == DOWN else (f if j == 0 else fp)

    def send_own(k, j):
        if j == 1 and k != DOWN:
            wait_block(k, fp)
        for i in range(2):
            send_one(k, j, i)

    def send_one(k, j, i):
        block_copy(k, own_place(k, j), wo_send.at[k], near[i]).start()

    def sent(view, sem):
        remote(view, view, sem, w_recv.at[0, 0], y_dev).wait_send()

    y_bufs = (y_rec, y_mix, y_gu, y_down)

    def y_copy(k):
        return remote(y_bufs[k], mats[k].at[f], wy_send.at[k], w_recv.at[k, f], y_dev)

    def forward_copy(k, far, j):
        plane = 3 * (2 - z) if far else 3 - z
        place = plane * 2 + (j if k == DOWN else (y if j == 0 else 1 - y))
        edge = 3 * (z - 1)
        return place, block_copy(k, place, wf_send.at[k], {"fs": edge * 2 + y})

    def forward_copies(k, far, j):
        place, copy = forward_copy(k, far, j)
        if k == DOWN and far and j:
            return place, last_copies(place, {"fs": 3 * (z - 1) * 2 + y})
        return place, [copy]

    def forward(k, far, j):
        @pl.when(inner)
        def _():
            place, copies = forward_copies(k, far, j)
            wait_block(k, place)
            for copy in copies:
                copy.start()

    def last_copies(place, device):
        view = down_w.at[place]
        return [
            remote(
                view.at[:, pl.ds(i * unit, unit)],
                view.at[:, pl.ds(i * unit, unit)],
                wf_send.at[DOWN],
                wl_recv.at[i],
                device,
            )
            for i in range(2)
        ]

    def need(k, p, piece=(0, 4)):
        def wait():
            for j in range(2):
                if k == DOWN and p == 3 and j == 1:
                    for i, copy in enumerate(last_copies(planes[p] * 2 + j, y_dev)):
                        if piece[0] <= 2 + i < sum(piece):
                            copy.wait_recv()
                elif piece[0] <= 2 * j < sum(piece):
                    wait_block(k, planes[p] * 2 + j)

        if p == 1:
            wait()
        elif p > 1:
            pl.when(jnp.logical_not(inner))(wait)

    def norm_rows(src, gain):
        def step(i, carry):
            at = pl.ds(pl.multiple_of(i * 16, 16), 16)
            v = src[at, :].astype(F32)
            inverse = lax.rsqrt(jnp.mean(v * v, axis=-1, keepdims=True) + EPS)
            nbuf[own, t, at, :] = (v * inverse * gain[...]).astype(LOW)
            return carry

        lax.fori_loop(0, half // 16, step, 0)

    def rows_copy(phase, role):
        seq, at, device = (
            (own, top, x_dev),
            (own, low, x_dev),
            (own, top, y_dev),
            (own, low, y_dev),
            (own_y, top, x_dev),
            (own_x, low, y_dev),
            (own, pl.ds(0, half), t_dev),
            (own_x, top, t_dev),
            (own_x, low, t_dev),
            (own_y, top, t_dev),
            (own_y, low, t_dev),
            (own_d, top, t_dev),
            (own_d, low, t_dev),
        )[role]
        view = nbuf.at[seq, t, at, :]
        return remote(view, view, g_send.at[role // 7], g_recv.at[min(role, 6)], device)

    def rows_wait(phase, role):
        if role == 6:
            view = nbuf.at[:, 1 - t]
        else:
            seq, at = (
                (own_x, top),
                (own_x, low),
                (own_y, top),
                (own_y, low),
                (own_d, top),
                (own_d, low),
            )[role]
            view = nbuf.at[seq, t, at, :]
        remote(view, view, g_send.at[0], g_recv.at[role], t_dev).wait_recv()

    def gather_start(phase):
        for role in (1, 2, 0, 3, 6):
            rows_copy(phase, role).start()

    def gather_first(phase):
        rows_wait(phase, 2)
        rows_copy(phase, 4).start()
        rows_wait(phase, 1)
        rows_copy(phase, 5).start()
        rows_copy(phase, 9).start()
        rows_copy(phase, 8).start()

    def gather_second(phase):
        rows_wait(phase, 0)
        rows_copy(phase, 7).start()
        rows_wait(phase, 3)
        rows_copy(phase, 10).start()

    def gather_last(phase):
        rows_wait(phase, 4)
        rows_copy(phase, 11).start()
        rows_wait(phase, 5)
        rows_copy(phase, 12).start()
        rows_wait(phase, 6)
        sent(nbuf.at[pl.ds(0, 2)], g_send.at[0])
        sent(nbuf.at[pl.ds(0, 3), 0], g_send.at[1])

    def products(phase, p, left, weights, k, piece=(0, 4)):
        need(k, p, piece)
        first, size = planes[p] * 2, min(piece[1], 2)

        def product(side, start):
            rows_now = left[:, side].reshape(4 * half, left.shape[-1])
            column = start % 2 * unit
            weight = weights[first + start // 2, :, column : column + size * unit]
            value = jnp.dot(rows_now, weight, preferred_element_type=F32)
            return value.astype(LOW).reshape(4, half, size * unit)

        starts = range(piece[0], sum(piece), size)
        for start in starts:
            oth[p, :, :, start * unit : (start + size) * unit] = product(1 - t, start)
        sum_copies(phase, p, 0, piece).start()
        for start in starts:
            value = product(t, start).reshape(2, 2, half, size * unit)
            kept[p, :, :, :, start * unit : (start + size) * unit] = value

    def span_of(piece):
        return pl.ds(piece[0] * unit, piece[1] * unit)

    def sum_copies(phase, p, number, piece):
        at = span_of(piece)
        src, dst, device = (
            (oth.at[p, :, :, at], rt.at[phase, p, :, :, at], t_dev),
            (kept.at[p, 1 - r, :, top, at], r1.at[phase, p, 0, :, :, at], x_dev),
            (kept.at[p, :, 1 - y, low, at], r1.at[phase, p, 1, :, :, at], y_dev),
            (kept.at[p, r, 1 - y, top, at], r2.at[phase, p, 0, :, at], y_dev),
            (kept.at[p, 1 - r, y, low, at], r2.at[phase, p, 1, :, at], x_dev),
        )[number]
        return remote(src, dst, *sum_sems(phase, p, number, piece), device)

    def sum_sems(phase, p, number, piece):
        place = PIECES.index((p, piece[0])) if phase else p
        return m_send.at[place, min(number, 1)], m_recv.at[4 * phase + place, number]

    def direct_copy(p, number, piece):
        at, device = span_of(piece), (x_dev, y_dev, d_dev)[number]
        a, b = ((1 - r, y), (r, 1 - y), (1 - r, 1 - y))[number]
        src, dst = kept.at[p, a, b, :, at], rd.at[piece[0] % 2, number]
        return remote(src, dst, *sum_sems(1, p, 1 + number, piece), device)

    def pair_sums(phase, p, piece=(0, 4)):
        sum_copies(phase, p, 0, piece).wait_recv()
        at = span_of(piece)

        def step(s, carry):
            a, b = lax.div(s, 2), lax.rem(s, 2)
            value = kept[p, a, b, :, at].astype(F32) + rt[phase, p, s, :, at].astype(F32)
            kept[p, a, b, :, at] = value.astype(LOW)
            return carry

        lax.fori_loop(0, 4, step, 0)
        if piece[1] == 1:
            for number in (2, 0, 1):
                direct_copy(p, number, piece).start()
        else:
            sum_copies(phase, p, 1, piece).start()
            sum_copies(phase, p, 2, piece).start()

    def line_sums(phase, p, piece=(0, 4)):
        at = span_of(piece)
        sum_copies(phase, p, 1, piece).wait_recv()
        for i in range(2):
            value = kept[p, r, i, top, at].astype(F32) + r1[phase, p, 0, i, :, at].astype(F32)
            kept[p, r, i, top, at] = value.astype(LOW)
        sum_copies(phase, p, 3, piece).start()
        sum_copies(phase, p, 2, piece).wait_recv()
        for i in range(2):
            value = kept[p, i, y, low, at].astype(F32) + r1[phase, p, 1, i, :, at].astype(F32)
            kept[p, i, y, low, at] = value.astype(LOW)
        sum_copies(phase, p, 4, piece).start()

    def columns_of(plane, piece):
        start = pl.multiple_of((plane * 4 + piece[0]) * unit, unit)
        return pl.ds(start, piece[1] * unit)

    def sums_sent(phase, p, piece):
        sum_copies(phase, p, 0, piece).wait_send()
        view = oth.at[p, pl.ds(0, 3), :, span_of(piece)]
        sent(view, sum_sems(phase, p, 1, piece)[0])

    def last_sums(phase, p, base, piece):
        at, inside = columns_of(planes[p], piece), span_of(piece)
        if piece[1] == 1:
            total = kept[p, r, y, :, inside].astype(F32)
            for number in range(3):
                direct_copy(p, number, piece).wait_recv()
                total = total + rd[piece[0] % 2, number].astype(F32)
            value = (base[:, at].astype(F32) + total).astype(LOW)
            sums_sent(phase, p, piece)
            return at, [value[:part], value[part:]]
        values = []
        for i, number in enumerate((3, 4)):
            span = slice(i * part, (i + 1) * part)
            sum_copies(phase, p, number, piece).wait_recv()
            value = kept[p, r, y, span, inside].astype(F32) + r2[phase, p, i, :, inside].astype(F32)
            values.append((base[span, at].astype(F32) + value).astype(LOW))
        sums_sent(phase, p, piece)
        return at, values

    def mix_done(p):
        at, values = last_sums(0, p, tk, (0, 4))
        for i, value in enumerate(values):
            mx[i * part : (i + 1) * part, at] = value

    def out_copy(p, piece):
        at = columns_of(lax.rem(planes[p], 2), piece)
        src = oo.at[p, :, span_of(piece)]
        return remote(src, out.at[t, :, at], o_sem.at[0], o_sem.at[1], t_dev)

    def down_done(p, piece=(0, 4)):
        _, values = last_sums(1, p, mx, piece)
        local = lax.div(planes[p], 2) == t
        at = columns_of(lax.rem(planes[p], 2), piece)

        @pl.when(local)
        def _():
            for i, value in enumerate(values):
                out[t, i * part : (i + 1) * part, at] = value

        @pl.when(jnp.logical_not(local))
        def _():
            for i, value in enumerate(values):
                oo[p, i * part : (i + 1) * part, span_of(piece)] = value
            out_copy(p, piece).start()

    loaded(REC, f_rec)
    y_rec[...] = f_rec[1].astype(LOW)
    rec_w[f] = f_rec[0].astype(LOW)
    pl.semaphore_wait(barrier, 6)
    token_swap.start()
    y_copy(REC).start()
    send_own(REC, 0)
    loaded(4, tk.at[:, side])
    token_swap.wait()
    norm_rows(tk, gain_one)
    gather_start(0)

    loaded(MIX, f_mix)
    y_mix[...] = (f_mix[1] * mix_scale[...]).astype(LOW)
    mix_w[f] = (f_mix[0] * mix_scale[...]).astype(LOW)


    @pl.when(inner)
    def _():
        send_one(MIX, 0, 1)

    send_own(REC, 1)
    for i in range(extra.shape[0]):
        lanes = slice(i * block, (i + 1) * block)
        ext[own, :, lanes] = jnp.broadcast_to(extra[i : i + 1, :], (ext.shape[1], block))
    ext_copies = [
        remote(ext.at[own], ext.at[own], ex_sem.at[0], ex_sem.at[1], device)
        for device in (x_dev, y_dev, d_dev)
    ]
    for copy in ext_copies:
        copy.start()
    loaded(GU, f_gu)
    loaded(DOWN, f_down)
    for i in range(2):
        y_gu[:, i * units : (i + 1) * units] = f_gu[1, i].astype(LOW)
        gu_w[f, :, i * units : (i + 1) * units] = f_gu[0, i].astype(LOW)
    y_down[...] = (f_down[1] * down_scale[...]).astype(LOW)
    down_w[f] = (f_down[0] * down_scale[...]).astype(LOW)

    send_one(MIX, 0, 0)

    @pl.when(jnp.logical_not(inner))
    def _():
        send_one(MIX, 0, 1)

    forward(REC, 0, 0)
    forward(REC, 1, 0)
    gather_first(0)
    y_copy(MIX).start()
    y_copy(GU).start()
    y_copy(DOWN).start()
    forward(REC, 0, 1)
    forward(REC, 1, 1)
    gather_second(0)
    forward(MIX, 0, 0)
    forward(MIX, 1, 0)
    gather_last(0)
    three = ext.at[pl.ds(0, 3)]
    remote(three, three, ex_sem.at[0], ex_sem.at[1], t_dev).wait_recv()
    for p in range(1, 4):
        need(REC, p)
    loaded(5, recur_blocks)
    loaded(6, input_blocks)

    at_chans = pl.multiple_of(q * chans, chans)

    def recur(s, carry):
        @pl.when(s == 1)
        def _():
            send_own(MIX, 1)
            send_own(GU, 0)

        @pl.when(s == 2)
        def _():
            forward(MIX, 0, 1)

        @pl.when(s == 3)
        def _():
            forward(MIX, 1, 1)

        left = nbuf[s].reshape(rows, width)
        total = jnp.dot(left, rec_w[...].reshape(width, chans), preferred_element_type=F32)
        for b in range(chans // block):
            here = slice(b * block, (b + 1) * block)
            number = q * (chans // block) + b
            ri[:, here] = (total[:, here] * rec_scale[pl.ds(number, 1), :]).astype(LOW)
        ecol[...] = jnp.broadcast_to(ext[s, 0:1, :], (block, rows)).T
        for b in range(chans // block):
            here = slice(b * block, (b + 1) * block)
            lanes = pl.ds(pl.multiple_of(at_chans + b * block, block), block)
            number = q * (chans // block) + b
            values = ri[:, here].astype(F32)
            places = lax.broadcasted_iota(jnp.int32, values.shape, 0)
            conv_out = taps[tap_count - 1 : tap_count, lanes] * values
            for back in range(1, tap_count):
                moved = jnp.where(places >= back, pltpu.roll(values, back, 0), 0.0)
                tap = tap_count - 1 - back
                conv_out = conv_out + taps[tap : tap + 1, lanes] * moved
            conv_low = conv_out.astype(LOW)
            recur_gate = jax.nn.sigmoid(
                jnp.dot(conv_low, recur_blocks[b], preferred_element_type=F32)
            )
            input_gate = jax.nn.sigmoid(
                jnp.dot(conv_low, input_blocks[b], preferred_element_type=F32)
            )
            param = -decay_param[pl.ds(number, 1), :]
            soft = jnp.maximum(param, 0.0) + jnp.log1p(jnp.exp(-jnp.abs(param)))
            log_decay = -DECAY_FACTOR * recur_gate * soft + ecol[...]
            decay = jnp.exp(log_decay)
            drive = jnp.sqrt(-jnp.tanh(log_decay) * (1.0 + decay * decay)) * input_gate * conv_out
            step = 1
            while step < rows:
                keep = places >= step
                drive = drive + decay * jnp.where(keep, pltpu.roll(drive, step, 0), 0.0)
                if step * 2 < rows:
                    decay = decay * jnp.where(keep, pltpu.roll(decay, step, 0), 1.0)
                step *= 2
            state = drive.astype(LOW)
            st[s, 0, :, here] = state[:half]
            st[s, 1, :, here] = state[half:]
        return carry

    lax.fori_loop(0, 4, recur, 0)

    products(0, 0, st, mix_w, MIX)
    products(0, 1, st, mix_w, MIX)
    pair_sums(0, 0)
    send_own(GU, 1)
    pair_sums(0, 1)
    products(0, 2, st, mix_w, MIX)
    line_sums(0, 0)
    pair_sums(0, 2)
    line_sums(0, 1)
    products(0, 3, st, mix_w, MIX)
    mix_done(0)
    pair_sums(0, 3)
    forward(GU, 0, 0)
    line_sums(0, 2)
    mix_done(1)
    forward(GU, 1, 0)
    line_sums(0, 3)
    mix_done(2)
    mix_done(3)

    norm_rows(mx, gain_two)
    gather_start(1)
    gather_first(1)
    wait_block(DOWN, fp)
    forward(GU, 0, 1)
    gather_second(1)
    forward(GU, 1, 1)
    gather_last(1)
    send_own(DOWN, 0)
    send_own(DOWN, 1)
    for p in range(1, 4):
        need(GU, p)

    unit_rows = units // block

    def unit_scales(scale):
        first = q * unit_rows
        return jnp.concatenate([scale[pl.ds(first + i, 1), :] for i in range(unit_rows)], 1)

    def hidden(s, carry):
        left = nbuf[s].reshape(rows, width)
        total = jnp.dot(left, gu_w[...].reshape(width, 2 * units), preferred_element_type=F32)
        gate = total[:, :units] * unit_scales(gate_scale)
        up = total[:, units:] * unit_scales(up_scale)
        value = (gate * jax.nn.sigmoid(gate) * up).astype(LOW)
        hid[s, 0] = value[:half]
        hid[s, 1] = value[half:]
        return carry

    lax.fori_loop(0, 4, hidden, 0)

    first, second, third, fourth = (0, 2), (2, 2), (2, 1), (3, 1)

    def down_products(p, piece=(0, 4)):
        products(1, p, hid, down_w, DOWN, piece)

    down_products(0)
    pair_sums(1, 0)
    down_products(1)
    forward(DOWN, 0, 0)
    pair_sums(1, 1)
    line_sums(1, 0)
    forward(DOWN, 0, 1)
    forward(DOWN, 1, 0)
    down_products(2, first)
    pair_sums(1, 2, first)
    down_done(0)
    line_sums(1, 1)
    line_sums(1, 2, first)
    forward(DOWN, 1, 1)
    down_products(2, second)
    pair_sums(1, 2, second)
    down_done(1)
    down_done(2, first)
    line_sums(1, 2, second)
    down_products(3, first)
    pair_sums(1, 3, first)
    down_products(3, third)
    down_done(2, second)
    pair_sums(1, 3, third)
    line_sums(1, 3, first)
    down_products(3, fourth)
    pair_sums(1, 3, fourth)
    down_done(3, first)
    down_done(3, third)
    down_done(3, fourth)

    theirs_here = out.at[1 - t]
    remote(theirs_here, theirs_here, o_sem.at[0], o_sem.at[1], t_dev).wait()
    for k in range(4):
        y_copy(k).wait_send()
        sent(mats[k].at[pl.ds(0, 4)], wo_send.at[k])

        @pl.when(inner)
        def _():
            sent(mats[k].at[pl.ds(0, 4)], wf_send.at[k])

    sent(ext.at[pl.ds(0, 3)], ex_sem.at[0])


def team_body(
    tokens,
    mixing_norm_gain,
    recurrent_input_weight,
    recurrent_input_scale,
    convolution_kernel_taps,
    recurrence_gate_weight_blocks,
    input_gate_weight_blocks,
    channel_decay_parameter,
    token_extra_log_decay,
    mixing_output_weight,
    mixing_output_scale,
    feedforward_norm_gain,
    feedforward_gate_weight,
    feedforward_gate_scale,
    feedforward_up_weight,
    feedforward_up_scale,
    feedforward_down_weight,
    feedforward_down_scale,
):
    rows, half_width = tokens.shape
    half, part = rows // 2, rows // 4
    width = half_width * 2
    depth = recurrent_input_weight.shape[0]
    chans = recurrent_input_weight.shape[1] // 4
    units = feedforward_gate_weight.shape[1] // 4
    cols = mixing_output_weight.shape[1]
    block = recurrence_gate_weight_blocks.shape[1]
    planes = width // depth
    any_spec = pl.BlockSpec(memory_space=pl.ANY)
    vmem_spec = pl.BlockSpec(memory_space=pltpu.VMEM)
    vmem = pltpu.VMEM
    dma = pltpu.SemaphoreType.DMA

    def row(vector):
        return vector.reshape(1, -1)

    def lines(vector):
        return vector.reshape(-1, block)

    out = pl.pallas_call(
        layer_kernel,
        out_shape=vmem((2, half, half_width), LOW),
        in_specs=[any_spec] * 6 + [vmem_spec] * 3 + [any_spec] * 2 + [vmem_spec] * 7,
        out_specs=vmem_spec,
        scratch_shapes=[
            vmem((4, 2, half, width), LOW),
            vmem((planes, depth, chans), LOW),
            vmem((planes, chans, cols), LOW),
            vmem((planes, depth, 2 * units), LOW),
            vmem((planes, units, cols), LOW),
            vmem((2, depth, chans), F32),
            vmem((2, chans, cols), F32),
            vmem((2, 2, depth, units), F32),
            vmem((2, units, cols), F32),
            vmem((depth, chans), LOW),
            vmem((chans, cols), LOW),
            vmem((depth, 2 * units), LOW),
            vmem((units, cols), LOW),
            vmem((half, width), LOW),
            vmem((half, width), LOW),
            vmem((4, 2, half, chans), LOW),
            vmem((4, 2, half, units), LOW),
            vmem((rows, chans), LOW),
            vmem((4, 8, rows), F32),
            vmem((rows, block), F32),
            vmem((4, 4, half, 2 * cols), LOW),
            vmem((4, 2, 2, half, 2 * cols), LOW),
            vmem((2, 4, 4, half, 2 * cols), LOW),
            vmem((2, 4, 2, 2, part, 2 * cols), LOW),
            vmem((2, 4, 2, part, 2 * cols), LOW),
            vmem((2, 3, half, cols // 2), LOW),
            vmem((4, half, 2 * cols), LOW),
            vmem((chans // block, block, block), LOW),
            vmem((chans // block, block, block), LOW),
            dma((7,)),
            dma((2,)),
            dma((4,)),
            dma((4,)),
            dma((4,)),
            dma((4, planes)),
            dma((2,)),
            dma((7,)),
            dma((2,)),
            dma((2,)),
            dma((len(PIECES), 2)),
            dma((4 + len(PIECES), 5)),
            dma((2,)),
        ],
        compiler_params=pltpu.CompilerParams(
            collective_id=0, has_side_effects=True, vmem_limit_bytes=VMEM_BYTES
        ),
    )(
        tokens,
        recurrent_input_weight,
        mixing_output_weight,
        feedforward_gate_weight,
        feedforward_up_weight,
        feedforward_down_weight,
        row(mixing_norm_gain),
        lines(recurrent_input_scale),
        convolution_kernel_taps,
        recurrence_gate_weight_blocks,
        input_gate_weight_blocks,
        lines(channel_decay_parameter),
        lines(token_extra_log_decay),
        row(mixing_output_scale),
        row(feedforward_norm_gain),
        lines(feedforward_gate_scale),
        lines(feedforward_up_scale),
        row(feedforward_down_scale),
    )
    return out.reshape(rows, half_width)


VMEM_BYTES = 60_000_000


def team_fits(mesh):
    sizes = mesh.shape
    return sizes["rep"] == 2 and sizes["tp"] == 2 and sizes["fs"] == 8


def solution(mesh):
    placed = (
        P(("rep", "fs"), "tp"),
        P(),
        P("fs", "tp"),
        P("tp"),
        P(None, "tp"),
        P("tp", None, None),
        P("tp", None, None),
        P("tp"),
        P(("rep", "fs")),
        P("tp", "fs"),
        P("fs"),
        P(),
        P("fs", "tp"),
        P("tp"),
        P("fs", "tp"),
        P("tp"),
        P("tp", "fs"),
        P("fs"),
    )

    def body(*args):
        blocks, hidden, rows = args[5].shape[0], args[12].shape[1], args[0].shape[0]
        if not team_fits(mesh) or blocks % 4 or hidden % 512 or rows % 64 or args[9].shape[1] % 256:
            return plain_body(*args)
        return team_body(*args)

    return jax.shard_map(
        body, mesh=mesh, in_specs=placed, out_specs=P(("rep", "fs"), "tp"), check_vma=False
    )
```

```python
import jax
import jax.numpy as jnp
from jax import lax
from jax.experimental import pallas as pl
from jax.experimental.pallas import tpu as pltpu
from jax.sharding import PartitionSpec as P

EPS = 1e-06
DECAY_FACTOR = 8.0


def row_norm(rows, gain_vec):
    values = rows.astype(jnp.float32)
    inverse = lax.rsqrt(jnp.mean(values * values, axis=-1, keepdims=True) + EPS)
    return (values * inverse * gain_vec).astype(jnp.bfloat16)


def gather_normed(rows, gain_vec):
    whole_rows = lax.all_gather(rows, "tp", axis=1, tiled=True)
    return row_norm(whole_rows, gain_vec)


def share_sums(terms):
    return lax.psum_scatter(
        terms.astype(jnp.bfloat16), "tp", scatter_dimension=1, tiled=True
    ).astype(jnp.float32)


def combine_pairs(earlier, later):
    decay_one, value_one = earlier
    decay_two, value_two = later
    return (decay_one * decay_two, decay_two * value_one + value_two)


def add_one(left_rows, weight_piece):
    return jnp.dot(left_rows, weight_piece, preferred_element_type=jnp.float32)


def place_columns(left_rows, total_now, pieces, start_row):
    weight_piece, scale_piece = pieces
    product = jnp.dot(left_rows, weight_piece, preferred_element_type=jnp.float32) * scale_piece
    return lax.dynamic_update_slice_in_dim(total_now, product, start_row, 1)


def plain_body(
    tokens,
    mixing_norm_gain,
    recurrent_input_weight,
    recurrent_input_scale,
    convolution_kernel_taps,
    recurrence_gate_weight_blocks,
    input_gate_weight_blocks,
    channel_decay_parameter,
    token_extra_log_decay,
    mixing_output_weight,
    mixing_output_scale,
    feedforward_norm_gain,
    feedforward_gate_weight,
    feedforward_gate_scale,
    feedforward_up_weight,
    feedforward_up_scale,
    feedforward_down_weight,
    feedforward_down_scale,
):
    normed = gather_normed(tokens, mixing_norm_gain)
    seq_rows = normed.shape[0]
    model_width = normed.shape[1]
    width_dev = recurrent_input_weight.shape[1]
    rec_sum = add_one(
        normed,
        lax.all_gather(recurrent_input_weight.astype(jnp.bfloat16), "fs", axis=0, tiled=True),
    )
    rec_input = (rec_sum * recurrent_input_scale).astype(jnp.bfloat16)
    rec_f32 = rec_input.astype(jnp.float32)
    tap_count = convolution_kernel_taps.shape[0]
    padded = jnp.pad(rec_f32, ((tap_count - 1, 0), (0, 0)))
    conv_out = jnp.zeros((seq_rows, width_dev), jnp.float32)
    for tap_index in range(tap_count):
        conv_out = (
            conv_out + convolution_kernel_taps[tap_index] * padded[tap_index : tap_index + seq_rows]
        )
    block_count = recurrence_gate_weight_blocks.shape[0]
    block_size = recurrence_gate_weight_blocks.shape[1]
    blocks = conv_out.astype(jnp.bfloat16).reshape(seq_rows, block_count, block_size)
    recurrence_gate_values = jax.nn.sigmoid(
        jnp.einsum(
            "lni,nij->lnj",
            blocks,
            recurrence_gate_weight_blocks,
            preferred_element_type=jnp.float32,
        ).reshape(seq_rows, width_dev)
    )
    input_gate = jax.nn.sigmoid(
        jnp.einsum(
            "lni,nij->lnj", blocks, input_gate_weight_blocks, preferred_element_type=jnp.float32
        ).reshape(seq_rows, width_dev)
    )
    decay_logarithm = (
        -DECAY_FACTOR * recurrence_gate_values * jax.nn.softplus(-channel_decay_parameter)
        + token_extra_log_decay[:, None]
    )
    decay = jnp.exp(decay_logarithm)
    drive = jnp.sqrt(-jnp.expm1(2.0 * decay_logarithm)) * input_gate * conv_out
    _, state = lax.associative_scan(combine_pairs, (decay, drive), axis=0)
    state_low = state.astype(jnp.bfloat16)
    mix_terms = place_columns(
        state_low,
        jnp.zeros((seq_rows, model_width), jnp.float32),
        (
            lax.all_gather(mixing_output_weight.astype(jnp.bfloat16), "fs", axis=1, tiled=True),
            lax.all_gather(
                mixing_output_scale.reshape(1, -1).astype(jnp.bfloat16), "fs", axis=1, tiled=True
            ).astype(jnp.float32),
        ),
        jnp.int32(0),
    )
    mixed = (tokens.astype(jnp.float32) + share_sums(mix_terms)).astype(jnp.bfloat16)
    normed_ffn = gather_normed(mixed, feedforward_norm_gain)
    gate_sum = add_one(
        normed_ffn,
        lax.all_gather(feedforward_gate_weight.astype(jnp.bfloat16), "fs", axis=0, tiled=True),
    )
    up_sum = add_one(
        normed_ffn,
        lax.all_gather(feedforward_up_weight.astype(jnp.bfloat16), "fs", axis=0, tiled=True),
    )
    hidden = (
        jax.nn.silu(gate_sum * feedforward_gate_scale) * (up_sum * feedforward_up_scale)
    ).astype(jnp.bfloat16)
    down_terms = place_columns(
        hidden,
        jnp.zeros((seq_rows, model_width), jnp.float32),
        (
            lax.all_gather(feedforward_down_weight.astype(jnp.bfloat16), "fs", axis=1, tiled=True),
            lax.all_gather(
                feedforward_down_scale.reshape(1, -1).astype(jnp.bfloat16), "fs", axis=1, tiled=True
            ).astype(jnp.float32),
        ),
        jnp.int32(0),
    )
    return (mixed.astype(jnp.float32) + share_sums(down_terms)).astype(jnp.bfloat16)


REC, MIX, GU, DOWN = range(4)
PIECES = ((0, 0), (1, 0), (2, 0), (2, 2), (3, 0), (3, 2), (3, 3))
LOW = jnp.bfloat16
F32 = jnp.float32


def remote(src, dst, send_sem, recv_sem, device):
    return pltpu.make_async_remote_copy(
        src_ref=src,
        dst_ref=dst,
        send_sem=send_sem,
        recv_sem=recv_sem,
        device_id=device,
        device_id_type=pl.DeviceIdType.MESH,
    )


def layer_kernel(
    tokens,
    w_rec,
    w_mix,
    w_gate,
    w_up,
    w_down,
    gain_one,
    rec_scale,
    taps,
    w_recur,
    w_input,
    decay_param,
    extra,
    mix_scale,
    gain_two,
    gate_scale,
    up_scale,
    down_scale,
    out,
    nbuf,
    rec_w,
    mix_w,
    gu_w,
    down_w,
    f_rec,
    f_mix,
    f_gu,
    f_down,
    y_rec,
    y_mix,
    y_gu,
    y_down,
    tk,
    mx,
    st,
    hid,
    ri,
    ext,
    ecol,
    oth,
    kept,
    rt,
    r1,
    r2,
    rd,
    rc,
    base_rows,
    oo,
    recur_blocks,
    input_blocks,
    load_sem,
    wl_recv,
    wy_send,
    wo_send,
    wf_send,
    w_recv,
    g_send,
    g_recv,
    tt_sem,
    ex_sem,
    m_send,
    m_recv,
    o_sem,
    c_send,
    c_recv,
):
    rows, half_width = tokens.shape
    half, part = rows // 2, rows // 4
    width = half_width * 2
    chans = rec_w.shape[2]
    units = down_w.shape[1]
    cols = mix_w.shape[2]
    unit = cols // 2
    block = recur_blocks.shape[1]
    tap_count = taps.shape[0]

    r, f, t = lax.axis_index("rep"), lax.axis_index("fs"), lax.axis_index("tp")
    y, z = lax.rem(f, 2), lax.div(f, 2)
    fp = f + 1 - 2 * y
    q = r * 2 + y
    own, own_x, own_y, own_d = q, (1 - r) * 2 + y, r * 2 + 1 - y, (1 - r) * 2 + 1 - y
    x_dev, y_dev, t_dev = {"rep": 1 - r}, {"fs": fp}, {"tp": 1 - t}
    d_dev = {"rep": 1 - r, "fs": fp}
    inner = lax.div(z + 1, 2) == 1
    near = (1 + lax.rem(z, 2), lax.rem(2 + 3 * z, 5))
    near = tuple({"fs": plane * 2 + y} for plane in near)
    planes = (z, z + 1 - 2 * lax.rem(z, 2), z + 2 - 4 * lax.div(z, 2), 3 - z)
    mats = (rec_w, mix_w, gu_w, down_w)
    top, low = pl.ds(0, part), pl.ds(part, part)

    barrier = pltpu.get_barrier_semaphore()

    def greet(device):
        pl.semaphore_signal(barrier, inc=1, device_id=device, device_id_type=pl.DeviceIdType.MESH)

    for device in (x_dev, y_dev, t_dev, d_dev, near[0]):
        greet(device)

    for device in (x_dev, y_dev, d_dev):
        greet({**device, "tp": 1 - t})

    @pl.when(inner)
    def _():
        greet({"fs": y})
        greet({"fs": 6 + y})

    quarters = (q, r * 2 + 1 - y)

    def load(number, src, dst):
        pltpu.make_async_copy(src, dst, load_sem.at[number]).start()

    def loaded(number, whole):
        pltpu.make_async_copy(whole, whole, load_sem.at[number]).wait()

    mine = pl.ds(pl.multiple_of(t * half, half), half)
    theirs = pl.ds(pl.multiple_of((1 - t) * half, half), half)
    side = pl.ds(pl.multiple_of(t * half_width, half_width), half_width)
    for i, piece in enumerate(quarters):
        at = pl.ds(pl.multiple_of(piece * chans, chans), chans)
        load(REC, w_rec.at[:, at], f_rec.at[i])
    load(4, tokens.at[mine, :], tk.at[:, side])
    for i, piece in enumerate(quarters):
        at = pl.ds(pl.multiple_of(piece * chans, chans), chans)
        load(MIX, w_mix.at[at, :], f_mix.at[i])
    for i, piece in enumerate(quarters):
        at = pl.ds(pl.multiple_of(piece * units, units), units)
        load(GU, w_gate.at[:, at], f_gu.at[i, 0])
        load(GU, w_up.at[:, at], f_gu.at[i, 1])
        load(DOWN, w_down.at[at, :], f_down.at[i])
    gate_blocks = pl.ds(q * (chans // block), chans // block)
    load(5, w_recur.at[gate_blocks], recur_blocks)
    load(6, w_input.at[gate_blocks], input_blocks)

    token_swap = remote(tokens.at[theirs, :], tk.at[:, side], tt_sem.at[0], tt_sem.at[1], t_dev)

    def block_copy(k, place, send_sem, device):
        view = mats[k].at[place]
        return remote(view, view, send_sem, w_recv.at[k, place], device)

    def wait_block(k, place):
        block_copy(k, place, wo_send.at[0], y_dev).wait_recv()

    def own_place(k, j):
        return z * 2 + j if k == DOWN else (f if j == 0 else fp)

    def send_own(k, j):
        if j == 1 and k != DOWN:
            wait_block(k, fp)
        for i in range(2):
            send_one(k, j, i)

    def send_one(k, j, i):
        block_copy(k, own_place(k, j), wo_send.at[k], near[i]).start()

    def sent(view, sem):
        remote(view, view, sem, w_recv.at[0, 0], y_dev).wait_send()

    y_bufs = (y_rec, y_mix, y_gu, y_down)

    def y_copy(k):
        return remote(y_bufs[k], mats[k].at[f], wy_send.at[k], w_recv.at[k, f], y_dev)

    def forward_copy(k, far, j):
        plane = 3 * (2 - z) if far else 3 - z
        place = plane * 2 + (j if k == DOWN else (y if j == 0 else 1 - y))
        edge = 3 * (z - 1)
        return place, block_copy(k, place, wf_send.at[k], {"fs": edge * 2 + y})

    def forward_copies(k, far, j):
        place, copy = forward_copy(k, far, j)
        if k == DOWN and far and j:
            return place, last_copies(place, {"fs": 3 * (z - 1) * 2 + y})
        return place, [copy]

    def forward(k, far, j):
        @pl.when(inner)
        def _():
            place, copies = forward_copies(k, far, j)
            wait_block(k, place)
            for copy in copies:
                copy.start()

    def last_copies(place, device):
        view = down_w.at[place]
        return [
            remote(
                view.at[:, pl.ds(i * unit, unit)],
                view.at[:, pl.ds(i * unit, unit)],
                wf_send.at[DOWN],
                wl_recv.at[i],
                device,
            )
            for i in range(2)
        ]

    def need(k, p, piece=(0, 4)):
        def wait():
            for j in range(2):
                if k == DOWN and p == 3 and j == 1:
                    for i, copy in enumerate(last_copies(planes[p] * 2 + j, y_dev)):
                        if piece[0] <= 2 + i < sum(piece):
                            copy.wait_recv()
                elif piece[0] <= 2 * j < sum(piece):
                    wait_block(k, planes[p] * 2 + j)

        if p == 1:
            wait()
        elif p > 1:
            pl.when(jnp.logical_not(inner))(wait)

    def norm_rows(src, gain):
        def step(i, carry):
            at = pl.ds(pl.multiple_of(i * 16, 16), 16)
            v = src[at, :].astype(F32)
            inverse = lax.rsqrt(jnp.mean(v * v, axis=-1, keepdims=True) + EPS)
            nbuf[own, t, at, :] = (v * inverse * gain[...]).astype(LOW)
            return carry

        lax.fori_loop(0, half // 16, step, 0)

    def rows_copy(phase, role):
        seq, at, device = (
            (own, top, x_dev),
            (own, low, x_dev),
            (own, top, y_dev),
            (own, low, y_dev),
            (own_y, top, x_dev),
            (own_x, low, y_dev),
            (own, pl.ds(0, half), t_dev),
            (own_x, top, t_dev),
            (own_x, low, t_dev),
            (own_y, top, t_dev),
            (own_y, low, t_dev),
            (own_d, top, t_dev),
            (own_d, low, t_dev),
        )[role]
        view = nbuf.at[seq, t, at, :]
        return remote(view, view, g_send.at[role // 7], g_recv.at[min(role, 6)], device)

    def rows_wait(phase, role):
        if role == 6:
            view = nbuf.at[:, 1 - t]
        else:
            seq, at = (
                (own_x, top),
                (own_x, low),
                (own_y, top),
                (own_y, low),
                (own_d, top),
                (own_d, low),
            )[role]
            view = nbuf.at[seq, t, at, :]
        remote(view, view, g_send.at[0], g_recv.at[role], t_dev).wait_recv()

    def gather_start(phase):
        for role in (1, 2, 0, 3, 6):
            rows_copy(phase, role).start()

    def gather_first(phase):
        rows_wait(phase, 2)
        rows_copy(phase, 4).start()
        rows_wait(phase, 1)
        rows_copy(phase, 5).start()
        rows_copy(phase, 9).start()
        rows_copy(phase, 8).start()

    def gather_second(phase):
        rows_wait(phase, 0)
        rows_copy(phase, 7).start()
        rows_wait(phase, 3)
        rows_copy(phase, 10).start()

    def gather_last(phase):
        rows_wait(phase, 4)
        rows_copy(phase, 11).start()
        rows_wait(phase, 5)
        rows_copy(phase, 12).start()
        rows_wait(phase, 6)
        sent(nbuf.at[pl.ds(0, 2)], g_send.at[0])
        sent(nbuf.at[pl.ds(0, 3), 0], g_send.at[1])

    def products(phase, p, left, weights, k, piece=(0, 4)):
        need(k, p, piece)
        first, size = planes[p] * 2, min(piece[1], 2)

        def product(side, start):
            rows_now = left[:, side].reshape(4 * half, left.shape[-1])
            column = start % 2 * unit
            weight = weights[first + start // 2, :, column : column + size * unit]
            value = jnp.dot(rows_now, weight, preferred_element_type=F32)
            return value.astype(LOW).reshape(4, half, size * unit)

        starts = range(piece[0], sum(piece), size)
        for start in starts:
            oth[p, :, :, start * unit : (start + size) * unit] = product(1 - t, start)
        sum_copies(phase, p, 0, piece).start()
        for start in starts:
            value = product(t, start).reshape(2, 2, half, size * unit)
            kept[p, :, :, :, start * unit : (start + size) * unit] = value

    def span_of(piece):
        return pl.ds(piece[0] * unit, piece[1] * unit)

    def sum_copies(phase, p, number, piece):
        at = span_of(piece)
        src, dst, device = (
            (oth.at[p, :, :, at], rt.at[phase, p, :, :, at], t_dev),
            (kept.at[p, 1 - r, :, top, at], r1.at[phase, p, 0, :, :, at], x_dev),
            (kept.at[p, :, 1 - y, low, at], r1.at[phase, p, 1, :, :, at], y_dev),
            (kept.at[p, r, 1 - y, top, at], r2.at[phase, p, 0, :, at], y_dev),
            (kept.at[p, 1 - r, y, low, at], r2.at[phase, p, 1, :, at], x_dev),
        )[number]
        return remote(src, dst, *sum_sems(phase, p, number, piece), device)

    def sum_sems(phase, p, number, piece):
        place = PIECES.index((p, piece[0])) if phase else p
        return m_send.at[place, min(number, 1)], m_recv.at[4 * phase + place, number]

    def direct_copy(p, number, piece):
        at, device = span_of(piece), (x_dev, y_dev, d_dev)[number]
        a, b = ((1 - r, y), (r, 1 - y), (1 - r, 1 - y))[number]
        src, dst = kept.at[p, a, b, :, at], rd.at[piece[0] % 2, number]
        return remote(src, dst, *sum_sems(1, p, 1 + number, piece), device)

    holder = lax.div(planes[3], 2)
    collects = t == holder

    def collect_copy(number):
        a, b = ((1 - r, y), (r, 1 - y), (1 - r, 1 - y), (r, y))[number]
        device = {**(x_dev, y_dev, d_dev, {})[number], "tp": holder}
        if number == 3:
            device = t_dev
        send = c_send.at[0] if number == 3 else sum_sems(1, 3, 1, (3, 1))[0]
        src = kept.at[3, a, b, :, span_of((3, 1))]
        return remote(src, rc.at[t, number], send, c_recv.at[t, number], device)

    def base_copy():
        src = mx.at[:, columns_of(planes[3], (3, 1))]
        return remote(src, base_rows, c_send.at[1], c_send.at[2], t_dev)

    def collected(side, number):
        view = rc.at[side, number]
        remote(view, view, c_send.at[0], c_recv.at[side, number], t_dev).wait_recv()
        return rc[side, number].astype(F32)

    def collect_done():
        piece = (3, 1)
        at = columns_of(lax.rem(planes[3], 2), piece)

        @pl.when(collects)
        def _():
            total = kept[3, r, y, :, span_of(piece)].astype(F32)
            for number in range(3):
                total = total + collected(t, number)
            base = mx[:, columns_of(planes[3], piece)].astype(F32)
            out[t, :, at] = (base + total).astype(LOW)
            base_copy().wait_recv()
            total = collected(1 - t, 3)
            for number in range(3):
                total = total + collected(1 - t, number)
            out[1 - t, :, at] = (base_rows[...].astype(F32) + total).astype(LOW)

        @pl.when(jnp.logical_not(collects))
        def _():
            collect_copy(3).wait_send()
            base_copy().wait_send()

        sums_sent(1, 3, piece)

    def pair_sums(phase, p, piece=(0, 4)):
        sum_copies(phase, p, 0, piece).wait_recv()
        at = span_of(piece)

        def step(s, carry):
            a, b = lax.div(s, 2), lax.rem(s, 2)
            value = kept[p, a, b, :, at].astype(F32) + rt[phase, p, s, :, at].astype(F32)
            kept[p, a, b, :, at] = value.astype(LOW)
            return carry

        lax.fori_loop(0, 4, step, 0)
        if piece == (3, 1):
            for number in (2, 0, 1):
                collect_copy(number).start()
            pl.when(jnp.logical_not(collects))(lambda: collect_copy(3).start())
        elif piece[1] == 1:
            for number in (2, 0, 1):
                direct_copy(p, number, piece).start()
        else:
            sum_copies(phase, p, 1, piece).start()
            sum_copies(phase, p, 2, piece).start()

    def line_sums(phase, p, piece=(0, 4)):
        at = span_of(piece)
        sum_copies(phase, p, 1, piece).wait_recv()
        for i in range(2):
            value = kept[p, r, i, top, at].astype(F32) + r1[phase, p, 0, i, :, at].astype(F32)
            kept[p, r, i, top, at] = value.astype(LOW)
        sum_copies(phase, p, 3, piece).start()
        sum_copies(phase, p, 2, piece).wait_recv()
        for i in range(2):
            value = kept[p, i, y, low, at].astype(F32) + r1[phase, p, 1, i, :, at].astype(F32)
            kept[p, i, y, low, at] = value.astype(LOW)
        sum_copies(phase, p, 4, piece).start()

    def columns_of(plane, piece):
        start = pl.multiple_of((plane * 4 + piece[0]) * unit, unit)
        return pl.ds(start, piece[1] * unit)

    def sums_sent(phase, p, piece):
        sum_copies(phase, p, 0, piece).wait_send()
        view = oth.at[p, pl.ds(0, 3), :, span_of(piece)]
        sent(view, sum_sems(phase, p, 1, piece)[0])

    def last_sums(phase, p, base, piece):
        at, inside = columns_of(planes[p], piece), span_of(piece)
        if piece[1] == 1:
            total = kept[p, r, y, :, inside].astype(F32)
            for number in range(3):
                direct_copy(p, number, piece).wait_recv()
                total = total + rd[piece[0] % 2, number].astype(F32)
            value = (base[:, at].astype(F32) + total).astype(LOW)
            sums_sent(phase, p, piece)
            return at, [value[:part], value[part:]]
        values = []
        for i, number in enumerate((3, 4)):
            span = slice(i * part, (i + 1) * part)
            sum_copies(phase, p, number, piece).wait_recv()
            value = kept[p, r, y, span, inside].astype(F32) + r2[phase, p, i, :, inside].astype(F32)
            values.append((base[span, at].astype(F32) + value).astype(LOW))
        sums_sent(phase, p, piece)
        return at, values

    def mix_done(p):
        at, values = last_sums(0, p, tk, (0, 4))
        for i, value in enumerate(values):
            mx[i * part : (i + 1) * part, at] = value

    def out_copy(p, piece):
        at = columns_of(lax.rem(planes[p], 2), piece)
        src = oo.at[p, :, span_of(piece)]
        return remote(src, out.at[t, :, at], o_sem.at[0], o_sem.at[1], t_dev)

    def down_done(p, piece=(0, 4)):
        _, values = last_sums(1, p, mx, piece)
        local = lax.div(planes[p], 2) == t
        at = columns_of(lax.rem(planes[p], 2), piece)

        @pl.when(local)
        def _():
            for i, value in enumerate(values):
                out[t, i * part : (i + 1) * part, at] = value

        @pl.when(jnp.logical_not(local))
        def _():
            for i, value in enumerate(values):
                oo[p, i * part : (i + 1) * part, span_of(piece)] = value
            out_copy(p, piece).start()

    loaded(REC, f_rec)
    y_rec[...] = f_rec[1].astype(LOW)
    rec_w[f] = f_rec[0].astype(LOW)
    pl.semaphore_wait(barrier, 9)
    token_swap.start()
    y_copy(REC).start()
    send_own(REC, 0)
    loaded(4, tk.at[:, side])
    token_swap.wait()
    norm_rows(tk, gain_one)
    gather_start(0)

    loaded(MIX, f_mix)
    y_mix[...] = (f_mix[1] * mix_scale[...]).astype(LOW)
    mix_w[f] = (f_mix[0] * mix_scale[...]).astype(LOW)


    @pl.when(inner)
    def _():
        send_one(MIX, 0, 1)

    send_own(REC, 1)
    for i in range(extra.shape[0]):
        lanes = slice(i * block, (i + 1) * block)
        ext[own, :, lanes] = jnp.broadcast_to(extra[i : i + 1, :], (ext.shape[1], block))
    ext_copies = [
        remote(ext.at[own], ext.at[own], ex_sem.at[0], ex_sem.at[1], device)
        for device in (x_dev, y_dev, d_dev)
    ]
    for copy in ext_copies:
        copy.start()
    loaded(GU, f_gu)
    loaded(DOWN, f_down)
    for i in range(2):
        y_gu[:, i * units : (i + 1) * units] = f_gu[1, i].astype(LOW)
        gu_w[f, :, i * units : (i + 1) * units] = f_gu[0, i].astype(LOW)
    y_down[...] = (f_down[1] * down_scale[...]).astype(LOW)
    down_w[f] = (f_down[0] * down_scale[...]).astype(LOW)

    send_one(MIX, 0, 0)

    @pl.when(jnp.logical_not(inner))
    def _():
        send_one(MIX, 0, 1)

    forward(REC, 0, 0)
    forward(REC, 1, 0)
    gather_first(0)
    y_copy(MIX).start()
    y_copy(GU).start()
    y_copy(DOWN).start()
    forward(REC, 0, 1)
    forward(REC, 1, 1)
    gather_second(0)
    forward(MIX, 0, 0)
    forward(MIX, 1, 0)
    gather_last(0)
    three = ext.at[pl.ds(0, 3)]
    remote(three, three, ex_sem.at[0], ex_sem.at[1], t_dev).wait_recv()
    for p in range(1, 4):
        need(REC, p)
    loaded(5, recur_blocks)
    loaded(6, input_blocks)

    at_chans = pl.multiple_of(q * chans, chans)

    def recur(s, carry):
        @pl.when(s == 1)
        def _():
            send_own(MIX, 1)
            send_own(GU, 0)

        @pl.when(s == 2)
        def _():
            forward(MIX, 0, 1)

        @pl.when(s == 3)
        def _():
            forward(MIX, 1, 1)

        left = nbuf[s].reshape(rows, width)
        total = jnp.dot(left, rec_w[...].reshape(width, chans), preferred_element_type=F32)
        for b in range(chans // block):
            here = slice(b * block, (b + 1) * block)
            number = q * (chans // block) + b
            ri[:, here] = (total[:, here] * rec_scale[pl.ds(number, 1), :]).astype(LOW)
        ecol[...] = jnp.broadcast_to(ext[s, 0:1, :], (block, rows)).T
        for b in range(chans // block):
            here = slice(b * block, (b + 1) * block)
            lanes = pl.ds(pl.multiple_of(at_chans + b * block, block), block)
            number = q * (chans // block) + b
            values = ri[:, here].astype(F32)
            places = lax.broadcasted_iota(jnp.int32, values.shape, 0)
            conv_out = taps[tap_count - 1 : tap_count, lanes] * values
            for back in range(1, tap_count):
                moved = jnp.where(places >= back, pltpu.roll(values, back, 0), 0.0)
                tap = tap_count - 1 - back
                conv_out = conv_out + taps[tap : tap + 1, lanes] * moved
            conv_low = conv_out.astype(LOW)
            recur_gate = jax.nn.sigmoid(
                jnp.dot(conv_low, recur_blocks[b], preferred_element_type=F32)
            )
            input_gate = jax.nn.sigmoid(
                jnp.dot(conv_low, input_blocks[b], preferred_element_type=F32)
            )
            param = -decay_param[pl.ds(number, 1), :]
            soft = jnp.maximum(param, 0.0) + jnp.log1p(jnp.exp(-jnp.abs(param)))
            log_decay = -DECAY_FACTOR * recur_gate * soft + ecol[...]
            decay = jnp.exp(log_decay)
            drive = jnp.sqrt(-jnp.tanh(log_decay) * (1.0 + decay * decay)) * input_gate * conv_out
            step = 1
            while step < rows:
                keep = places >= step
                drive = drive + decay * jnp.where(keep, pltpu.roll(drive, step, 0), 0.0)
                if step * 2 < rows:
                    decay = decay * jnp.where(keep, pltpu.roll(decay, step, 0), 1.0)
                step *= 2
            state = drive.astype(LOW)
            st[s, 0, :, here] = state[:half]
            st[s, 1, :, here] = state[half:]
        return carry

    lax.fori_loop(0, 4, recur, 0)

    products(0, 0, st, mix_w, MIX)
    products(0, 1, st, mix_w, MIX)
    pair_sums(0, 0)
    send_own(GU, 1)
    pair_sums(0, 1)
    products(0, 2, st, mix_w, MIX)
    line_sums(0, 0)
    pair_sums(0, 2)
    line_sums(0, 1)
    products(0, 3, st, mix_w, MIX)
    mix_done(0)
    pair_sums(0, 3)
    forward(GU, 0, 0)
    line_sums(0, 2)
    mix_done(1)
    forward(GU, 1, 0)
    line_sums(0, 3)
    mix_done(2)
    mix_done(3)

    norm_rows(mx, gain_two)
    gather_start(1)
    pl.when(jnp.logical_not(collects))(lambda: base_copy().start())
    gather_first(1)
    wait_block(DOWN, fp)
    forward(GU, 0, 1)
    gather_second(1)
    forward(GU, 1, 1)
    gather_last(1)
    send_own(DOWN, 0)
    send_own(DOWN, 1)
    for p in range(1, 4):
        need(GU, p)

    unit_rows = units // block

    def unit_scales(scale):
        first = q * unit_rows
        return jnp.concatenate([scale[pl.ds(first + i, 1), :] for i in range(unit_rows)], 1)

    def hidden(s, carry):
        left = nbuf[s].reshape(rows, width)
        total = jnp.dot(left, gu_w[...].reshape(width, 2 * units), preferred_element_type=F32)
        gate = total[:, :units] * unit_scales(gate_scale)
        up = total[:, units:] * unit_scales(up_scale)
        value = (gate * jax.nn.sigmoid(gate) * up).astype(LOW)
        hid[s, 0] = value[:half]
        hid[s, 1] = value[half:]
        return carry

    lax.fori_loop(0, 4, hidden, 0)

    first, second, third, fourth = (0, 2), (2, 2), (2, 1), (3, 1)

    def down_products(p, piece=(0, 4)):
        products(1, p, hid, down_w, DOWN, piece)

    down_products(0)
    pair_sums(1, 0)
    down_products(1)
    forward(DOWN, 0, 0)
    pair_sums(1, 1)
    line_sums(1, 0)
    forward(DOWN, 0, 1)
    forward(DOWN, 1, 0)
    down_products(2, first)
    pair_sums(1, 2, first)
    down_done(0)
    line_sums(1, 1)
    line_sums(1, 2, first)
    forward(DOWN, 1, 1)
    down_products(2, second)
    pair_sums(1, 2, second)
    down_done(1)
    down_done(2, first)
    line_sums(1, 2, second)
    down_products(3, first)
    pair_sums(1, 3, first)
    down_products(3, third)
    down_done(2, second)
    pair_sums(1, 3, third)
    line_sums(1, 3, first)
    down_products(3, fourth)
    pair_sums(1, 3, fourth)
    down_done(3, first)
    down_done(3, third)
    collect_done()

    whole, less = out.at[1 - t], out.at[1 - t, :, pl.ds(0, half_width - unit)]
    whole = remote(whole, whole, o_sem.at[0], o_sem.at[1], t_dev)
    less = remote(less, less, o_sem.at[0], o_sem.at[1], t_dev)

    @pl.when(collects)
    def _():
        less.wait_recv()
        whole.wait_send()

    @pl.when(jnp.logical_not(collects))
    def _():
        whole.wait_recv()
        less.wait_send()

    for k in range(4):
        y_copy(k).wait_send()
        sent(mats[k].at[pl.ds(0, 4)], wo_send.at[k])

        @pl.when(inner)
        def _():
            sent(mats[k].at[pl.ds(0, 4)], wf_send.at[k])

    sent(ext.at[pl.ds(0, 3)], ex_sem.at[0])


def team_body(
    tokens,
    mixing_norm_gain,
    recurrent_input_weight,
    recurrent_input_scale,
    convolution_kernel_taps,
    recurrence_gate_weight_blocks,
    input_gate_weight_blocks,
    channel_decay_parameter,
    token_extra_log_decay,
    mixing_output_weight,
    mixing_output_scale,
    feedforward_norm_gain,
    feedforward_gate_weight,
    feedforward_gate_scale,
    feedforward_up_weight,
    feedforward_up_scale,
    feedforward_down_weight,
    feedforward_down_scale,
):
    rows, half_width = tokens.shape
    half, part = rows // 2, rows // 4
    width = half_width * 2
    depth = recurrent_input_weight.shape[0]
    chans = recurrent_input_weight.shape[1] // 4
    units = feedforward_gate_weight.shape[1] // 4
    cols = mixing_output_weight.shape[1]
    block = recurrence_gate_weight_blocks.shape[1]
    planes = width // depth
    any_spec = pl.BlockSpec(memory_space=pl.ANY)
    vmem_spec = pl.BlockSpec(memory_space=pltpu.VMEM)
    vmem = pltpu.VMEM
    dma = pltpu.SemaphoreType.DMA

    def row(vector):
        return vector.reshape(1, -1)

    def lines(vector):
        return vector.reshape(-1, block)

    out = pl.pallas_call(
        layer_kernel,
        out_shape=vmem((2, half, half_width), LOW),
        in_specs=[any_spec] * 6 + [vmem_spec] * 3 + [any_spec] * 2 + [vmem_spec] * 7,
        out_specs=vmem_spec,
        scratch_shapes=[
            vmem((4, 2, half, width), LOW),
            vmem((planes, depth, chans), LOW),
            vmem((planes, chans, cols), LOW),
            vmem((planes, depth, 2 * units), LOW),
            vmem((planes, units, cols), LOW),
            vmem((2, depth, chans), F32),
            vmem((2, chans, cols), F32),
            vmem((2, 2, depth, units), F32),
            vmem((2, units, cols), F32),
            vmem((depth, chans), LOW),
            vmem((chans, cols), LOW),
            vmem((depth, 2 * units), LOW),
            vmem((units, cols), LOW),
            vmem((half, width), LOW),
            vmem((half, width), LOW),
            vmem((4, 2, half, chans), LOW),
            vmem((4, 2, half, units), LOW),
            vmem((rows, chans), LOW),
            vmem((4, 8, rows), F32),
            vmem((rows, block), F32),
            vmem((4, 4, half, 2 * cols), LOW),
            vmem((4, 2, 2, half, 2 * cols), LOW),
            vmem((2, 4, 4, half, 2 * cols), LOW),
            vmem((2, 4, 2, 2, part, 2 * cols), LOW),
            vmem((2, 4, 2, part, 2 * cols), LOW),
            vmem((2, 3, half, cols // 2), LOW),
            vmem((2, 4, half, cols // 2), LOW),
            vmem((half, cols // 2), LOW),
            vmem((4, half, 2 * cols), LOW),
            vmem((chans // block, block, block), LOW),
            vmem((chans // block, block, block), LOW),
            dma((7,)),
            dma((2,)),
            dma((4,)),
            dma((4,)),
            dma((4,)),
            dma((4, planes)),
            dma((2,)),
            dma((7,)),
            dma((2,)),
            dma((2,)),
            dma((len(PIECES), 2)),
            dma((4 + len(PIECES), 5)),
            dma((2,)),
            dma((3,)),
            dma((2, 4)),
        ],
        compiler_params=pltpu.CompilerParams(
            collective_id=0, has_side_effects=True, vmem_limit_bytes=VMEM_BYTES
        ),
    )(
        tokens,
        recurrent_input_weight,
        mixing_output_weight,
        feedforward_gate_weight,
        feedforward_up_weight,
        feedforward_down_weight,
        row(mixing_norm_gain),
        lines(recurrent_input_scale),
        convolution_kernel_taps,
        recurrence_gate_weight_blocks,
        input_gate_weight_blocks,
        lines(channel_decay_parameter),
        lines(token_extra_log_decay),
        row(mixing_output_scale),
        row(feedforward_norm_gain),
        lines(feedforward_gate_scale),
        lines(feedforward_up_scale),
        row(feedforward_down_scale),
    )
    return out.reshape(rows, half_width)


VMEM_BYTES = 60_000_000


def team_fits(mesh):
    sizes = mesh.shape
    return sizes["rep"] == 2 and sizes["tp"] == 2 and sizes["fs"] == 8


def solution(mesh):
    placed = (
        P(("rep", "fs"), "tp"),
        P(),
        P("fs", "tp"),
        P("tp"),
        P(None, "tp"),
        P("tp", None, None),
        P("tp", None, None),
        P("tp"),
        P(("rep", "fs")),
        P("tp", "fs"),
        P("fs"),
        P(),
        P("fs", "tp"),
        P("tp"),
        P("fs", "tp"),
        P("tp"),
        P("tp", "fs"),
        P("fs"),
    )

    def body(*args):
        blocks, hidden, rows = args[5].shape[0], args[12].shape[1], args[0].shape[0]
        if not team_fits(mesh) or blocks % 4 or hidden % 512 or rows % 64 or args[9].shape[1] % 256:
            return plain_body(*args)
        return team_body(*args)

    return jax.shard_map(
        body, mesh=mesh, in_specs=placed, out_specs=P(("rep", "fs"), "tp"), check_vma=False
    )
```

```python
import jax
import jax.numpy as jnp
from jax import lax
from jax.experimental import pallas as pl
from jax.experimental.pallas import tpu as pltpu
from jax.sharding import PartitionSpec as P

EPS = 1e-06
DECAY_FACTOR = 8.0


def row_norm(rows, gain_vec):
    values = rows.astype(jnp.float32)
    inverse = lax.rsqrt(jnp.mean(values * values, axis=-1, keepdims=True) + EPS)
    return (values * inverse * gain_vec).astype(jnp.bfloat16)


def gather_normed(rows, gain_vec):
    whole_rows = lax.all_gather(rows, "tp", axis=1, tiled=True)
    return row_norm(whole_rows, gain_vec)


def share_sums(terms):
    return lax.psum_scatter(
        terms.astype(jnp.bfloat16), "tp", scatter_dimension=1, tiled=True
    ).astype(jnp.float32)


def combine_pairs(earlier, later):
    decay_one, value_one = earlier
    decay_two, value_two = later
    return (decay_one * decay_two, decay_two * value_one + value_two)


def add_one(left_rows, weight_piece):
    return jnp.dot(left_rows, weight_piece, preferred_element_type=jnp.float32)


def place_columns(left_rows, total_now, pieces, start_row):
    weight_piece, scale_piece = pieces
    product = jnp.dot(left_rows, weight_piece, preferred_element_type=jnp.float32) * scale_piece
    return lax.dynamic_update_slice_in_dim(total_now, product, start_row, 1)


def plain_body(
    tokens,
    mixing_norm_gain,
    recurrent_input_weight,
    recurrent_input_scale,
    convolution_kernel_taps,
    recurrence_gate_weight_blocks,
    input_gate_weight_blocks,
    channel_decay_parameter,
    token_extra_log_decay,
    mixing_output_weight,
    mixing_output_scale,
    feedforward_norm_gain,
    feedforward_gate_weight,
    feedforward_gate_scale,
    feedforward_up_weight,
    feedforward_up_scale,
    feedforward_down_weight,
    feedforward_down_scale,
):
    normed = gather_normed(tokens, mixing_norm_gain)
    seq_rows = normed.shape[0]
    model_width = normed.shape[1]
    width_dev = recurrent_input_weight.shape[1]
    rec_sum = add_one(
        normed,
        lax.all_gather(recurrent_input_weight.astype(jnp.bfloat16), "fs", axis=0, tiled=True),
    )
    rec_input = (rec_sum * recurrent_input_scale).astype(jnp.bfloat16)
    rec_f32 = rec_input.astype(jnp.float32)
    tap_count = convolution_kernel_taps.shape[0]
    padded = jnp.pad(rec_f32, ((tap_count - 1, 0), (0, 0)))
    conv_out = jnp.zeros((seq_rows, width_dev), jnp.float32)
    for tap_index in range(tap_count):
        conv_out = (
            conv_out + convolution_kernel_taps[tap_index] * padded[tap_index : tap_index + seq_rows]
        )
    block_count = recurrence_gate_weight_blocks.shape[0]
    block_size = recurrence_gate_weight_blocks.shape[1]
    blocks = conv_out.astype(jnp.bfloat16).reshape(seq_rows, block_count, block_size)
    recurrence_gate_values = jax.nn.sigmoid(
        jnp.einsum(
            "lni,nij->lnj",
            blocks,
            recurrence_gate_weight_blocks,
            preferred_element_type=jnp.float32,
        ).reshape(seq_rows, width_dev)
    )
    input_gate = jax.nn.sigmoid(
        jnp.einsum(
            "lni,nij->lnj", blocks, input_gate_weight_blocks, preferred_element_type=jnp.float32
        ).reshape(seq_rows, width_dev)
    )
    decay_logarithm = (
        -DECAY_FACTOR * recurrence_gate_values * jax.nn.softplus(-channel_decay_parameter)
        + token_extra_log_decay[:, None]
    )
    decay = jnp.exp(decay_logarithm)
    drive = jnp.sqrt(-jnp.expm1(2.0 * decay_logarithm)) * input_gate * conv_out
    _, state = lax.associative_scan(combine_pairs, (decay, drive), axis=0)
    state_low = state.astype(jnp.bfloat16)
    mix_terms = place_columns(
        state_low,
        jnp.zeros((seq_rows, model_width), jnp.float32),
        (
            lax.all_gather(mixing_output_weight.astype(jnp.bfloat16), "fs", axis=1, tiled=True),
            lax.all_gather(
                mixing_output_scale.reshape(1, -1).astype(jnp.bfloat16), "fs", axis=1, tiled=True
            ).astype(jnp.float32),
        ),
        jnp.int32(0),
    )
    mixed = (tokens.astype(jnp.float32) + share_sums(mix_terms)).astype(jnp.bfloat16)
    normed_ffn = gather_normed(mixed, feedforward_norm_gain)
    gate_sum = add_one(
        normed_ffn,
        lax.all_gather(feedforward_gate_weight.astype(jnp.bfloat16), "fs", axis=0, tiled=True),
    )
    up_sum = add_one(
        normed_ffn,
        lax.all_gather(feedforward_up_weight.astype(jnp.bfloat16), "fs", axis=0, tiled=True),
    )
    hidden = (
        jax.nn.silu(gate_sum * feedforward_gate_scale) * (up_sum * feedforward_up_scale)
    ).astype(jnp.bfloat16)
    down_terms = place_columns(
        hidden,
        jnp.zeros((seq_rows, model_width), jnp.float32),
        (
            lax.all_gather(feedforward_down_weight.astype(jnp.bfloat16), "fs", axis=1, tiled=True),
            lax.all_gather(
                feedforward_down_scale.reshape(1, -1).astype(jnp.bfloat16), "fs", axis=1, tiled=True
            ).astype(jnp.float32),
        ),
        jnp.int32(0),
    )
    return (mixed.astype(jnp.float32) + share_sums(down_terms)).astype(jnp.bfloat16)


REC, MIX, GU, DOWN = range(4)
PIECES = ((0, 0), (1, 0), (2, 0), (2, 2), (3, 0), (3, 2), (3, 3))
LOW = jnp.bfloat16
F32 = jnp.float32


def remote(src, dst, send_sem, recv_sem, device):
    return pltpu.make_async_remote_copy(
        src_ref=src,
        dst_ref=dst,
        send_sem=send_sem,
        recv_sem=recv_sem,
        device_id=device,
        device_id_type=pl.DeviceIdType.MESH,
    )


def layer_kernel(
    tokens,
    w_rec,
    w_mix,
    w_gate,
    w_up,
    w_down,
    gain_one,
    rec_scale,
    taps,
    w_recur,
    w_input,
    decay_param,
    extra,
    mix_scale,
    gain_two,
    gate_scale,
    up_scale,
    down_scale,
    out,
    nbuf,
    rec_w,
    mix_w,
    gu_w,
    down_w,
    f_rec,
    f_mix,
    f_gu,
    f_down,
    y_rec,
    y_mix,
    y_gu,
    y_down,
    tk,
    mx,
    st,
    hid,
    ri,
    ext,
    ecol,
    oth,
    kept,
    rt,
    r1,
    r2,
    rd,
    rc,
    base_rows,
    oo,
    recur_blocks,
    input_blocks,
    load_sem,
    wl_recv,
    wy_send,
    wo_send,
    wf_send,
    w_recv,
    g_send,
    g_recv,
    tt_sem,
    ex_sem,
    m_send,
    m_recv,
    o_sem,
    c_send,
    c_recv,
):
    rows, half_width = tokens.shape
    half, part = rows // 2, rows // 4
    width = half_width * 2
    chans = rec_w.shape[2]
    units = down_w.shape[1]
    cols = mix_w.shape[2]
    unit = cols // 2
    block = recur_blocks.shape[1]
    tap_count = taps.shape[0]

    r, f, t = lax.axis_index("rep"), lax.axis_index("fs"), lax.axis_index("tp")
    y, z = lax.rem(f, 2), lax.div(f, 2)
    fp = f + 1 - 2 * y
    q = r * 2 + y
    own, own_x, own_y, own_d = q, (1 - r) * 2 + y, r * 2 + 1 - y, (1 - r) * 2 + 1 - y
    x_dev, y_dev, t_dev = {"rep": 1 - r}, {"fs": fp}, {"tp": 1 - t}
    d_dev = {"rep": 1 - r, "fs": fp}
    inner = lax.div(z + 1, 2) == 1
    near = (1 + lax.rem(z, 2), lax.rem(2 + 3 * z, 5))
    near = tuple({"fs": plane * 2 + y} for plane in near)
    planes = (z, z + 1 - 2 * lax.rem(z, 2), z + 2 - 4 * lax.div(z, 2), 3 - z)
    mats = (rec_w, mix_w, gu_w, down_w)
    top, low = pl.ds(0, part), pl.ds(part, part)

    barrier = pltpu.get_barrier_semaphore()

    def greet(device):
        pl.semaphore_signal(barrier, inc=1, device_id=device, device_id_type=pl.DeviceIdType.MESH)

    for device in (x_dev, y_dev, t_dev, d_dev, near[0]):
        greet(device)

    for device in (x_dev, y_dev, d_dev):
        greet({**device, "tp": 1 - t})

    @pl.when(inner)
    def _():
        greet({"fs": y})
        greet({"fs": 6 + y})

    quarters = (q, r * 2 + 1 - y)

    def load(number, src, dst):
        pltpu.make_async_copy(src, dst, load_sem.at[number]).start()

    def loaded(number, whole):
        pltpu.make_async_copy(whole, whole, load_sem.at[number]).wait()

    mine = pl.ds(pl.multiple_of(t * half, half), half)
    theirs = pl.ds(pl.multiple_of((1 - t) * half, half), half)
    side = pl.ds(pl.multiple_of(t * half_width, half_width), half_width)
    for i, piece in enumerate(quarters):
        at = pl.ds(pl.multiple_of(piece * chans, chans), chans)
        load(REC, w_rec.at[:, at], f_rec.at[i])
    load(4, tokens.at[mine, :], tk.at[:, side])
    for i, piece in enumerate(quarters):
        at = pl.ds(pl.multiple_of(piece * chans, chans), chans)
        load(MIX, w_mix.at[at, :], f_mix.at[i])
    for i, piece in enumerate(quarters):
        at = pl.ds(pl.multiple_of(piece * units, units), units)
        load(GU, w_gate.at[:, at], f_gu.at[i, 0])
        load(GU, w_up.at[:, at], f_gu.at[i, 1])
        load(DOWN, w_down.at[at, :], f_down.at[i])
    gate_blocks = pl.ds(q * (chans // block), chans // block)
    load(5, w_recur.at[gate_blocks], recur_blocks)
    load(6, w_input.at[gate_blocks], input_blocks)

    token_swap = remote(tokens.at[theirs, :], tk.at[:, side], tt_sem.at[0], tt_sem.at[1], t_dev)

    def block_copy(k, place, send_sem, device):
        view = mats[k].at[place]
        return remote(view, view, send_sem, w_recv.at[k, place], device)

    def wait_block(k, place):
        block_copy(k, place, wo_send.at[0], y_dev).wait_recv()

    def own_place(k, j):
        return z * 2 + j if k == DOWN else (f if j == 0 else fp)

    def send_own(k, j):
        if j == 1 and k != DOWN:
            wait_block(k, fp)
        for i in range(2):
            send_one(k, j, i)

    def send_one(k, j, i):
        block_copy(k, own_place(k, j), wo_send.at[k], near[i]).start()

    def sent(view, sem):
        remote(view, view, sem, w_recv.at[0, 0], y_dev).wait_send()

    y_bufs = (y_rec, y_mix, y_gu, y_down)

    def y_copy(k):
        return remote(y_bufs[k], mats[k].at[f], wy_send.at[k], w_recv.at[k, f], y_dev)

    def forward_copy(k, far, j):
        plane = 3 * (2 - z) if far else 3 - z
        place = plane * 2 + (j if k == DOWN else (y if j == 0 else 1 - y))
        edge = 3 * (z - 1)
        return place, block_copy(k, place, wf_send.at[k], {"fs": edge * 2 + y})

    def forward_copies(k, far, j):
        place, copy = forward_copy(k, far, j)
        if k == DOWN and far and j:
            return place, last_copies(place, {"fs": 3 * (z - 1) * 2 + y})
        return place, [copy]

    def forward(k, far, j):
        @pl.when(inner)
        def _():
            place, copies = forward_copies(k, far, j)
            wait_block(k, place)
            for copy in copies:
                copy.start()

    def last_copies(place, device):
        view = down_w.at[place]
        return [
            remote(
                view.at[:, pl.ds(i * unit, unit)],
                view.at[:, pl.ds(i * unit, unit)],
                wf_send.at[DOWN],
                wl_recv.at[i],
                device,
            )
            for i in range(2)
        ]

    def need(k, p, piece=(0, 4)):
        def wait():
            for j in range(2):
                if k == DOWN and p == 3 and j == 1:
                    for i, copy in enumerate(last_copies(planes[p] * 2 + j, y_dev)):
                        if piece[0] <= 2 + i < sum(piece):
                            copy.wait_recv()
                elif piece[0] <= 2 * j < sum(piece):
                    wait_block(k, planes[p] * 2 + j)

        if p == 1:
            wait()
        elif p > 1:
            pl.when(jnp.logical_not(inner))(wait)

    def norm_rows(src, gain):
        def step(i, carry):
            at = pl.ds(pl.multiple_of(i * 16, 16), 16)
            v = src[at, :].astype(F32)
            inverse = lax.rsqrt(jnp.mean(v * v, axis=-1, keepdims=True) + EPS)
            nbuf[own, t, at, :] = (v * inverse * gain[...]).astype(LOW)
            return carry

        lax.fori_loop(0, half // 16, step, 0)

    def rows_copy(phase, role):
        seq, at, device = (
            (own, top, x_dev),
            (own, low, x_dev),
            (own, top, y_dev),
            (own, low, y_dev),
            (own_y, top, x_dev),
            (own_x, low, y_dev),
            (own, pl.ds(0, half), t_dev),
            (own_x, top, t_dev),
            (own_x, low, t_dev),
            (own_y, top, t_dev),
            (own_y, low, t_dev),
            (own_d, top, t_dev),
            (own_d, low, t_dev),
        )[role]
        view = nbuf.at[seq, t, at, :]
        return remote(view, view, g_send.at[role // 7], g_recv.at[min(role, 6)], device)

    def rows_wait(phase, role):
        if role == 6:
            view = nbuf.at[:, 1 - t]
        else:
            seq, at = (
                (own_x, top),
                (own_x, low),
                (own_y, top),
                (own_y, low),
                (own_d, top),
                (own_d, low),
            )[role]
            view = nbuf.at[seq, t, at, :]
        remote(view, view, g_send.at[0], g_recv.at[role], t_dev).wait_recv()

    def gather_start(phase):
        for role in (1, 2, 0, 3, 6):
            rows_copy(phase, role).start()

    def gather_first(phase):
        rows_wait(phase, 2)
        rows_copy(phase, 4).start()
        rows_wait(phase, 1)
        rows_copy(phase, 5).start()
        rows_copy(phase, 9).start()
        rows_copy(phase, 8).start()

    def gather_second(phase):
        rows_wait(phase, 0)
        rows_copy(phase, 7).start()
        rows_wait(phase, 3)
        rows_copy(phase, 10).start()

    def gather_last(phase):
        rows_wait(phase, 4)
        rows_copy(phase, 11).start()
        rows_wait(phase, 5)
        rows_copy(phase, 12).start()
        rows_wait(phase, 6)
        sent(nbuf.at[pl.ds(0, 2)], g_send.at[0])
        sent(nbuf.at[pl.ds(0, 3), 0], g_send.at[1])

    def products(phase, p, left, weights, k, piece=(0, 4)):
        need(k, p, piece)
        first, size = planes[p] * 2, min(piece[1], 2)

        def product(side, start):
            rows_now = left[:, side].reshape(4 * half, left.shape[-1])
            column = start % 2 * unit
            weight = weights[first + start // 2, :, column : column + size * unit]
            value = jnp.dot(rows_now, weight, preferred_element_type=F32)
            return value.astype(LOW).reshape(4, half, size * unit)

        starts = range(piece[0], sum(piece), size)
        for start in starts:
            oth[p, :, :, start * unit : (start + size) * unit] = product(1 - t, start)
        sum_copies(phase, p, 0, piece).start()
        for start in starts:
            value = product(t, start).reshape(2, 2, half, size * unit)
            kept[p, :, :, :, start * unit : (start + size) * unit] = value

    def span_of(piece):
        return pl.ds(piece[0] * unit, piece[1] * unit)

    def sum_copies(phase, p, number, piece):
        at = span_of(piece)
        src, dst, device = (
            (oth.at[p, :, :, at], rt.at[phase, p, :, :, at], t_dev),
            (kept.at[p, 1 - r, :, top, at], r1.at[phase, p, 0, :, :, at], x_dev),
            (kept.at[p, :, 1 - y, low, at], r1.at[phase, p, 1, :, :, at], y_dev),
            (kept.at[p, r, 1 - y, top, at], r2.at[phase, p, 0, :, at], y_dev),
            (kept.at[p, 1 - r, y, low, at], r2.at[phase, p, 1, :, at], x_dev),
        )[number]
        return remote(src, dst, *sum_sems(phase, p, number, piece), device)

    def sum_sems(phase, p, number, piece):
        place = PIECES.index((p, piece[0])) if phase else p
        return m_send.at[place, min(number, 1)], m_recv.at[place, number]

    def direct_copy(p, number, piece):
        at, device = span_of(piece), (x_dev, y_dev, d_dev)[number]
        a, b = ((1 - r, y), (r, 1 - y), (1 - r, 1 - y))[number]
        src, dst = kept.at[p, a, b, :, at], rd.at[piece[0] % 2, number]
        return remote(src, dst, *sum_sems(1, p, 1 + number, piece), device)

    holder = lax.div(planes[3], 2)
    collects = t == holder

    def collect_copy(number):
        a, b = ((1 - r, y), (r, 1 - y), (1 - r, 1 - y), (r, y))[number]
        device = {**(x_dev, y_dev, d_dev, {})[number], "tp": holder}
        if number == 3:
            device = t_dev
        send = c_send.at[0] if number == 3 else sum_sems(1, 3, 1, (3, 1))[0]
        src = kept.at[3, a, b, :, span_of((3, 1))]
        return remote(src, rc.at[t, number], send, c_recv.at[t, number], device)

    def base_copy():
        src = mx.at[:, columns_of(planes[3], (3, 1))]
        return remote(src, base_rows, c_send.at[1], c_send.at[2], t_dev)

    def collected(side, number):
        view = rc.at[side, number]
        remote(view, view, c_send.at[0], c_recv.at[side, number], t_dev).wait_recv()
        return rc[side, number].astype(F32)

    def collect_done():
        piece = (3, 1)
        at = columns_of(lax.rem(planes[3], 2), piece)

        @pl.when(collects)
        def _():
            total = kept[3, r, y, :, span_of(piece)].astype(F32)
            for number in range(3):
                total = total + collected(t, number)
            base = mx[:, columns_of(planes[3], piece)].astype(F32)
            out[t, :, at] = (base + total).astype(LOW)
            base_copy().wait_recv()
            total = collected(1 - t, 3)
            for number in range(3):
                total = total + collected(1 - t, number)
            out[1 - t, :, at] = (base_rows[...].astype(F32) + total).astype(LOW)

        @pl.when(jnp.logical_not(collects))
        def _():
            collect_copy(3).wait_send()
            base_copy().wait_send()

        sums_sent(1, 3, piece)

    def pair_sums(phase, p, piece=(0, 4)):
        sum_copies(phase, p, 0, piece).wait_recv()
        at = span_of(piece)

        def step(s, carry):
            a, b = lax.div(s, 2), lax.rem(s, 2)
            value = kept[p, a, b, :, at].astype(F32) + rt[phase, p, s, :, at].astype(F32)
            kept[p, a, b, :, at] = value.astype(LOW)
            return carry

        lax.fori_loop(0, 4, step, 0)
        if piece == (3, 1):
            for number in (2, 0, 1):
                collect_copy(number).start()
            pl.when(jnp.logical_not(collects))(lambda: collect_copy(3).start())
        elif piece[1] == 1:
            for number in (2, 0, 1):
                direct_copy(p, number, piece).start()
        else:
            sum_copies(phase, p, 1, piece).start()
            sum_copies(phase, p, 2, piece).start()

    def line_sums(phase, p, piece=(0, 4)):
        at = span_of(piece)
        sum_copies(phase, p, 1, piece).wait_recv()
        for i in range(2):
            value = kept[p, r, i, top, at].astype(F32) + r1[phase, p, 0, i, :, at].astype(F32)
            kept[p, r, i, top, at] = value.astype(LOW)
        sum_copies(phase, p, 3, piece).start()
        sum_copies(phase, p, 2, piece).wait_recv()
        for i in range(2):
            value = kept[p, i, y, low, at].astype(F32) + r1[phase, p, 1, i, :, at].astype(F32)
            kept[p, i, y, low, at] = value.astype(LOW)
        sum_copies(phase, p, 4, piece).start()

    def columns_of(plane, piece):
        start = pl.multiple_of((plane * 4 + piece[0]) * unit, unit)
        return pl.ds(start, piece[1] * unit)

    def sums_sent(phase, p, piece):
        sum_copies(phase, p, 0, piece).wait_send()
        view = oth.at[p, pl.ds(0, 3), :, span_of(piece)]
        sent(view, sum_sems(phase, p, 1, piece)[0])

    def last_sums(phase, p, base, piece):
        at, inside = columns_of(planes[p], piece), span_of(piece)
        if piece[1] == 1:
            total = kept[p, r, y, :, inside].astype(F32)
            for number in range(3):
                direct_copy(p, number, piece).wait_recv()
                total = total + rd[piece[0] % 2, number].astype(F32)
            value = (base[:, at].astype(F32) + total).astype(LOW)
            sums_sent(phase, p, piece)
            return at, [value[:part], value[part:]]
        values = []
        for i, number in enumerate((3, 4)):
            span = slice(i * part, (i + 1) * part)
            sum_copies(phase, p, number, piece).wait_recv()
            value = kept[p, r, y, span, inside].astype(F32) + r2[phase, p, i, :, inside].astype(F32)
            values.append((base[span, at].astype(F32) + value).astype(LOW))
        sums_sent(phase, p, piece)
        return at, values

    def mix_done(p):
        at, values = last_sums(0, p, tk, (0, 4))
        for i, value in enumerate(values):
            mx[i * part : (i + 1) * part, at] = value

    def out_copy(p, piece):
        at = columns_of(lax.rem(planes[p], 2), piece)
        src = oo.at[p, :, span_of(piece)]
        return remote(src, out.at[t, :, at], o_sem.at[0], o_sem.at[1], t_dev)

    def down_done(p, piece=(0, 4)):
        _, values = last_sums(1, p, mx, piece)
        local = lax.div(planes[p], 2) == t
        at = columns_of(lax.rem(planes[p], 2), piece)

        @pl.when(local)
        def _():
            for i, value in enumerate(values):
                out[t, i * part : (i + 1) * part, at] = value

        @pl.when(jnp.logical_not(local))
        def _():
            for i, value in enumerate(values):
                oo[p, i * part : (i + 1) * part, span_of(piece)] = value
            out_copy(p, piece).start()

    loaded(REC, f_rec)
    y_rec[...] = f_rec[1].astype(LOW)
    rec_w[f] = f_rec[0].astype(LOW)
    pl.semaphore_wait(barrier, 9)
    token_swap.start()
    y_copy(REC).start()
    send_own(REC, 0)
    loaded(4, tk.at[:, side])
    token_swap.wait()
    norm_rows(tk, gain_one)
    gather_start(0)

    loaded(MIX, f_mix)
    y_mix[...] = (f_mix[1] * mix_scale[...]).astype(LOW)
    mix_w[f] = (f_mix[0] * mix_scale[...]).astype(LOW)


    @pl.when(inner)
    def _():
        send_one(MIX, 0, 1)

    send_own(REC, 1)
    for i in range(extra.shape[0]):
        lanes = slice(i * block, (i + 1) * block)
        ext[own, :, lanes] = jnp.broadcast_to(extra[i : i + 1, :], (ext.shape[1], block))
    ext_copies = [
        remote(ext.at[own], ext.at[own], ex_sem.at[0], ex_sem.at[1], device)
        for device in (x_dev, y_dev, d_dev)
    ]
    for copy in ext_copies:
        copy.start()
    loaded(GU, f_gu)
    loaded(DOWN, f_down)
    for i in range(2):
        y_gu[:, i * units : (i + 1) * units] = f_gu[1, i].astype(LOW)
        gu_w[f, :, i * units : (i + 1) * units] = f_gu[0, i].astype(LOW)
    y_down[...] = (f_down[1] * down_scale[...]).astype(LOW)
    down_w[f] = (f_down[0] * down_scale[...]).astype(LOW)

    send_one(MIX, 0, 0)

    @pl.when(jnp.logical_not(inner))
    def _():
        send_one(MIX, 0, 1)

    forward(REC, 0, 0)
    forward(REC, 1, 0)
    gather_first(0)
    y_copy(MIX).start()
    y_copy(GU).start()
    y_copy(DOWN).start()
    forward(REC, 0, 1)
    forward(REC, 1, 1)
    gather_second(0)
    forward(MIX, 0, 0)
    forward(MIX, 1, 0)
    gather_last(0)
    three = ext.at[pl.ds(0, 3)]
    remote(three, three, ex_sem.at[0], ex_sem.at[1], t_dev).wait_recv()
    for p in range(1, 4):
        need(REC, p)
    loaded(5, recur_blocks)
    loaded(6, input_blocks)

    at_chans = pl.multiple_of(q * chans, chans)

    def recur(s, carry):
        @pl.when(s == 1)
        def _():
            send_own(MIX, 1)
            send_own(GU, 0)

        @pl.when(s == 2)
        def _():
            forward(MIX, 0, 1)

        @pl.when(s == 3)
        def _():
            forward(MIX, 1, 1)

        left = nbuf[s].reshape(rows, width)
        total = jnp.dot(left, rec_w[...].reshape(width, chans), preferred_element_type=F32)
        for b in range(chans // block):
            here = slice(b * block, (b + 1) * block)
            number = q * (chans // block) + b
            ri[:, here] = (total[:, here] * rec_scale[pl.ds(number, 1), :]).astype(LOW)
        ecol[...] = jnp.broadcast_to(ext[s, 0:1, :], (block, rows)).T
        for b in range(chans // block):
            here = slice(b * block, (b + 1) * block)
            lanes = pl.ds(pl.multiple_of(at_chans + b * block, block), block)
            number = q * (chans // block) + b
            values = ri[:, here].astype(F32)
            places = lax.broadcasted_iota(jnp.int32, values.shape, 0)
            conv_out = taps[tap_count - 1 : tap_count, lanes] * values
            for back in range(1, tap_count):
                moved = jnp.where(places >= back, pltpu.roll(values, back, 0), 0.0)
                tap = tap_count - 1 - back
                conv_out = conv_out + taps[tap : tap + 1, lanes] * moved
            conv_low = conv_out.astype(LOW)
            recur_gate = jax.nn.sigmoid(
                jnp.dot(conv_low, recur_blocks[b], preferred_element_type=F32)
            )
            input_gate = jax.nn.sigmoid(
                jnp.dot(conv_low, input_blocks[b], preferred_element_type=F32)
            )
            param = -decay_param[pl.ds(number, 1), :]
            soft = jnp.maximum(param, 0.0) + jnp.log1p(jnp.exp(-jnp.abs(param)))
            log_decay = -DECAY_FACTOR * recur_gate * soft + ecol[...]
            decay = jnp.exp(log_decay)
            drive = jnp.sqrt(-jnp.tanh(log_decay) * (1.0 + decay * decay)) * input_gate * conv_out
            step = 1
            while step < rows:
                keep = places >= step
                drive = drive + decay * jnp.where(keep, pltpu.roll(drive, step, 0), 0.0)
                if step * 2 < rows:
                    decay = decay * jnp.where(keep, pltpu.roll(decay, step, 0), 1.0)
                step *= 2
            state = drive.astype(LOW)
            st[s, 0, :, here] = state[:half]
            st[s, 1, :, here] = state[half:]
        return carry

    lax.fori_loop(0, 4, recur, 0)

    products(0, 0, st, mix_w, MIX)
    products(0, 1, st, mix_w, MIX)
    pair_sums(0, 0)
    send_own(GU, 1)
    pair_sums(0, 1)
    products(0, 2, st, mix_w, MIX)
    line_sums(0, 0)
    pair_sums(0, 2)
    line_sums(0, 1)
    products(0, 3, st, mix_w, MIX)
    mix_done(0)
    pair_sums(0, 3)
    forward(GU, 0, 0)
    line_sums(0, 2)
    mix_done(1)
    forward(GU, 1, 0)
    line_sums(0, 3)
    mix_done(2)
    mix_done(3)

    norm_rows(mx, gain_two)
    gather_start(1)
    pl.when(jnp.logical_not(collects))(lambda: base_copy().start())
    gather_first(1)
    wait_block(DOWN, fp)
    forward(GU, 0, 1)
    gather_second(1)
    forward(GU, 1, 1)
    gather_last(1)
    send_own(DOWN, 0)
    send_own(DOWN, 1)
    for p in range(1, 4):
        need(GU, p)

    unit_rows = units // block

    def unit_scales(scale):
        first = q * unit_rows
        return jnp.concatenate([scale[pl.ds(first + i, 1), :] for i in range(unit_rows)], 1)

    def hidden(s, carry):
        left = nbuf[s].reshape(rows, width)
        total = jnp.dot(left, gu_w[...].reshape(width, 2 * units), preferred_element_type=F32)
        gate = total[:, :units] * unit_scales(gate_scale)
        up = total[:, units:] * unit_scales(up_scale)
        value = (gate * jax.nn.sigmoid(gate) * up).astype(LOW)
        hid[s, 0] = value[:half]
        hid[s, 1] = value[half:]
        return carry

    lax.fori_loop(0, 4, hidden, 0)

    first, second, third, fourth = (0, 2), (2, 2), (2, 1), (3, 1)

    def down_products(p, piece=(0, 4)):
        products(1, p, hid, down_w, DOWN, piece)

    down_products(0)
    pair_sums(1, 0)
    down_products(1)
    forward(DOWN, 0, 0)
    pair_sums(1, 1)
    line_sums(1, 0)
    forward(DOWN, 0, 1)
    forward(DOWN, 1, 0)
    down_products(2, first)
    pair_sums(1, 2, first)
    down_done(0)
    line_sums(1, 1)
    line_sums(1, 2, first)
    forward(DOWN, 1, 1)
    down_products(2, second)
    pair_sums(1, 2, second)
    down_done(1)
    down_done(2, first)
    line_sums(1, 2, second)
    down_products(3, first)
    pair_sums(1, 3, first)
    down_products(3, third)
    down_done(2, second)
    pair_sums(1, 3, third)
    line_sums(1, 3, first)
    down_products(3, fourth)
    pair_sums(1, 3, fourth)
    down_done(3, first)
    down_done(3, third)
    collect_done()

    whole, less = out.at[1 - t], out.at[1 - t, :, pl.ds(0, half_width - unit)]
    whole = remote(whole, whole, o_sem.at[0], o_sem.at[1], t_dev)
    less = remote(less, less, o_sem.at[0], o_sem.at[1], t_dev)

    @pl.when(collects)
    def _():
        less.wait_recv()
        whole.wait_send()

    @pl.when(jnp.logical_not(collects))
    def _():
        whole.wait_recv()
        less.wait_send()

    for k in range(4):
        y_copy(k).wait_send()
        sent(mats[k].at[pl.ds(0, 4)], wo_send.at[k])

        @pl.when(inner)
        def _():
            sent(mats[k].at[pl.ds(0, 4)], wf_send.at[k])

    sent(ext.at[pl.ds(0, 3)], ex_sem.at[0])


def team_body(
    tokens,
    mixing_norm_gain,
    recurrent_input_weight,
    recurrent_input_scale,
    convolution_kernel_taps,
    recurrence_gate_weight_blocks,
    input_gate_weight_blocks,
    channel_decay_parameter,
    token_extra_log_decay,
    mixing_output_weight,
    mixing_output_scale,
    feedforward_norm_gain,
    feedforward_gate_weight,
    feedforward_gate_scale,
    feedforward_up_weight,
    feedforward_up_scale,
    feedforward_down_weight,
    feedforward_down_scale,
):
    rows, half_width = tokens.shape
    half, part = rows // 2, rows // 4
    width = half_width * 2
    depth = recurrent_input_weight.shape[0]
    chans = recurrent_input_weight.shape[1] // 4
    units = feedforward_gate_weight.shape[1] // 4
    cols = mixing_output_weight.shape[1]
    block = recurrence_gate_weight_blocks.shape[1]
    planes = width // depth
    any_spec = pl.BlockSpec(memory_space=pl.ANY)
    vmem_spec = pl.BlockSpec(memory_space=pltpu.VMEM)
    vmem = pltpu.VMEM
    dma = pltpu.SemaphoreType.DMA

    def row(vector):
        return vector.reshape(1, -1)

    def lines(vector):
        return vector.reshape(-1, block)

    out = pl.pallas_call(
        layer_kernel,
        out_shape=vmem((2, half, half_width), LOW),
        in_specs=[any_spec] * 6 + [vmem_spec] * 3 + [any_spec] * 2 + [vmem_spec] * 7,
        out_specs=vmem_spec,
        scratch_shapes=[
            vmem((4, 2, half, width), LOW),
            vmem((planes, depth, chans), LOW),
            vmem((planes, chans, cols), LOW),
            vmem((planes, depth, 2 * units), LOW),
            vmem((planes, units, cols), LOW),
            vmem((2, depth, chans), F32),
            vmem((2, chans, cols), F32),
            vmem((2, 2, depth, units), F32),
            vmem((2, units, cols), F32),
            vmem((depth, chans), LOW),
            vmem((chans, cols), LOW),
            vmem((depth, 2 * units), LOW),
            vmem((units, cols), LOW),
            vmem((half, width), LOW),
            vmem((half, width), LOW),
            vmem((4, 2, half, chans), LOW),
            vmem((4, 2, half, units), LOW),
            vmem((rows, chans), LOW),
            vmem((4, 8, rows), F32),
            vmem((rows, block), F32),
            vmem((4, 4, half, 2 * cols), LOW),
            vmem((4, 2, 2, half, 2 * cols), LOW),
            vmem((2, 4, 4, half, 2 * cols), LOW),
            vmem((2, 4, 2, 2, part, 2 * cols), LOW),
            vmem((2, 4, 2, part, 2 * cols), LOW),
            vmem((2, 3, half, cols // 2), LOW),
            vmem((2, 4, half, cols // 2), LOW),
            vmem((half, cols // 2), LOW),
            vmem((4, half, 2 * cols), LOW),
            vmem((chans // block, block, block), LOW),
            vmem((chans // block, block, block), LOW),
            dma((7,)),
            dma((2,)),
            dma((4,)),
            dma((4,)),
            dma((4,)),
            dma((4, planes)),
            dma((2,)),
            dma((7,)),
            dma((2,)),
            dma((2,)),
            dma((len(PIECES), 2)),
            dma((len(PIECES), 5)),
            dma((2,)),
            dma((3,)),
            dma((2, 4)),
        ],
        compiler_params=pltpu.CompilerParams(
            collective_id=0, has_side_effects=True, vmem_limit_bytes=VMEM_BYTES
        ),
    )(
        tokens,
        recurrent_input_weight,
        mixing_output_weight,
        feedforward_gate_weight,
        feedforward_up_weight,
        feedforward_down_weight,
        row(mixing_norm_gain),
        lines(recurrent_input_scale),
        convolution_kernel_taps,
        recurrence_gate_weight_blocks,
        input_gate_weight_blocks,
        lines(channel_decay_parameter),
        lines(token_extra_log_decay),
        row(mixing_output_scale),
        row(feedforward_norm_gain),
        lines(feedforward_gate_scale),
        lines(feedforward_up_scale),
        row(feedforward_down_scale),
    )
    return out.reshape(rows, half_width)


VMEM_BYTES = 60_000_000


def team_fits(mesh):
    sizes = mesh.shape
    return sizes["rep"] == 2 and sizes["tp"] == 2 and sizes["fs"] == 8


def solution(mesh):
    placed = (
        P(("rep", "fs"), "tp"),
        P(),
        P("fs", "tp"),
        P("tp"),
        P(None, "tp"),
        P("tp", None, None),
        P("tp", None, None),
        P("tp"),
        P(("rep", "fs")),
        P("tp", "fs"),
        P("fs"),
        P(),
        P("fs", "tp"),
        P("tp"),
        P("fs", "tp"),
        P("tp"),
        P("tp", "fs"),
        P("fs"),
    )

    def body(*args):
        blocks, hidden, rows = args[5].shape[0], args[12].shape[1], args[0].shape[0]
        if not team_fits(mesh) or blocks % 4 or hidden % 512 or rows % 64 or args[9].shape[1] % 256:
            return plain_body(*args)
        return team_body(*args)

    return jax.shard_map(
        body, mesh=mesh, in_specs=placed, out_specs=P(("rep", "fs"), "tp"), check_vma=False
    )
```
